32 devices in a mesh: sp: 16 (over z, y, core), tp: 2 (over x).
Axes of the slice: x: 2, y: 2, z: 4, core: 2. Of those that a mesh axis runs over, the one named last changes fastest.
Arguments:
- layer_source_rows: bfloat16 [6144, 2048], P(('sp', 'tp')), may hold values from -6 to 6
- entry_rescale_factor: bfloat16 [2048], replicated, may hold values from 0.099609375 to 1.8984375
- sliding_mixer_entry_matrix: bfloat16 [3, 2048, 1024], P(None, 'sp', 'tp'), may hold values from -0.125 to 0.125
- recurrent_mixer_entry_matrix: bfloat16 [2, 2048, 1024], P(None, 'sp', 'tp'), may hold values from -0.125 to 0.125
- latent_write_read_matrix: bfloat16 [2, 2048, 2048], P(None, 'sp', 'tp'), may hold values from -0.125 to 0.125
- timestep_matrix: bfloat16 [2048, 2, 16], P(None, None, 'tp'), may hold values from -0.125 to 0.125
- sliding_kernel_coefficients: bfloat16 [3, 1024], P(None, 'tp'), may hold values from -3.5 to 3.5
- recurrent_kernel_coefficients: bfloat16 [5, 1024], P(None, 'tp'), may hold values from -0.5 to 0.5
- latent_kernel_coefficients: bfloat16 [5, 2, 2048], P(None, None, 'tp'), may hold values from -0.5 to 0.5
- lane_forgetting_rate: float32 [2, 16], P(None, 'tp'), may hold values from 0 to 1
- spike_forgetting_rate: float32 [6144, 16], P('sp', 'tp'), may hold values from -2 to 0
- lane_rescale_factor: bfloat16 [1024], P('tp'), may hold values from 0.099609375 to 1.8984375
- sliding_mixer_exit_matrix: bfloat16 [1024, 2048], P('tp', 'sp'), may hold values from -0.125 to 0.125
- recurrent_mixer_exit_matrix: bfloat16 [1024, 2048], P('tp', 'sp'), may hold values from -0.125 to 0.125
Outputs:
- mixed_out: bfloat16 [6144, 2048], P(('sp', 'tp'))
The draws below stay inside these ranges and needn't reach their ends.
All inputs are finite; a program needn't handle non-finite values.
Results may differ from the reference program's by a relative error of at most 0.017.
Values may be sent and summed in bfloat16 or wider, within the bound.
A program may use at most 64 MiB of HBM per device.

```python
import jax
import jax.numpy as jnp
from jax import lax

D = 2048
CONV_CH = 1024
MIXER_LANES = 16
HEAD_DIM = 64
GROUPS = 16
STATE = 128
BLOCK = 128
CONV_TAPS = 3
SSD_TAPS = 5
TOK_DEV = 384
SSD_W = 1024
GROUP_HEADS = 1
SEQ_LENGTH = 6144
N_TP = 2


def draw_lane_forgetting_rate(key, part):
    flag_key = jax.random.fold_in(key, 11)
    level_key = jax.random.fold_in(key, 12)
    fraction = jax.random.uniform(level_key, (2, MIXER_LANES), jnp.float32)
    slow_rates = jnp.exp(jnp.log(0.1 / SEQ_LENGTH) + fraction * jnp.log(5.0))
    fast_rates = jnp.exp(jnp.log(0.01) + fraction * jnp.log(4.0))
    fast_flag = jax.random.randint(flag_key, (2, MIXER_LANES), 0, 2) == 1
    return jnp.where(fast_flag, fast_rates, slow_rates).astype(jnp.float32)


def draw_spike_forgetting_rate(key, part):
    level_key = jax.random.fold_in(key, 21)
    where_random_seed = jax.random.fold_in(key, 22)
    amount_random_seed = jax.random.fold_in(key, 23)
    blocks = SEQ_LENGTH // TOK_DEV
    fraction = jax.random.uniform(level_key, (blocks, MIXER_LANES), jnp.float32)
    levels = jnp.exp(jnp.log(0.1 / SEQ_LENGTH) + fraction * jnp.log(10.0))
    spread_amounts = jnp.repeat(levels, TOK_DEV, axis=0)
    spike_sites = jax.random.randint(where_random_seed, (3, MIXER_LANES), 0, SEQ_LENGTH)
    spike_amounts = jax.random.uniform(amount_random_seed, (3, MIXER_LANES), jnp.float32, 0.22, 0.5)
    sequence_indices = jnp.arange(SEQ_LENGTH)[:, None, None]
    spike_counts = (sequence_indices == spike_sites[None]).astype(jnp.float32)
    return (-spread_amounts - jnp.sum(spike_counts * spike_amounts[None], axis=1)).astype(jnp.float32)


def level_of(key, shape, pieces, least, high):
    loudness, own = 1.0, jax.random.fold_in(key, 6)
    for dim, shards_of in pieces:
        draws = jnp.exp(jax.random.uniform(jax.random.fold_in(own, dim), (shards_of,), jnp.float32, least / len(pieces), high / len(pieces)))
        loudness = loudness * jnp.repeat(draws, shape[dim] // shards_of).reshape([-1 if axis == dim else 1 for axis in range(len(shape))])
    return loudness


def gaussian(own_key, extent, deviation, reach, shards=(), kind=jnp.bfloat16):
    values = deviation * jax.random.normal(own_key, extent, jnp.float32)
    if shards:
        values = values * level_of(own_key, extent, shards, -0.22, 0.18)
    return jnp.clip(values, -reach, reach).astype(kind)


def setup_inputs(seed: int = 0) -> dict:
    streams_of = jax.random.split(jax.random.key(seed), 15)
    layer_source_rows = gaussian(streams_of[0], (SEQ_LENGTH, D), 1.0, 6.0, ((0, 32),))
    entry_rescale_factor = jnp.clip(1.0 + 0.18 * jax.random.normal(streams_of[1], (D,), jnp.float32), 0.099609375, 1.8984375).astype(jnp.bfloat16)
    sliding_mixer_entry_matrix = gaussian(streams_of[2], (3, D, CONV_CH), D ** -0.5, 0.125, ((1, 16), (2, 2)))
    recurrent_mixer_entry_matrix = gaussian(streams_of[3], (2, D, SSD_W), D ** -0.5, 0.125, ((1, 16), (2, 2)))
    latent_write_read_matrix = gaussian(streams_of[4], (2, D, GROUPS * STATE), D ** -0.5, 0.125, ((1, 16), (2, 2)))
    timestep_matrix = gaussian(streams_of[5], (D, 2, MIXER_LANES), D ** -0.5, 0.125, ((2, 2),))
    sliding_kernel_coefficients = gaussian(streams_of[6], (CONV_TAPS, CONV_CH), CONV_TAPS ** -0.5, 3.5, ((1, 2),))
    recurrent_kernel_coefficients = gaussian(streams_of[7], (SSD_TAPS, SSD_W), 0.09, 0.5, ((1, 2),))
    latent_kernel_coefficients = gaussian(streams_of[8], (SSD_TAPS, 2, GROUPS * STATE), 0.09, 0.5, ((2, 2),))
    lane_forgetting_rate = draw_lane_forgetting_rate(jax.random.fold_in(streams_of[14], 71), 0)
    spike_forgetting_rate = draw_spike_forgetting_rate(jax.random.fold_in(streams_of[14], 71), 0)
    lane_rescale_factor = jnp.clip(1.0 + 0.18 * jax.random.normal(streams_of[11], (SSD_W,), jnp.float32), 0.099609375, 1.8984375).astype(jnp.bfloat16)
    sliding_mixer_exit_matrix = gaussian(streams_of[12], (CONV_CH, D), (CONV_CH + SSD_W) ** -0.5, 0.125, ((0, 2), (1, 16)))
    recurrent_mixer_exit_matrix = gaussian(streams_of[13], (SSD_W, D), (CONV_CH + SSD_W) ** -0.5, 0.125, ((0, 2), (1, 16)))
    return dict(layer_source_rows=layer_source_rows, entry_rescale_factor=entry_rescale_factor, sliding_mixer_entry_matrix=sliding_mixer_entry_matrix, recurrent_mixer_entry_matrix=recurrent_mixer_entry_matrix, latent_write_read_matrix=latent_write_read_matrix, timestep_matrix=timestep_matrix, sliding_kernel_coefficients=sliding_kernel_coefficients, recurrent_kernel_coefficients=recurrent_kernel_coefficients, latent_kernel_coefficients=latent_kernel_coefficients, lane_forgetting_rate=lane_forgetting_rate, spike_forgetting_rate=spike_forgetting_rate, lane_rescale_factor=lane_rescale_factor, sliding_mixer_exit_matrix=sliding_mixer_exit_matrix, recurrent_mixer_exit_matrix=recurrent_mixer_exit_matrix)


epsilon = 1e-05

def centred_taps(values, tap_table):
    tap_count = tap_table.shape[0]
    half_width = tap_count // 2
    length = values.shape[0]
    padded = jnp.pad(values, ((half_width, half_width), (0, 0)))
    summed = jnp.zeros(values.shape, jnp.float32)
    for offset in range(tap_count):
        summed = summed + padded[offset:offset + length] * tap_table[offset].astype(jnp.float32)
    return summed

def project(normed, weight):
    return jnp.dot(normed, weight, preferred_element_type=jnp.float32).astype(jnp.bfloat16)

def direction_pass(ssd_x, keys_b, reads_c, timestep_deltas, forgetting_exponent):
    length = ssd_x.shape[0]
    blocks = length // BLOCK
    x_blocks = ssd_x.reshape(blocks, BLOCK, GROUPS, GROUP_HEADS, HEAD_DIM)
    b_blocks = keys_b.reshape(blocks, BLOCK, GROUPS, STATE)
    c_blocks = reads_c.reshape(blocks, BLOCK, GROUPS, STATE)
    d_blocks = timestep_deltas.reshape(blocks, BLOCK, GROUPS, GROUP_HEADS)
    l_blocks = forgetting_exponent.reshape(blocks, BLOCK, GROUPS, GROUP_HEADS)
    lower_mask = (jnp.arange(BLOCK)[:, None] >= jnp.arange(BLOCK)[None, :])[:, :, None, None]

    def one_block(carry_state, inputs):
        x_block, b_block, c_block, d_block, l_block = inputs
        running = jnp.cumsum(l_block, axis=0)
        log_gaps = jnp.where(lower_mask, running[:, None] - running[None, :], 0.0)
        decays = jnp.where(lower_mask, jnp.exp(log_gaps), 0.0)
        scores = jnp.einsum('tgn,sgn->tsg', c_block.astype(jnp.float32), b_block.astype(jnp.float32))
        weights = (scores[..., None] * decays * d_block[None]).astype(jnp.bfloat16)
        within = jnp.einsum('tsgr,sgrp->tgrp', weights.astype(jnp.float32), x_block.astype(jnp.float32))
        entering = lax.optimization_barrier(carry_state.astype(jnp.bfloat16)).astype(jnp.float32)
        carried = jnp.einsum('tgn,grpn->tgrp', c_block.astype(jnp.float32), entering) * jnp.exp(running)[..., None]
        to_end = jnp.exp(running[-1][None] - running) * d_block
        weighted = (x_block.astype(jnp.float32) * to_end[..., None]).astype(jnp.bfloat16)
        contribution = jnp.einsum('sgrp,sgn->grpn', weighted.astype(jnp.float32), b_block.astype(jnp.float32))
        next_state = carry_state * jnp.exp(running[-1])[..., None, None] + contribution
        return (next_state, within + carried)
    initial = jnp.zeros((GROUPS, GROUP_HEADS, HEAD_DIM, STATE), jnp.float32)
    final_state, outputs = lax.scan(one_block, initial, (x_blocks, b_blocks, c_blocks, d_blocks, l_blocks))
    return outputs.reshape(length, GROUPS, GROUP_HEADS, HEAD_DIM)

def reference(layer_source_rows, entry_rescale_factor, sliding_mixer_entry_matrix, recurrent_mixer_entry_matrix, latent_write_read_matrix, timestep_matrix, sliding_kernel_coefficients, recurrent_kernel_coefficients, latent_kernel_coefficients, lane_forgetting_rate, spike_forgetting_rate, lane_rescale_factor, sliding_mixer_exit_matrix, recurrent_mixer_exit_matrix):
    float_rows = layer_source_rows.astype(jnp.float32)
    normed = (float_rows * lax.rsqrt(lax.optimization_barrier(jnp.mean(float_rows * float_rows, axis=-1, keepdims=True)) + epsilon) * entry_rescale_factor.astype(jnp.float32)).astype(jnp.bfloat16)
    out_gate = project(normed, sliding_mixer_entry_matrix[0])
    in_gate = project(normed, sliding_mixer_entry_matrix[1])
    values = project(normed, sliding_mixer_entry_matrix[2])
    ssd_gate = project(normed, recurrent_mixer_entry_matrix[0])
    ssd_in = project(normed, recurrent_mixer_entry_matrix[1])
    inject = project(normed, latent_write_read_matrix[0])
    readout = project(normed, latent_write_read_matrix[1])
    raw_step = project(normed, timestep_matrix.reshape(timestep_matrix.shape[0], 2 * MIXER_LANES)).reshape(-1, 2, MIXER_LANES)
    gated_in = (in_gate.astype(jnp.float32) * values.astype(jnp.float32)).astype(jnp.bfloat16)
    y_conv = (out_gate.astype(jnp.float32) * centred_taps(gated_in.astype(jnp.float32), sliding_kernel_coefficients)).astype(jnp.bfloat16)
    joined = jnp.concatenate([ssd_in, inject, readout], axis=1).astype(jnp.float32)
    joined_taps = jnp.concatenate([recurrent_kernel_coefficients, latent_kernel_coefficients.reshape(latent_kernel_coefficients.shape[0], -1)], axis=1)
    mixed_ssd = jax.nn.silu(centred_taps(joined, joined_taps)).astype(jnp.bfloat16)
    length = layer_source_rows.shape[0]
    ssd_x = mixed_ssd[:, :SSD_W]
    keys_b = mixed_ssd[:, SSD_W:SSD_W + GROUPS * STATE]
    reads_c = mixed_ssd[:, SSD_W + GROUPS * STATE:]
    timestep_deltas = jax.nn.softplus(raw_step.astype(jnp.float32))
    forgetting_exponent = -timestep_deltas * lane_forgetting_rate.astype(jnp.float32)[None] + spike_forgetting_rate.astype(jnp.float32)[:, None, :]
    y_fwd = direction_pass(ssd_x, keys_b, reads_c, timestep_deltas[:, 0], forgetting_exponent[:, 0])
    y_bwd = jnp.flip(direction_pass(jnp.flip(ssd_x, 0), jnp.flip(keys_b, 0), jnp.flip(reads_c, 0), jnp.flip(timestep_deltas[:, 1], 0), jnp.flip(forgetting_exponent[:, 1], 0)), 0)
    gated_out = (y_fwd + y_bwd).reshape(length, SSD_W) * jax.nn.silu(ssd_gate.astype(jnp.float32))
    grouped = gated_out.reshape(length, GROUPS, GROUP_HEADS * HEAD_DIM)
    grouped = grouped * lax.rsqrt(lax.optimization_barrier(jnp.mean(grouped * grouped, axis=-1, keepdims=True)) + epsilon)
    y_ssd = (grouped.reshape(length, SSD_W) * lane_rescale_factor.astype(jnp.float32)).astype(jnp.bfloat16)
    conv_part = CONV_CH // N_TP
    ssd_part = SSD_W // N_TP
    summed = jnp.zeros((length, D), jnp.float32)
    for source in range(N_TP):
        partial_value = jnp.dot(y_conv[:, source * conv_part:(source + 1) * conv_part], sliding_mixer_exit_matrix[source * conv_part:(source + 1) * conv_part], preferred_element_type=jnp.float32)
        partial_value = partial_value + jnp.dot(y_ssd[:, source * ssd_part:(source + 1) * ssd_part], recurrent_mixer_exit_matrix[source * ssd_part:(source + 1) * ssd_part], preferred_element_type=jnp.float32)
        summed = summed + lax.optimization_barrier(partial_value.astype(jnp.bfloat16)).astype(jnp.float32)
    return summed.astype(jnp.bfloat16)
```

```python
import functools

import jax
import jax.numpy as jnp
from jax import lax
from jax.experimental import pallas as pl
from jax.experimental.pallas import tpu as pltpu
from jax.sharding import PartitionSpec as P

HEAD_DIM = 64
STATE = 128
HALO = 16
CHUNKS = 2
epsilon = 1e-05
F32 = jnp.float32
BF16 = jnp.bfloat16
HIGHEST = lax.Precision.HIGHEST


def ring_kernel(n, w_ref, out_ref, own_sem, ring_send, ring_recv, mate_send, mate_recv):
    chips = n // 2
    me = lax.axis_index("sp")
    core, chip = me % 2, me // 2
    odd = chip % 2
    spot = (1 - odd) * (chip // 2) + odd * (chips - 1 - chip // 2)

    def device(position):
        position = (position + 2 * chips) % chips
        half = (chips + 1) // 2
        late = position // half
        late_chip = 2 * (chips - 1 - position) + 1
        return 2 * ((1 - late) * 2 * position + late * late_chip) + core

    mate = me + 1 - 2 * core
    ways = (device(spot + 1), device(spot - 1))
    rows = w_ref.shape[0] // (2 * CHUNKS)

    barrier = pltpu.get_barrier_semaphore()
    for other in (mate,) + ways:
        pl.semaphore_signal(
            barrier, inc=1, device_id={"sp": other}, device_id_type=pl.DeviceIdType.MESH
        )
    pl.semaphore_wait(barrier, 3)

    def piece(way, chunk):
        return pl.ds((way * CHUNKS + chunk) * rows, rows)

    def ring_copy(step, way, chunk):
        owner = device(spot - step if way == 0 else spot + step)
        part = piece(way, chunk)
        return pltpu.make_async_remote_copy(
            src_ref=w_ref.at[part] if step == 0 else out_ref.at[owner, part],
            dst_ref=out_ref.at[owner, part],
            send_sem=ring_send.at[step, way, chunk],
            recv_sem=ring_recv.at[step, way, chunk],
            device_id={"sp": ways[way]},
            device_id_type=pl.DeviceIdType.MESH,
        )

    def arrival(step, way, chunk):
        owner = device(spot - step - 1 if way == 0 else spot + step + 1)
        part = piece(way, chunk)
        return pltpu.make_async_remote_copy(
            src_ref=out_ref.at[owner, part],
            dst_ref=out_ref.at[owner, part],
            send_sem=ring_send.at[step, way, chunk],
            recv_sem=ring_recv.at[step, way, chunk],
            device_id={"sp": ways[way]},
            device_id_type=pl.DeviceIdType.MESH,
        )

    def mate_copy(step, way, chunk, incoming=False):
        owner = device(spot - step if way == 0 else spot + step)
        if incoming:
            owner = owner + 1 - 2 * core
        part = piece(way, chunk)
        return pltpu.make_async_remote_copy(
            src_ref=w_ref.at[part] if step == 0 else out_ref.at[owner, part],
            dst_ref=out_ref.at[owner, part],
            send_sem=mate_send.at[step, way, chunk],
            recv_sem=mate_recv.at[step, way, chunk],
            device_id={"sp": mate},
            device_id_type=pl.DeviceIdType.MESH,
        )

    parts = [(way, chunk) for chunk in range(CHUNKS) for way in range(2)]
    for way, chunk in parts:
        ring_copy(0, way, chunk).start()
    for way, chunk in parts:
        mate_copy(0, way, chunk).start()
    own = pltpu.make_async_copy(w_ref, out_ref.at[me], own_sem)
    own.start()
    for step in range(chips - 1):
        for way, chunk in parts:
            arrival(step, way, chunk).wait_recv()
            if step < chips - 2:
                ring_copy(step + 1, way, chunk).start()
            mate_copy(step + 1, way, chunk).start()
    own.wait()
    for step in range(chips):
        for way, chunk in parts:
            if step < chips - 1:
                ring_copy(step, way, chunk).wait_send()
            mate_copy(step, way, chunk).wait_send()
            mate_copy(step, way, chunk, True).wait_recv()


def gather_rows(block):
    n = lax.axis_size("sp")
    chips = n // 2
    rows, cols = block.shape
    return pl.pallas_call(
        functools.partial(ring_kernel, n),
        out_shape=jax.ShapeDtypeStruct((n, rows, cols), block.dtype),
        in_specs=[pl.BlockSpec(memory_space=pltpu.VMEM)],
        out_specs=pl.BlockSpec(memory_space=pl.ANY),
        scratch_shapes=[
            pltpu.SemaphoreType.DMA,
            pltpu.SemaphoreType.DMA((chips - 1, 2, CHUNKS)),
            pltpu.SemaphoreType.DMA((chips - 1, 2, CHUNKS)),
            pltpu.SemaphoreType.DMA((chips, 2, CHUNKS)),
            pltpu.SemaphoreType.DMA((chips, 2, CHUNKS)),
        ],
        compiler_params=pltpu.CompilerParams(
            collective_id=0, has_side_effects=True, vmem_limit_bytes=16 * 2**20
        ),
        cost_estimate=pl.CostEstimate(
            flops=0, bytes_accessed=n * rows * cols * 16, transcendentals=0
        ),
    )(block)


def taps_of(padded, table, length):
    full = padded.shape[0]
    half = table.shape[0] // 2
    total = None
    for k in range(table.shape[0]):
        moved = padded if k == half else pltpu.roll(padded, (half - k) % full, 0)
        term = moved[HALO : HALO + length] * table[k : k + 1].astype(F32)
        total = term if total is None else total + term
    return total


def silu(v):
    return v * jax.nn.sigmoid(v)


def mix_kernel(
    og_ref, ig_ref, va_ref, x_ref, b_ref, c_ref, ct_ref, xt_ref, bt_ref, rt_ref,
    col_ref, row_ref, yconv_ref, within_ref, reads_ref, state_ref,
):
    length = yconv_ref.shape[0]
    gated = (ig_ref[...].astype(F32) * va_ref[...].astype(F32)).astype(BF16).astype(F32)
    conv = taps_of(gated, ct_ref[...], length)
    yconv_ref[...] = (og_ref[pl.ds(HALO, length), :].astype(F32) * conv).astype(BF16)
    xs = silu(taps_of(x_ref[...].astype(F32), xt_ref[...], length)).astype(BF16)
    bs = silu(taps_of(b_ref[...].astype(F32), bt_ref[...], length)).astype(BF16)
    cs = silu(taps_of(c_ref[...].astype(F32), rt_ref[...], length)).astype(BF16)
    reads_ref[...] = cs
    cols = col_ref[0]
    rows = row_ref[0]
    t_at = lax.broadcasted_iota(jnp.int32, (length, length), 0)
    s_at = lax.broadcasted_iota(jnp.int32, (length, length), 1)
    outs, weighted = [], []
    for h in range(2):
        c_h = cs[:, h * STATE : (h + 1) * STATE]
        b_h = bs[:, h * STATE : (h + 1) * STATE]
        x_h = xs[:, h * HEAD_DIM : (h + 1) * HEAD_DIM]
        o = 4 * h
        scores = lax.dot_general(
            c_h, b_h, (((1,), (1,)), ((), ())), preferred_element_type=F32
        )
        gap = jnp.where(
            t_at >= s_at,
            cols[:, o + 2 : o + 3] - rows[o + 2 : o + 3],
            cols[:, o + 3 : o + 4] - rows[o + 3 : o + 4],
        )
        d_f, d_b = rows[o : o + 1], rows[o + 1 : o + 2]
        scale = jnp.where(t_at > s_at, d_f, jnp.where(t_at < s_at, d_b, d_f + d_b))
        w = (scores * jnp.exp(gap) * scale).astype(BF16)
        outs.append(jnp.dot(w, x_h, preferred_element_type=F32))
        x32 = x_h.astype(F32)
        end_f = jnp.exp(rows[o + 2 : o + 3, length - 1 : length] - cols[:, o + 2 : o + 3])
        end_b = jnp.exp(rows[o + 3 : o + 4, 0:1] - cols[:, o + 3 : o + 4])
        both = jnp.concatenate(
            [x32 * (end_f * cols[:, o : o + 1]), x32 * (end_b * cols[:, o + 1 : o + 2])], axis=1
        ).astype(BF16)
        state_ref[h * STATE : (h + 1) * STATE] = lax.dot_general(
            both, b_h, (((0,), (0,)), ((), ())), preferred_element_type=F32
        ).astype(BF16)
    within_ref[...] = jnp.concatenate(outs, axis=1)


def exchange_kernel(
    n, share, s_ref, l_ref, out_ref, got, logs, enter, s_out, s_in, l_out, l_in, e_out, e_in
):
    me = lax.axis_index("sp")
    barrier = pltpu.get_barrier_semaphore()
    for k in range(1, n):
        pl.semaphore_signal(
            barrier,
            inc=1,
            device_id={"sp": (me + k) % n},
            device_id_type=pl.DeviceIdType.MESH,
        )
    pl.semaphore_wait(barrier, n - 1)

    def copy(src, dst, out_sem, in_sem, k, there, slot):
        return pltpu.make_async_remote_copy(
            src_ref=src.at[there],
            dst_ref=dst.at[slot],
            send_sem=out_sem.at[k],
            recv_sem=in_sem.at[k],
            device_id={"sp": there},
            device_id_type=pl.DeviceIdType.MESH,
        )

    for k in range(1, n):
        there = (me + k) % n
        copy(s_ref, got, s_out, s_in, k, there, me).start()
        copy(l_ref, logs, l_out, l_in, k, there, me).start()
    got[me] = s_ref[me]
    logs[me] = l_ref[me]
    for k in range(1, n):
        here = (me + n - k) % n
        copy(s_ref, got, s_out, s_in, k, here, here).wait_recv()
        copy(l_ref, logs, l_out, l_in, k, here, here).wait_recv()
    back = (me * share // HEAD_DIM) % 2
    acc = jnp.zeros(s_ref.shape[1:], F32)
    for i in range(n):
        j = back * (n - 1 - i) + (1 - back) * i
        enter[j] = acc.astype(BF16)
        acc = acc * jnp.exp(logs[j][0:1, :]) + got[j].astype(F32)
    out_ref[me] = enter[me]
    for k in range(1, n):
        copy(enter, out_ref, e_out, e_in, k, (me + k) % n, me).start()
    for k in range(1, n):
        here = (me + n - k) % n
        copy(enter, out_ref, e_out, e_in, k, here, here).wait_recv()
    for k in range(1, n):
        there = (me + k) % n
        copy(s_ref, got, s_out, s_in, k, there, me).wait_send()
        copy(l_ref, logs, l_out, l_in, k, there, me).wait_send()
        copy(enter, out_ref, e_out, e_in, k, there, me).wait_send()


def exchange_states(states, span_log):
    n, share, _ = states.shape
    assert HEAD_DIM % share == 0
    tables = jnp.repeat(span_log.reshape(-1), HEAD_DIM // share)
    tables = jnp.broadcast_to(tables[:, None, None], (n, 8, STATE))
    return pl.pallas_call(
        functools.partial(exchange_kernel, n, share),
        out_shape=jax.ShapeDtypeStruct(states.shape, BF16),
        in_specs=[pl.BlockSpec(memory_space=pltpu.VMEM)] * 2,
        out_specs=pl.BlockSpec(memory_space=pltpu.VMEM),
        scratch_shapes=[
            pltpu.VMEM(states.shape, BF16),
            pltpu.VMEM(tables.shape, F32),
            pltpu.VMEM(states.shape, BF16),
        ]
        + [pltpu.SemaphoreType.DMA((n,))] * 6,
        compiler_params=pltpu.CompilerParams(collective_id=1, has_side_effects=True),
        cost_estimate=pl.CostEstimate(flops=0, bytes_accessed=2**25, transcendentals=0),
    )(states, tables)


def ring_spot(n):
    chips = n // 2
    me = lax.axis_index("sp")
    core, chip = me % 2, me // 2
    odd = chip % 2
    spot = (1 - odd) * (chip // 2) + odd * (chips - 1 - chip // 2)

    def device(position):
        position = (position + 2 * chips) % chips
        half = (chips + 1) // 2
        late = position // half
        late_chip = 2 * (chips - 1 - position) + 1
        return 2 * ((1 - late) * 2 * position + late * late_chip) + core

    return me, core, spot, device


def send_to(src, dst, out_sem, in_sem, target):
    return pltpu.make_async_remote_copy(
        src_ref=src,
        dst_ref=dst,
        send_sem=out_sem,
        recv_sem=in_sem,
        device_id=target,
        device_id_type=pl.DeviceIdType.MESH,
    )


def softplus(v):
    return jnp.maximum(v, 0.0) + jnp.log1p(jnp.exp(-jnp.abs(v)))


def front_kernel(
    n, x_ref, gain_ref, conv_ref, rec_ref, lat_ref, step_ref, rate_ref, spike_ref,
    proj_ref, table_ref,
    w_buf, raw, normed, acc, own_sems, x_own, x_send, x_recv,
    ring_send, ring_recv, mate_send, mate_recv,
):
    chips = n // 2
    me, core, spot, device = ring_spot(n)
    tp_me = lax.axis_index("tp")
    mate = me + 1 - 2 * core
    ways = (device(spot + 1), device(spot - 1))
    own_rows, width = x_ref.shape
    depth = w_buf.shape[0] // n
    length = 2 * own_rows
    piece = w_buf.shape[1] // (2 * CHUNKS)

    offset, own = 0, []
    for ref in (conv_ref, rec_ref, lat_ref):
        for i in range(ref.shape[0]):
            cols = ref.shape[2]
            own.append(
                pltpu.make_async_copy(
                    ref.at[i],
                    w_buf.at[pl.ds(pl.multiple_of(me * depth, depth), depth), pl.ds(offset, cols)],
                    own_sems.at[len(own)],
                )
            )
            offset += cols
    for copy in own:
        copy.start()

    up, down = (me + 1) % n, (me + n - 1) % n
    barrier = pltpu.get_barrier_semaphore()
    greeted = [{"sp": other} for other in (mate,) + ways] + [{"tp": 1 - tp_me}]
    greeted += [{"sp": other, "tp": t} for other in (up, down) for t in range(2)]
    for other in greeted:
        pl.semaphore_signal(
            barrier, inc=1, device_id=other, device_id_type=pl.DeviceIdType.MESH
        )
    pl.semaphore_wait(barrier, len(greeted))

    def rows_of(owner):
        return pl.ds(pl.multiple_of(owner * depth, depth), depth)

    def cols_of(way, chunk):
        return pl.ds((way * CHUNKS + chunk) * piece, piece)

    def owner_of(step, way):
        return device(spot - step if way == 0 else spot + step)

    def ring_copy(step, way, chunk, shift=0):
        part = w_buf.at[rows_of(owner_of(step + shift, way)), cols_of(way, chunk)]
        at = (step, way, chunk)
        return send_to(part, part, ring_send.at[at], ring_recv.at[at], {"sp": ways[way]})

    def mate_copy(step, way, chunk, incoming=False):
        owner = owner_of(step, way)
        if incoming:
            owner = owner + 1 - 2 * core
        part = w_buf.at[rows_of(owner), cols_of(way, chunk)]
        at = (step, way, chunk)
        return send_to(part, part, mate_send.at[at], mate_recv.at[at], {"sp": mate})

    parts = [(way, chunk) for chunk in range(CHUNKS) for way in range(2)]
    for copy in own:
        copy.wait()
    for way, chunk in parts:
        ring_copy(0, way, chunk).start()
    for way, chunk in parts:
        mate_copy(0, way, chunk).start()

    mine = pl.ds(pl.multiple_of(HALO + own_rows * tp_me, HALO), own_rows)
    across = send_to(x_ref, raw.at[mine], x_send.at[0], x_recv.at[0], {"tp": 1 - tp_me})
    across.start()
    here = pltpu.make_async_copy(x_ref, raw.at[mine], x_own)
    here.start()
    before, after = pl.ds(0, HALO), pl.ds(HALO + length, HALO)

    def halo(t, low):
        if low:
            return send_to(
                x_ref.at[pl.ds(own_rows - HALO, HALO)], raw.at[before],
                x_send.at[1 + t], x_recv.at[1], {"sp": up, "tp": t},
            )
        return send_to(
            x_ref.at[pl.ds(0, HALO)], raw.at[after],
            x_send.at[1 + t], x_recv.at[2], {"sp": down, "tp": t},
        )

    sends_up = jnp.logical_and(tp_me == 1, me < n - 1)
    sends_down = jnp.logical_and(tp_me == 0, me > 0)

    @pl.when(sends_up)
    def _():
        for t in range(2):
            halo(t, True).start()

    @pl.when(sends_down)
    def _():
        for t in range(2):
            halo(t, False).start()

    @pl.when(me == 0)
    def _():
        raw[0:HALO, :] = jnp.zeros((HALO, width), BF16)

    @pl.when(me == n - 1)
    def _():
        raw[HALO + length :, :] = jnp.zeros((HALO, width), BF16)

    here.wait()
    across.wait()

    @pl.when(me > 0)
    def _():
        halo(0, True).wait_recv()

    @pl.when(me < n - 1)
    def _():
        halo(0, False).wait_recv()

    @pl.when(sends_up)
    def _():
        for t in range(2):
            halo(t, True).wait_send()

    @pl.when(sends_down)
    def _():
        for t in range(2):
            halo(t, False).wait_send()

    gain = gain_ref[...].astype(F32)
    tall = 2 * HALO

    def norm_block(i, _):
        at = pl.ds(pl.multiple_of(i * tall, tall), tall)
        x32 = raw[at, :].astype(F32)
        scale = lax.rsqrt(jnp.mean(x32 * x32, axis=-1, keepdims=True) + epsilon)
        normed[at, :] = (x32 * scale * gain).astype(BF16)
        return 0

    lax.fori_loop(0, raw.shape[0] // tall, norm_block, 0)

    def dot_part(step, way, chunk, first=False):
        start = pl.multiple_of((owner_of(step, way) - core) * depth, 2 * depth)
        span = pl.ds(start, 2 * depth)
        cols = cols_of(way, chunk)
        value = jnp.dot(normed[:, span], w_buf[span, cols], preferred_element_type=F32)
        if first:
            acc[:, cols] = value
        else:
            acc[:, cols] += value

    def forward(step, way, chunk):
        ring_copy(step, way, chunk, 1).wait_recv()

        @pl.when(step < chips - 2)
        def _():
            ring_copy(step + 1, way, chunk).start()

        mate_copy(step + 1, way, chunk).start()

    for way, chunk in parts:
        forward(0, way, chunk)
    for way, chunk in parts:
        mate_copy(0, way, chunk, True).wait_recv()
        dot_part(0, way, chunk, True)

    heads = spike_ref.shape[1]
    raw_step = jnp.dot(
        normed[HALO : HALO + length, :], step_ref[...], preferred_element_type=F32
    ).astype(BF16)
    row = lax.broadcasted_iota(jnp.int32, (2 * heads, 4 * heads), 0)
    col = lax.broadcasted_iota(jnp.int32, (2 * heads, 4 * heads), 1)
    pick = jnp.where((row % heads == col // 4) & (row // heads == col % 2), 1.0, 0.0)
    head_row = lax.broadcasted_iota(jnp.int32, (heads, 4 * heads), 0)
    head_col = lax.broadcasted_iota(jnp.int32, (heads, 4 * heads), 1)
    spread = jnp.where(head_row == head_col // 4, 1.0, 0.0).astype(F32)
    deltas = softplus(jnp.dot(raw_step, pick.astype(BF16), preferred_element_type=F32))
    rates = jnp.dot(rate_ref[...], spread, precision=HIGHEST, preferred_element_type=F32)
    side = lax.broadcasted_iota(jnp.int32, (2, 4 * heads), 0)
    kind2 = lax.broadcasted_iota(jnp.int32, (2, 4 * heads), 1) % 2
    rates = jnp.sum(jnp.where(side == kind2, rates, 0.0), axis=0, keepdims=True)
    spikes = jnp.dot(spike_ref[...], spread, precision=HIGHEST, preferred_element_type=F32)
    logs = spikes - deltas * rates
    t_at = lax.broadcasted_iota(jnp.int32, (length, length), 0)
    s_at = lax.broadcasted_iota(jnp.int32, (length, length), 1)
    tri = jnp.where(t_at >= s_at, 1.0, 0.0).astype(F32)
    run_f = jnp.dot(tri, logs, precision=HIGHEST, preferred_element_type=F32)
    tri = jnp.where(t_at <= s_at, 1.0, 0.0).astype(F32)
    run_b = jnp.dot(tri, logs, precision=HIGHEST, preferred_element_type=F32)
    kind = lax.broadcasted_iota(jnp.int32, (length, 4 * heads), 1) % 4
    table_ref[...] = jnp.where(kind < 2, deltas, jnp.where(kind == 2, run_f, run_b))

    def ring_step(step, _):
        for way, chunk in parts:
            forward(step, way, chunk)
            mate_copy(step, way, chunk, True).wait_recv()
            dot_part(step, way, chunk)
        return 0

    lax.fori_loop(1, chips - 1, ring_step, 0)
    for way, chunk in parts:
        mate_copy(chips - 1, way, chunk, True).wait_recv()
        dot_part(chips - 1, way, chunk)
        cols = cols_of(way, chunk)
        proj_ref[:, cols] = acc[:, cols].astype(BF16)

    def drain(step, _):
        for way, chunk in parts:
            @pl.when(step < chips - 1)
            def _():
                ring_copy(step, way, chunk).wait_send()

            mate_copy(step, way, chunk).wait_send()
        return 0

    lax.fori_loop(0, chips, drain, 0)


def front(rows, gain, conv_w, rec_w, lat_w, step_w, rate, spike):
    n = lax.axis_size("sp")
    chips = n // 2
    own_rows, width = rows.shape
    length = 2 * own_rows
    full = length + 2 * HALO
    depth = conv_w.shape[1]
    cols = sum(w.shape[0] * w.shape[2] for w in (conv_w, rec_w, lat_w))
    blocks = sum(w.shape[0] for w in (conv_w, rec_w, lat_w))
    heads = spike.shape[1]
    vmem = pl.BlockSpec(memory_space=pltpu.VMEM)
    hbm = pl.BlockSpec(memory_space=pl.ANY)
    return pl.pallas_call(
        functools.partial(front_kernel, n),
        out_shape=[
            jax.ShapeDtypeStruct((full, cols), BF16),
            jax.ShapeDtypeStruct((length, 4 * heads), F32),
        ],
        in_specs=[vmem, vmem, hbm, hbm, hbm, vmem, vmem, vmem],
        out_specs=[vmem, vmem],
        scratch_shapes=[
            pltpu.VMEM((n * depth, cols), BF16),
            pltpu.VMEM((full, width), BF16),
            pltpu.VMEM((full, width), BF16),
            pltpu.VMEM((full, cols), F32),
            pltpu.SemaphoreType.DMA((blocks,)),
            pltpu.SemaphoreType.DMA,
            pltpu.SemaphoreType.DMA((3,)),
            pltpu.SemaphoreType.DMA((3,)),
            pltpu.SemaphoreType.DMA((chips - 1, 2, CHUNKS)),
            pltpu.SemaphoreType.DMA((chips - 1, 2, CHUNKS)),
            pltpu.SemaphoreType.DMA((chips, 2, CHUNKS)),
            pltpu.SemaphoreType.DMA((chips, 2, CHUNKS)),
        ],
        compiler_params=pltpu.CompilerParams(
            collective_id=2, has_side_effects=True, vmem_limit_bytes=56 * 2**20
        ),
        cost_estimate=pl.CostEstimate(
            flops=2 * full * width * cols, bytes_accessed=2 * width * cols, transcendentals=0
        ),
    )(rows, gain.reshape(1, -1), conv_w, rec_w, lat_w, step_w, rate, spike)


def exit_ring(n, c_ref, s_ref, c_out, s_out, own_sems, sems):
    chips = n // 2
    me, core, spot, device = ring_spot(n)
    mate = me + 1 - 2 * core
    ways = (device(spot + 1), device(spot - 1))
    ring_send, ring_recv, mate_send, mate_recv = sems
    refs, outs = (c_ref, s_ref), (c_out, s_out)
    rows, wide = c_ref.shape
    tall = rows // CHUNKS

    def spot_in(owner, way, chunk):
        cols = pl.ds(pl.multiple_of(owner * wide, wide), wide)
        return outs[way].at[pl.ds(chunk * tall, tall), cols]

    def owner_of(step, way):
        return device(spot - step if way == 0 else spot + step)

    def source(step, way, chunk):
        if step == 0:
            return refs[way].at[pl.ds(chunk * tall, tall)]
        return spot_in(owner_of(step, way), way, chunk)

    def ring_copy(step, way, chunk):
        at = (step, way, chunk)
        return send_to(
            source(step, way, chunk), spot_in(owner_of(step, way), way, chunk),
            ring_send.at[at], ring_recv.at[at], {"sp": ways[way]},
        )

    def arrival(step, way, chunk):
        part = spot_in(owner_of(step + 1, way), way, chunk)
        at = (step, way, chunk)
        return send_to(part, part, ring_send.at[at], ring_recv.at[at], {"sp": ways[way]})

    def mate_copy(step, way, chunk, incoming=False):
        owner = owner_of(step, way)
        at = (step, way, chunk)
        there = spot_in(owner + 1 - 2 * core if incoming else owner, way, chunk)
        src = there if incoming else source(step, way, chunk)
        return send_to(src, there, mate_send.at[at], mate_recv.at[at], {"sp": mate})

    parts = [(way, chunk) for chunk in range(CHUNKS) for way in range(2)]
    cols = pl.ds(pl.multiple_of(me * wide, wide), wide)
    own = [
        pltpu.make_async_copy(refs[way], outs[way].at[:, cols], own_sems.at[way])
        for way in range(2)
    ]

    def start():
        for way, chunk in parts:
            ring_copy(0, way, chunk).start()
        for way, chunk in parts:
            mate_copy(0, way, chunk).start()
        for copy in own:
            copy.start()

    def advance(step):
        for way, chunk in parts:
            arrival(step, way, chunk).wait_recv()
            if step < chips - 2:
                ring_copy(step + 1, way, chunk).start()
            mate_copy(step + 1, way, chunk).start()

    def finish():
        for copy in own:
            copy.wait()
        for step in range(chips):
            for way, chunk in parts:
                if step < chips - 1:
                    ring_copy(step, way, chunk).wait_send()
                mate_copy(step, way, chunk).wait_send()
                mate_copy(step, way, chunk, True).wait_recv()

    return chips, start, advance, finish


def exchange_exit_kernel(
    n, share, s_ref, l_ref, c_ref, x_ref, out_ref, c_out, x_out,
    got, logs, enter, s_sem, s_in, l_out, l_in, e_out, e_in,
    own_sems, ring_send, ring_recv, mate_send, mate_recv,
):
    me = lax.axis_index("sp")
    barrier = pltpu.get_barrier_semaphore()
    for k in range(1, n):
        pl.semaphore_signal(
            barrier,
            inc=1,
            device_id={"sp": (me + k) % n},
            device_id_type=pl.DeviceIdType.MESH,
        )
    pl.semaphore_wait(barrier, n - 1)
    chips, start, advance, finish = exit_ring(
        n, c_ref, x_ref, c_out, x_out, own_sems, (ring_send, ring_recv, mate_send, mate_recv)
    )

    def copy(src, dst, out_sem, in_sem, k, there, slot):
        return send_to(
            src.at[there], dst.at[slot], out_sem.at[k], in_sem.at[k], {"sp": there}
        )

    for k in range(1, n):
        there = (me + k) % n
        copy(s_ref, got, s_sem, s_in, k, there, me).start()
        copy(l_ref, logs, l_out, l_in, k, there, me).start()
    start()
    got[me] = s_ref[me]
    logs[me] = l_ref[me]
    advance(0)
    advance(1)
    for k in range(1, n):
        here = (me + n - k) % n
        copy(s_ref, got, s_sem, s_in, k, here, here).wait_recv()
        copy(l_ref, logs, l_out, l_in, k, here, here).wait_recv()
    back = (me * share // HEAD_DIM) % 2
    acc = jnp.zeros(s_ref.shape[1:], F32)
    for i in range(n):
        j = back * (n - 1 - i) + (1 - back) * i
        enter[j] = acc.astype(BF16)
        acc = acc * jnp.exp(logs[j][0:1, :]) + got[j].astype(F32)
    out_ref[me] = enter[me]
    for k in range(1, n):
        copy(enter, out_ref, e_out, e_in, k, (me + k) % n, me).start()
    for step in range(2, chips - 1):
        advance(step)
    for k in range(1, n):
        here = (me + n - k) % n
        copy(enter, out_ref, e_out, e_in, k, here, here).wait_recv()
    for k in range(1, n):
        there = (me + k) % n
        copy(s_ref, got, s_sem, s_in, k, there, me).wait_send()
        copy(l_ref, logs, l_out, l_in, k, there, me).wait_send()
        copy(enter, out_ref, e_out, e_in, k, there, me).wait_send()
    finish()


def exchange_exit(states, span_log, exit_c, exit_s):
    n, share, _ = states.shape
    chips = n // 2
    assert HEAD_DIM % share == 0
    tables = jnp.repeat(span_log.reshape(-1), HEAD_DIM // share)
    tables = jnp.broadcast_to(tables[:, None, None], (n, 8, STATE))
    wide = (exit_c.shape[0], exit_c.shape[1] * n)
    vmem = pl.BlockSpec(memory_space=pltpu.VMEM)
    return pl.pallas_call(
        functools.partial(exchange_exit_kernel, n, share),
        out_shape=[
            jax.ShapeDtypeStruct(states.shape, BF16),
            jax.ShapeDtypeStruct(wide, BF16),
            jax.ShapeDtypeStruct(wide, BF16),
        ],
        in_specs=[vmem] * 4,
        out_specs=[vmem] * 3,
        scratch_shapes=[
            pltpu.VMEM(states.shape, BF16),
            pltpu.VMEM(tables.shape, F32),
            pltpu.VMEM(states.shape, BF16),
        ]
        + [pltpu.SemaphoreType.DMA((n,))] * 6
        + [pltpu.SemaphoreType.DMA((2,))]
        + [pltpu.SemaphoreType.DMA((chips - 1, 2, CHUNKS))] * 2
        + [pltpu.SemaphoreType.DMA((chips, 2, CHUNKS))] * 2,
        compiler_params=pltpu.CompilerParams(collective_id=3, has_side_effects=True),
        cost_estimate=pl.CostEstimate(flops=0, bytes_accessed=2**25, transcendentals=0),
    )(states, tables, exit_c, exit_s)


def project_kernel(r_ref, w_ref, o_ref):
    o_ref[...] = jnp.dot(r_ref[...], w_ref[...], preferred_element_type=F32).astype(BF16)


def project(rows, weights):
    count, width = rows.shape
    cols = weights.shape[1]
    tile = cols // 9
    return pl.pallas_call(
        project_kernel,
        grid=(9,),
        in_specs=[
            pl.BlockSpec((count, width), lambda j: (0, 0)),
            pl.BlockSpec((width, tile), lambda j: (0, j)),
        ],
        out_specs=pl.BlockSpec((count, tile), lambda j: (0, j)),
        out_shape=jax.ShapeDtypeStruct((count, cols), BF16),
        cost_estimate=pl.CostEstimate(
            flops=2 * count * width * cols, bytes_accessed=2 * width * cols, transcendentals=0
        ),
    )(rows, weights)


def finish_kernel(within_ref, reads_ref, enter_ref, gate_ref, gain_ref, col_ref, y_ref):
    length = y_ref.shape[0]
    cols = col_ref[0]
    outs = []
    for h in range(2):
        o = 4 * h
        both = lax.dot_general(
            reads_ref[:, h * STATE : (h + 1) * STATE],
            enter_ref[h * STATE : (h + 1) * STATE],
            (((1,), (1,)), ((), ())),
            preferred_element_type=F32,
        )
        here = slice(h * HEAD_DIM, (h + 1) * HEAD_DIM)
        y = within_ref[:, here]
        y = y + both[:, :HEAD_DIM] * jnp.exp(cols[:, o + 2 : o + 3])
        y = y + both[:, HEAD_DIM:] * jnp.exp(cols[:, o + 3 : o + 4])
        g = y * silu(gate_ref[pl.ds(HALO, length), :].astype(F32)[:, here])
        g = g * lax.rsqrt(jnp.mean(g * g, axis=-1, keepdims=True) + epsilon)
        outs.append(g * gain_ref[:, here].astype(F32))
    y_ref[...] = jnp.concatenate(outs, axis=1).astype(BF16)


def local(
    layer_source_rows, entry_rescale_factor, sliding_mixer_entry_matrix,
    recurrent_mixer_entry_matrix, latent_write_read_matrix, timestep_matrix,
    sliding_kernel_coefficients, recurrent_kernel_coefficients, latent_kernel_coefficients,
    lane_forgetting_rate, spike_forgetting_rate, lane_rescale_factor,
    sliding_mixer_exit_matrix, recurrent_mixer_exit_matrix,
):
    n = lax.axis_size("sp")
    tp = lax.axis_size("tp")
    own_rows, width = layer_source_rows.shape
    length = own_rows * tp
    full = length + 2 * HALO
    conv_width = sliding_mixer_entry_matrix.shape[2]
    ssd_width = recurrent_mixer_entry_matrix.shape[2]
    state_width = latent_write_read_matrix.shape[2]
    heads = timestep_matrix.shape[2]
    pairs = heads // 2
    cw = conv_width // pairs

    share = heads * 2 * HEAD_DIM // n
    ringed = tp == 2
    if ringed:
        proj, table = front(
            layer_source_rows, entry_rescale_factor, sliding_mixer_entry_matrix,
            recurrent_mixer_entry_matrix, latent_write_read_matrix,
            timestep_matrix.reshape(width, 2 * heads), lane_forgetting_rate,
            spike_forgetting_rate,
        )
        col_table = table.reshape(length, pairs, 8).transpose(1, 0, 2)
        row_table = table.T.reshape(pairs, 8, length)
        ends = table.reshape(length, heads, 4)
        span_log = jnp.stack([ends[length - 1, :, 2], ends[0, :, 3]], axis=1)
    else:
        block = jnp.concatenate(
            [sliding_mixer_entry_matrix[i] for i in range(3)]
            + [recurrent_mixer_entry_matrix[i] for i in range(2)]
            + [latent_write_read_matrix[i] for i in range(2)],
            axis=1,
        )
        gathered = gather_rows(block)
        weights = gathered.reshape(n * block.shape[0], block.shape[1])

        x32 = layer_source_rows.astype(F32)
        normed = (
            x32
            * lax.rsqrt(jnp.mean(x32 * x32, axis=-1, keepdims=True) + epsilon)
            * entry_rescale_factor.astype(F32)
        ).astype(BF16)
        up = [(i, i + 1) for i in range(n - 1)]
        down = [(i + 1, i) for i in range(n - 1)]
        before = lax.ppermute(normed[own_rows - HALO :], "sp", up)
        after = lax.ppermute(normed[:HALO], "sp", down)
        shared = lax.all_gather(jnp.concatenate([before, normed, after], axis=0), "tp", axis=0)
        rows = jnp.concatenate(
            [shared[tp - 1, :HALO]]
            + [shared[i, HALO : HALO + own_rows] for i in range(tp)]
            + [shared[0, HALO + own_rows :]],
            axis=0,
        )

        step_weight = timestep_matrix.reshape(width, 2 * heads)
        raw = jnp.dot(rows, step_weight, preferred_element_type=F32).astype(BF16)
        raw = raw[HALO : HALO + length].astype(F32).reshape(length, 2, heads)
        deltas = jax.nn.softplus(raw)
        logs = -deltas * lane_forgetting_rate[None] + spike_forgetting_rate[:, None, :]
        tri = (jnp.arange(length)[:, None] >= jnp.arange(length)[None, :]).astype(F32)
        run_f = jnp.dot(tri, logs[:, 0], precision=HIGHEST)
        run_b = jnp.dot(tri.T, logs[:, 1], precision=HIGHEST)
        table = jnp.stack([deltas[:, 0], deltas[:, 1], run_f, run_b], axis=2)
        col_table = table.reshape(length, pairs, 8).transpose(1, 0, 2)
        row_table = table.reshape(length, pairs, 8).transpose(1, 2, 0)
        span_log = jnp.stack([run_f[length - 1], run_b[0]], axis=1)
        exit_c, exit_s, weights = lax.optimization_barrier(
            (sliding_mixer_exit_matrix, recurrent_mixer_exit_matrix, weights)
        )
        proj = project(rows, weights)
        exit_c = lax.all_gather(exit_c, "sp", axis=1, tiled=True)
        exit_s = lax.all_gather(exit_s, "sp", axis=1, tiled=True)

    latent = latent_kernel_coefficients
    pw, sw = 2 * HEAD_DIM, 2 * STATE
    g0 = 3 * conv_width
    at_gate, at_x = g0 // pw, (g0 + ssd_width) // pw
    at_b = (g0 + 2 * ssd_width) // sw
    at_c = at_b + pairs
    y_conv, within, reads, states = pl.pallas_call(
        mix_kernel,
        grid=(pairs,),
        in_specs=[
            pl.BlockSpec((full, cw), lambda j: (0, j)),
            pl.BlockSpec((full, cw), lambda j: (0, pairs + j)),
            pl.BlockSpec((full, cw), lambda j: (0, 2 * pairs + j)),
            pl.BlockSpec((full, pw), lambda j: (0, at_x + j)),
            pl.BlockSpec((full, sw), lambda j: (0, at_b + j)),
            pl.BlockSpec((full, sw), lambda j: (0, at_c + j)),
            pl.BlockSpec((3, cw), lambda j: (0, j)),
            pl.BlockSpec((5, pw), lambda j: (0, j)),
            pl.BlockSpec((5, sw), lambda j: (0, j)),
            pl.BlockSpec((5, sw), lambda j: (0, pairs + j)),
            pl.BlockSpec((1, length, 8), lambda j: (j, 0, 0)),
            pl.BlockSpec((1, 8, length), lambda j: (j, 0, 0)),
        ],
        out_specs=[
            pl.BlockSpec((length, cw), lambda j: (0, j)),
            pl.BlockSpec((length, pw), lambda j: (0, j)),
            pl.BlockSpec((length, sw), lambda j: (0, j)),
            pl.BlockSpec((sw, STATE), lambda j: (j, 0)),
        ],
        out_shape=[
            jax.ShapeDtypeStruct((length, conv_width), BF16),
            jax.ShapeDtypeStruct((length, ssd_width), F32),
            jax.ShapeDtypeStruct((length, state_width), BF16),
            jax.ShapeDtypeStruct((pairs * sw, STATE), BF16),
        ],
        cost_estimate=pl.CostEstimate(
            flops=8 * length * length * heads * STATE, bytes_accessed=2**24, transcendentals=0
        ),
    )(
        proj, proj, proj, proj, proj, proj,
        sliding_kernel_coefficients, recurrent_kernel_coefficients,
        latent.reshape(latent.shape[0], -1), latent.reshape(latent.shape[0], -1),
        col_table, row_table,
    )

    states = states.reshape(n, share, STATE)
    if ringed:
        entering, exit_c, exit_s = exchange_exit(
            states, span_log, sliding_mixer_exit_matrix, recurrent_mixer_exit_matrix
        )
    else:
        entering = exchange_states(states, span_log)
    entering = entering.reshape(pairs * sw, STATE)

    y_ssd = pl.pallas_call(
        finish_kernel,
        grid=(pairs,),
        in_specs=[
            pl.BlockSpec((length, pw), lambda j: (0, j)),
            pl.BlockSpec((length, sw), lambda j: (0, j)),
            pl.BlockSpec((sw, STATE), lambda j: (j, 0)),
            pl.BlockSpec((full, pw), lambda j: (0, at_gate + j)),
            pl.BlockSpec((1, pw), lambda j: (0, j)),
            pl.BlockSpec((1, length, 8), lambda j: (j, 0, 0)),
        ],
        out_specs=pl.BlockSpec((length, pw), lambda j: (0, j)),
        out_shape=jax.ShapeDtypeStruct((length, ssd_width), BF16),
    )(within, reads, entering, proj, lane_rescale_factor.reshape(1, -1), col_table)

    def partial(y_c, y_s):
        return (
            jnp.dot(y_c, exit_c, preferred_element_type=F32)
            + jnp.dot(y_s, exit_s, preferred_element_type=F32)
        ).astype(BF16)

    if tp != 2:
        return lax.psum_scatter(
            partial(y_conv, y_ssd), "tp", scatter_dimension=0, tiled=True
        )
    tp_me = lax.axis_index("tp")

    def rows_of(owner, y):
        return lax.dynamic_slice_in_dim(y, owner * own_rows, own_rows, axis=0)

    away = partial(rows_of(1 - tp_me, y_conv), rows_of(1 - tp_me, y_ssd))
    arrived = lax.ppermute(away, "tp", [(0, 1), (1, 0)])
    kept = partial(rows_of(tp_me, y_conv), rows_of(tp_me, y_ssd))
    return (kept.astype(F32) + arrived.astype(F32)).astype(BF16)


def solution(mesh):
    placed = (
        P(("sp", "tp"), None),
        P(),
        P(None, "sp", "tp"),
        P(None, "sp", "tp"),
        P(None, "sp", "tp"),
        P(None, None, "tp"),
        P(None, "tp"),
        P(None, "tp"),
        P(None, None, "tp"),
        P(None, "tp"),
        P("sp", "tp"),
        P("tp"),
        P("tp", "sp"),
        P("tp", "sp"),
    )
    return jax.shard_map(
        local, mesh=mesh, in_specs=placed, out_specs=P(("sp", "tp"), None), check_vma=False
    )
```

```python
import functools

import jax
import jax.numpy as jnp
from jax import lax
from jax.experimental import pallas as pl
from jax.experimental.pallas import tpu as pltpu
from jax.sharding import PartitionSpec as P

HEAD_DIM = 64
STATE = 128
HALO = 16
CHUNKS = 2
EARLY = 2
BLOCKS = 4
epsilon = 1e-05
F32 = jnp.float32
BF16 = jnp.bfloat16
HIGHEST = lax.Precision.HIGHEST


def ring_kernel(n, w_ref, out_ref, own_sem, ring_send, ring_recv, mate_send, mate_recv):
    chips = n // 2
    me = lax.axis_index("sp")
    core, chip = me % 2, me // 2
    odd = chip % 2
    spot = (1 - odd) * (chip // 2) + odd * (chips - 1 - chip // 2)

    def device(position):
        position = (position + 2 * chips) % chips
        half = (chips + 1) // 2
        late = position // half
        late_chip = 2 * (chips - 1 - position) + 1
        return 2 * ((1 - late) * 2 * position + late * late_chip) + core

    mate = me + 1 - 2 * core
    ways = (device(spot + 1), device(spot - 1))
    rows = w_ref.shape[0] // (2 * CHUNKS)

    barrier = pltpu.get_barrier_semaphore()
    for other in (mate,) + ways:
        pl.semaphore_signal(
            barrier, inc=1, device_id={"sp": other}, device_id_type=pl.DeviceIdType.MESH
        )
    pl.semaphore_wait(barrier, 3)

    def piece(way, chunk):
        return pl.ds((way * CHUNKS + chunk) * rows, rows)

    def ring_copy(step, way, chunk):
        owner = device(spot - step if way == 0 else spot + step)
        part = piece(way, chunk)
        return pltpu.make_async_remote_copy(
            src_ref=w_ref.at[part] if step == 0 else out_ref.at[owner, part],
            dst_ref=out_ref.at[owner, part],
            send_sem=ring_send.at[step, way, chunk],
            recv_sem=ring_recv.at[step, way, chunk],
            device_id={"sp": ways[way]},
            device_id_type=pl.DeviceIdType.MESH,
        )

    def arrival(step, way, chunk):
        owner = device(spot - step - 1 if way == 0 else spot + step + 1)
        part = piece(way, chunk)
        return pltpu.make_async_remote_copy(
            src_ref=out_ref.at[owner, part],
            dst_ref=out_ref.at[owner, part],
            send_sem=ring_send.at[step, way, chunk],
            recv_sem=ring_recv.at[step, way, chunk],
            device_id={"sp": ways[way]},
            device_id_type=pl.DeviceIdType.MESH,
        )

    def mate_copy(step, way, chunk, incoming=False):
        owner = device(spot - step if way == 0 else spot + step)
        if incoming:
            owner = owner + 1 - 2 * core
        part = piece(way, chunk)
        return pltpu.make_async_remote_copy(
            src_ref=w_ref.at[part] if step == 0 else out_ref.at[owner, part],
            dst_ref=out_ref.at[owner, part],
            send_sem=mate_send.at[step, way, chunk],
            recv_sem=mate_recv.at[step, way, chunk],
            device_id={"sp": mate},
            device_id_type=pl.DeviceIdType.MESH,
        )

    parts = [(way, chunk) for chunk in range(CHUNKS) for way in range(2)]
    for way, chunk in parts:
        ring_copy(0, way, chunk).start()
    for way, chunk in parts:
        mate_copy(0, way, chunk).start()
    own = pltpu.make_async_copy(w_ref, out_ref.at[me], own_sem)
    own.start()
    for step in range(chips - 1):
        for way, chunk in parts:
            arrival(step, way, chunk).wait_recv()
            if step < chips - 2:
                ring_copy(step + 1, way, chunk).start()
            mate_copy(step + 1, way, chunk).start()
    own.wait()
    for step in range(chips):
        for way, chunk in parts:
            if step < chips - 1:
                ring_copy(step, way, chunk).wait_send()
            mate_copy(step, way, chunk).wait_send()
            mate_copy(step, way, chunk, True).wait_recv()


def gather_rows(block):
    n = lax.axis_size("sp")
    chips = n // 2
    rows, cols = block.shape
    return pl.pallas_call(
        functools.partial(ring_kernel, n),
        out_shape=jax.ShapeDtypeStruct((n, rows, cols), block.dtype),
        in_specs=[pl.BlockSpec(memory_space=pltpu.VMEM)],
        out_specs=pl.BlockSpec(memory_space=pl.ANY),
        scratch_shapes=[
            pltpu.SemaphoreType.DMA,
            pltpu.SemaphoreType.DMA((chips - 1, 2, CHUNKS)),
            pltpu.SemaphoreType.DMA((chips - 1, 2, CHUNKS)),
            pltpu.SemaphoreType.DMA((chips, 2, CHUNKS)),
            pltpu.SemaphoreType.DMA((chips, 2, CHUNKS)),
        ],
        compiler_params=pltpu.CompilerParams(
            collective_id=0, has_side_effects=True, vmem_limit_bytes=16 * 2**20
        ),
        cost_estimate=pl.CostEstimate(
            flops=0, bytes_accessed=n * rows * cols * 16, transcendentals=0
        ),
    )(block)


def taps_of(padded, table, length):
    full = padded.shape[0]
    half = table.shape[0] // 2
    total = None
    for k in range(table.shape[0]):
        moved = padded if k == half else pltpu.roll(padded, (half - k) % full, 0)
        term = moved[HALO : HALO + length] * table[k : k + 1].astype(F32)
        total = term if total is None else total + term
    return total


def silu(v):
    return v * jax.nn.sigmoid(v)


def mix_kernel(
    og_ref, ig_ref, va_ref, x_ref, b_ref, c_ref, ct_ref, xt_ref, bt_ref, rt_ref,
    col_ref, row_ref, yconv_ref, within_ref, reads_ref, state_ref,
):
    length = yconv_ref.shape[0]
    gated = (ig_ref[...].astype(F32) * va_ref[...].astype(F32)).astype(BF16).astype(F32)
    conv = taps_of(gated, ct_ref[...], length)
    yconv_ref[...] = (og_ref[pl.ds(HALO, length), :].astype(F32) * conv).astype(BF16)
    xs = silu(taps_of(x_ref[...].astype(F32), xt_ref[...], length)).astype(BF16)
    bs = silu(taps_of(b_ref[...].astype(F32), bt_ref[...], length)).astype(BF16)
    cs = silu(taps_of(c_ref[...].astype(F32), rt_ref[...], length)).astype(BF16)
    reads_ref[...] = cs
    cols = col_ref[0]
    rows = row_ref[0]
    t_at = lax.broadcasted_iota(jnp.int32, (length, length), 0)
    s_at = lax.broadcasted_iota(jnp.int32, (length, length), 1)
    outs, weighted = [], []
    for h in range(2):
        c_h = cs[:, h * STATE : (h + 1) * STATE]
        b_h = bs[:, h * STATE : (h + 1) * STATE]
        x_h = xs[:, h * HEAD_DIM : (h + 1) * HEAD_DIM]
        o = 4 * h
        scores = lax.dot_general(
            c_h, b_h, (((1,), (1,)), ((), ())), preferred_element_type=F32
        )
        gap = jnp.where(
            t_at >= s_at,
            cols[:, o + 2 : o + 3] - rows[o + 2 : o + 3],
            cols[:, o + 3 : o + 4] - rows[o + 3 : o + 4],
        )
        d_f, d_b = rows[o : o + 1], rows[o + 1 : o + 2]
        scale = jnp.where(t_at > s_at, d_f, jnp.where(t_at < s_at, d_b, d_f + d_b))
        w = (scores * jnp.exp(gap) * scale).astype(BF16)
        outs.append(jnp.dot(w, x_h, preferred_element_type=F32))
        x32 = x_h.astype(F32)
        end_f = jnp.exp(rows[o + 2 : o + 3, length - 1 : length] - cols[:, o + 2 : o + 3])
        end_b = jnp.exp(rows[o + 3 : o + 4, 0:1] - cols[:, o + 3 : o + 4])
        both = jnp.concatenate(
            [x32 * (end_f * cols[:, o : o + 1]), x32 * (end_b * cols[:, o + 1 : o + 2])], axis=1
        ).astype(BF16)
        state_ref[h * STATE : (h + 1) * STATE] = lax.dot_general(
            both, b_h, (((0,), (0,)), ((), ())), preferred_element_type=F32
        ).astype(BF16)
    within_ref[...] = jnp.concatenate(outs, axis=1)


def exchange_kernel(
    n, share, s_ref, l_ref, out_ref, got, logs, enter, s_out, s_in, l_out, l_in, e_out, e_in
):
    me = lax.axis_index("sp")
    barrier = pltpu.get_barrier_semaphore()
    for k in range(1, n):
        pl.semaphore_signal(
            barrier,
            inc=1,
            device_id={"sp": (me + k) % n},
            device_id_type=pl.DeviceIdType.MESH,
        )
    pl.semaphore_wait(barrier, n - 1)

    def copy(src, dst, out_sem, in_sem, k, there, slot):
        return pltpu.make_async_remote_copy(
            src_ref=src.at[there],
            dst_ref=dst.at[slot],
            send_sem=out_sem.at[k],
            recv_sem=in_sem.at[k],
            device_id={"sp": there},
            device_id_type=pl.DeviceIdType.MESH,
        )

    for k in range(1, n):
        there = (me + k) % n
        copy(s_ref, got, s_out, s_in, k, there, me).start()
        copy(l_ref, logs, l_out, l_in, k, there, me).start()
    got[me] = s_ref[me]
    logs[me] = l_ref[me]
    for k in range(1, n):
        here = (me + n - k) % n
        copy(s_ref, got, s_out, s_in, k, here, here).wait_recv()
        copy(l_ref, logs, l_out, l_in, k, here, here).wait_recv()
    back = (me * share // HEAD_DIM) % 2
    acc = jnp.zeros(s_ref.shape[1:], F32)
    for i in range(n):
        j = back * (n - 1 - i) + (1 - back) * i
        enter[j] = acc.astype(BF16)
        acc = acc * jnp.exp(logs[j][0:1, :]) + got[j].astype(F32)
    out_ref[me] = enter[me]
    for k in range(1, n):
        copy(enter, out_ref, e_out, e_in, k, (me + k) % n, me).start()
    for k in range(1, n):
        here = (me + n - k) % n
        copy(enter, out_ref, e_out, e_in, k, here, here).wait_recv()
    for k in range(1, n):
        there = (me + k) % n
        copy(s_ref, got, s_out, s_in, k, there, me).wait_send()
        copy(l_ref, logs, l_out, l_in, k, there, me).wait_send()
        copy(enter, out_ref, e_out, e_in, k, there, me).wait_send()


def exchange_states(states, span_log):
    n, share, _ = states.shape
    assert HEAD_DIM % share == 0
    tables = jnp.repeat(span_log.reshape(-1), HEAD_DIM // share)
    tables = jnp.broadcast_to(tables[:, None, None], (n, 8, STATE))
    return pl.pallas_call(
        functools.partial(exchange_kernel, n, share),
        out_shape=jax.ShapeDtypeStruct(states.shape, BF16),
        in_specs=[pl.BlockSpec(memory_space=pltpu.VMEM)] * 2,
        out_specs=pl.BlockSpec(memory_space=pltpu.VMEM),
        scratch_shapes=[
            pltpu.VMEM(states.shape, BF16),
            pltpu.VMEM(tables.shape, F32),
            pltpu.VMEM(states.shape, BF16),
        ]
        + [pltpu.SemaphoreType.DMA((n,))] * 6,
        compiler_params=pltpu.CompilerParams(collective_id=1, has_side_effects=True),
        cost_estimate=pl.CostEstimate(flops=0, bytes_accessed=2**25, transcendentals=0),
    )(states, tables)


def ring_spot(n):
    chips = n // 2
    me = lax.axis_index("sp")
    core, chip = me % 2, me // 2
    odd = chip % 2
    spot = (1 - odd) * (chip // 2) + odd * (chips - 1 - chip // 2)

    def device(position):
        position = (position + 2 * chips) % chips
        half = (chips + 1) // 2
        late = position // half
        late_chip = 2 * (chips - 1 - position) + 1
        return 2 * ((1 - late) * 2 * position + late * late_chip) + core

    return me, core, spot, device


def send_to(src, dst, out_sem, in_sem, target):
    return pltpu.make_async_remote_copy(
        src_ref=src,
        dst_ref=dst,
        send_sem=out_sem,
        recv_sem=in_sem,
        device_id=target,
        device_id_type=pl.DeviceIdType.MESH,
    )


def softplus(v):
    return jnp.maximum(v, 0.0) + jnp.log1p(jnp.exp(-jnp.abs(v)))


def front_kernel(
    n, x_ref, gain_ref, conv_ref, rec_ref, lat_ref, step_ref, rate_ref, spike_ref,
    proj_ref, table_ref, turned_ref, ends_ref,
    w_buf, raw, normed, acc, own_sems, x_own, x_send, x_recv,
    ring_send, ring_recv, mate_send, mate_recv,
):
    chips = n // 2
    me, core, spot, device = ring_spot(n)
    tp_me = lax.axis_index("tp")
    mate = me + 1 - 2 * core
    ways = (device(spot + 1), device(spot - 1))
    own_rows, width = x_ref.shape
    depth = w_buf.shape[0] // n
    length = 2 * own_rows
    piece = w_buf.shape[1] // (2 * CHUNKS)

    offset, own = 0, []
    for ref in (conv_ref, rec_ref, lat_ref):
        for i in range(ref.shape[0]):
            cols = ref.shape[2]
            own.append(
                pltpu.make_async_copy(
                    ref.at[i],
                    w_buf.at[pl.ds(pl.multiple_of(me * depth, depth), depth), pl.ds(offset, cols)],
                    own_sems.at[len(own)],
                )
            )
            offset += cols
    for copy in own:
        copy.start()

    up, down = (me + 1) % n, (me + n - 1) % n
    barrier = pltpu.get_barrier_semaphore()
    greeted = [{"sp": other} for other in (mate,) + ways] + [{"tp": 1 - tp_me}]
    greeted += [{"sp": other, "tp": t} for other in (up, down) for t in range(2)]
    for other in greeted:
        pl.semaphore_signal(
            barrier, inc=1, device_id=other, device_id_type=pl.DeviceIdType.MESH
        )
    pl.semaphore_wait(barrier, len(greeted))

    def rows_of(owner):
        return pl.ds(pl.multiple_of(owner * depth, depth), depth)

    def cols_of(way, chunk):
        return pl.ds((way * CHUNKS + chunk) * piece, piece)

    def owner_of(step, way):
        return device(spot - step if way == 0 else spot + step)

    def ring_copy(step, way, chunk, shift=0):
        part = w_buf.at[rows_of(owner_of(step + shift, way)), cols_of(way, chunk)]
        at = (step, way, chunk)
        return send_to(part, part, ring_send.at[at], ring_recv.at[at], {"sp": ways[way]})

    def mate_copy(step, way, chunk, incoming=False):
        owner = owner_of(step, way)
        if incoming:
            owner = owner + 1 - 2 * core
        part = w_buf.at[rows_of(owner), cols_of(way, chunk)]
        at = (step, way, chunk)
        return send_to(part, part, mate_send.at[at], mate_recv.at[at], {"sp": mate})

    parts = [(way, chunk) for chunk in range(CHUNKS) for way in range(2)]
    for copy in own:
        copy.wait()
    for way, chunk in parts:
        ring_copy(0, way, chunk).start()
    for way, chunk in parts:
        mate_copy(0, way, chunk).start()

    mine = pl.ds(pl.multiple_of(HALO + own_rows * tp_me, HALO), own_rows)
    across = send_to(x_ref, raw.at[mine], x_send.at[0], x_recv.at[0], {"tp": 1 - tp_me})
    across.start()
    here = pltpu.make_async_copy(x_ref, raw.at[mine], x_own)
    here.start()
    before, after = pl.ds(0, HALO), pl.ds(HALO + length, HALO)

    def halo(t, low):
        if low:
            return send_to(
                x_ref.at[pl.ds(own_rows - HALO, HALO)], raw.at[before],
                x_send.at[1 + t], x_recv.at[1], {"sp": up, "tp": t},
            )
        return send_to(
            x_ref.at[pl.ds(0, HALO)], raw.at[after],
            x_send.at[1 + t], x_recv.at[2], {"sp": down, "tp": t},
        )

    sends_up = jnp.logical_and(tp_me == 1, me < n - 1)
    sends_down = jnp.logical_and(tp_me == 0, me > 0)

    @pl.when(sends_up)
    def _():
        for t in range(2):
            halo(t, True).start()

    @pl.when(sends_down)
    def _():
        for t in range(2):
            halo(t, False).start()

    @pl.when(me == 0)
    def _():
        raw[0:HALO, :] = jnp.zeros((HALO, width), BF16)

    @pl.when(me == n - 1)
    def _():
        raw[HALO + length :, :] = jnp.zeros((HALO, width), BF16)

    def dot_part(step, way, chunk, first=False):
        start = pl.multiple_of((owner_of(step, way) - core) * depth, 2 * depth)
        span = pl.ds(start, 2 * depth)
        cols = cols_of(way, chunk)
        value = jnp.dot(normed[:, span], w_buf[span, cols], preferred_element_type=F32)
        if first:
            acc[:, cols] = value
        else:
            acc[:, cols] += value

    def forward(step, way, chunk):
        ring_copy(step, way, chunk, 1).wait_recv()

        @pl.when(step < chips - 2)
        def _():
            ring_copy(step + 1, way, chunk).start()

        mate_copy(step + 1, way, chunk).start()

    for step in range(EARLY):
        for way, chunk in parts:
            forward(step, way, chunk)
    here.wait()
    across.wait()

    @pl.when(me > 0)
    def _():
        halo(0, True).wait_recv()

    @pl.when(me < n - 1)
    def _():
        halo(0, False).wait_recv()

    @pl.when(sends_up)
    def _():
        for t in range(2):
            halo(t, True).wait_send()

    @pl.when(sends_down)
    def _():
        for t in range(2):
            halo(t, False).wait_send()

    gain = gain_ref[...].astype(F32)
    tall = 2 * HALO

    def norm_block(i, _):
        at = pl.ds(pl.multiple_of(i * tall, tall), tall)
        x32 = raw[at, :].astype(F32)
        scale = lax.rsqrt(jnp.mean(x32 * x32, axis=-1, keepdims=True) + epsilon)
        normed[at, :] = (x32 * scale * gain).astype(BF16)
        return 0

    lax.fori_loop(0, raw.shape[0] // tall, norm_block, 0)

    for way, chunk in parts:
        forward(EARLY, way, chunk)
        mate_copy(0, way, chunk, True).wait_recv()
        dot_part(0, way, chunk, True)

    heads = spike_ref.shape[0]
    raw_step = lax.dot_general(
        normed[HALO : HALO + length, :], step_ref[...],
        (((1,), (1,)), ((), ())), preferred_element_type=F32,
    ).astype(BF16)
    lanes = table_ref.shape[1]
    row = lax.broadcasted_iota(jnp.int32, (2 * heads, lanes), 0)
    col = lax.broadcasted_iota(jnp.int32, (2 * heads, lanes), 1)
    pick = jnp.where((row % heads == col // 4) & (row // heads == col % 2), 1.0, 0.0)
    head_row = lax.broadcasted_iota(jnp.int32, (heads, lanes), 0)
    head_col = lax.broadcasted_iota(jnp.int32, (heads, lanes), 1)
    spread = jnp.where(head_row == head_col // 4, 1.0, 0.0).astype(F32)
    deltas = softplus(jnp.dot(raw_step, pick.astype(BF16), preferred_element_type=F32))
    rates = jnp.dot(rate_ref[...], spread, precision=HIGHEST, preferred_element_type=F32)
    side = lax.broadcasted_iota(jnp.int32, (2, lanes), 0)
    kind2 = lax.broadcasted_iota(jnp.int32, (2, lanes), 1) % 2
    rates = jnp.sum(jnp.where(side == kind2, rates, 0.0), axis=0, keepdims=True)
    spikes = lax.dot_general(
        spike_ref[...], spread, (((0,), (0,)), ((), ())),
        precision=HIGHEST, preferred_element_type=F32,
    )
    logs = spikes - deltas * rates
    t_at = lax.broadcasted_iota(jnp.int32, (length, length), 0)
    s_at = lax.broadcasted_iota(jnp.int32, (length, length), 1)
    tri = jnp.where(t_at >= s_at, 1.0, 0.0).astype(F32)
    run_f = jnp.dot(tri, logs, precision=HIGHEST, preferred_element_type=F32)
    tri = jnp.where(t_at <= s_at, 1.0, 0.0).astype(F32)
    run_b = jnp.dot(tri, logs, precision=HIGHEST, preferred_element_type=F32)
    kind = lax.broadcasted_iota(jnp.int32, (length, lanes), 1) % 4
    table = jnp.where(kind < 2, deltas, jnp.where(kind == 2, run_f, run_b))
    table_ref[...] = table
    turned_ref[...] = table.T
    ends = jnp.where(kind[0:1] == 2, run_f[length - 1 : length], run_b[0:1])
    ends_ref[...] = jnp.broadcast_to(ends, ends_ref.shape)

    def ring_step(step, _):
        for way, chunk in parts:
            forward(step, way, chunk)
            mate_copy(step - EARLY, way, chunk, True).wait_recv()
            dot_part(step - EARLY, way, chunk)
        return 0

    def catch_up(step, _):
        for way, chunk in parts:
            mate_copy(step, way, chunk, True).wait_recv()
            dot_part(step, way, chunk)
        return 0

    lax.fori_loop(EARLY + 1, 2 * EARLY + 1, ring_step, 0)
    lax.fori_loop(EARLY + 1, 2 * EARLY + 1, catch_up, 0)

    def late_step(step, _):
        for way, chunk in parts:
            forward(step, way, chunk)
            mate_copy(step, way, chunk, True).wait_recv()
            dot_part(step, way, chunk)
        return 0

    lax.fori_loop(2 * EARLY + 1, chips - 1, late_step, 0)
    for way, chunk in parts:
        mate_copy(chips - 1, way, chunk, True).wait_recv()
        dot_part(chips - 1, way, chunk)
        cols = cols_of(way, chunk)
        proj_ref[:, cols] = acc[:, cols].astype(BF16)

    def drain(step, _):
        for way, chunk in parts:
            @pl.when(step < chips - 1)
            def _():
                ring_copy(step, way, chunk).wait_send()

            mate_copy(step, way, chunk).wait_send()
        return 0

    lax.fori_loop(0, chips, drain, 0)


def front(rows, gain, conv_w, rec_w, lat_w, step_w, rate, spike):
    n = lax.axis_size("sp")
    chips = n // 2
    own_rows, width = rows.shape
    length = 2 * own_rows
    full = length + 2 * HALO
    depth = conv_w.shape[1]
    cols = sum(w.shape[0] * w.shape[2] for w in (conv_w, rec_w, lat_w))
    blocks = sum(w.shape[0] for w in (conv_w, rec_w, lat_w))
    heads = spike.shape[0]
    assert 4 * heads <= STATE and 2 * EARLY + 1 < chips
    vmem = pl.BlockSpec(memory_space=pltpu.VMEM)
    hbm = pl.BlockSpec(memory_space=pl.ANY)
    return pl.pallas_call(
        functools.partial(front_kernel, n),
        out_shape=[
            jax.ShapeDtypeStruct((full, cols), BF16),
            jax.ShapeDtypeStruct((length, STATE), F32),
            jax.ShapeDtypeStruct((STATE, length), F32),
            jax.ShapeDtypeStruct((8, STATE), F32),
        ],
        in_specs=[vmem, vmem, hbm, hbm, hbm, vmem, vmem, vmem],
        out_specs=[vmem] * 4,
        scratch_shapes=[
            pltpu.VMEM((n * depth, cols), BF16),
            pltpu.VMEM((full, width), BF16),
            pltpu.VMEM((full, width), BF16),
            pltpu.VMEM((full, cols), F32),
            pltpu.SemaphoreType.DMA((blocks,)),
            pltpu.SemaphoreType.DMA,
            pltpu.SemaphoreType.DMA((3,)),
            pltpu.SemaphoreType.DMA((3,)),
            pltpu.SemaphoreType.DMA((chips - 1, 2, CHUNKS)),
            pltpu.SemaphoreType.DMA((chips - 1, 2, CHUNKS)),
            pltpu.SemaphoreType.DMA((chips, 2, CHUNKS)),
            pltpu.SemaphoreType.DMA((chips, 2, CHUNKS)),
        ],
        compiler_params=pltpu.CompilerParams(
            collective_id=2, has_side_effects=True, vmem_limit_bytes=56 * 2**20
        ),
        cost_estimate=pl.CostEstimate(
            flops=2 * full * width * cols, bytes_accessed=2 * width * cols, transcendentals=0
        ),
    )(rows, gain.reshape(1, -1), conv_w, rec_w, lat_w, step_w, rate, spike)


def exit_ring(n, c_ref, s_ref, c_out, s_out, own_sems, sems):
    chips = n // 2
    me, core, spot, device = ring_spot(n)
    mate = me + 1 - 2 * core
    ways = (device(spot + 1), device(spot - 1))
    ring_send, ring_recv, mate_send, mate_recv = sems
    refs, outs = (c_ref, s_ref), (c_out, s_out)
    rows, wide = c_ref.shape
    tall = rows // CHUNKS

    def spot_in(owner, way, chunk):
        cols = pl.ds(pl.multiple_of(owner * wide, wide), wide)
        return outs[way].at[pl.ds(chunk * tall, tall), cols]

    def owner_of(step, way):
        return device(spot - step if way == 0 else spot + step)

    def source(step, way, chunk):
        if step == 0:
            return refs[way].at[pl.ds(chunk * tall, tall)]
        return spot_in(owner_of(step, way), way, chunk)

    def ring_copy(step, way, chunk):
        at = (step, way, chunk)
        return send_to(
            source(step, way, chunk), spot_in(owner_of(step, way), way, chunk),
            ring_send.at[at], ring_recv.at[at], {"sp": ways[way]},
        )

    def arrival(step, way, chunk):
        part = spot_in(owner_of(step + 1, way), way, chunk)
        at = (step, way, chunk)
        return send_to(part, part, ring_send.at[at], ring_recv.at[at], {"sp": ways[way]})

    def mate_copy(step, way, chunk, incoming=False):
        owner = owner_of(step, way)
        at = (step, way, chunk)
        there = spot_in(owner + 1 - 2 * core if incoming else owner, way, chunk)
        src = there if incoming else source(step, way, chunk)
        return send_to(src, there, mate_send.at[at], mate_recv.at[at], {"sp": mate})

    parts = [(way, chunk) for chunk in range(CHUNKS) for way in range(2)]
    cols = pl.ds(pl.multiple_of(me * wide, wide), wide)
    own = [
        pltpu.make_async_copy(refs[way], outs[way].at[:, cols], own_sems.at[way])
        for way in range(2)
    ]

    def start():
        for way, chunk in parts:
            ring_copy(0, way, chunk).start()
        for way, chunk in parts:
            mate_copy(0, way, chunk).start()
        for copy in own:
            copy.start()

    def advance(step):
        for way, chunk in parts:
            arrival(step, way, chunk).wait_recv()
            if step < chips - 2:
                ring_copy(step + 1, way, chunk).start()
            mate_copy(step + 1, way, chunk).start()

    def finish():
        for copy in own:
            copy.wait()
        for step in range(chips):
            for way, chunk in parts:
                if step < chips - 1:
                    ring_copy(step, way, chunk).wait_send()
                mate_copy(step, way, chunk).wait_send()
                mate_copy(step, way, chunk, True).wait_recv()

    return chips, start, advance, finish


def tap_sum(padded, taps, length):
    full = padded.shape[0]
    half = len(taps) // 2
    total = None
    for k, tap in enumerate(taps):
        moved = padded if k == half else pltpu.roll(padded, (half - k) % full, 0)
        term = moved[HALO : HALO + length] * tap
        total = term if total is None else total + term
    return total


def tail_kernel(
    n, proj_ref, table_ref, turned_ref, ends_ref, ct_ref, xt_ref, lt_ref, gain_ref,
    c_ref, x_ref, out_ref,
    c_all, x_all, y_c, y_s, within, reads, states, got, logs, enter, entered, away, came,
    s_out, s_in, l_out, l_in, e_out, e_in, p_out, p_in,
    own_sems, ring_send, ring_recv, mate_send, mate_recv,
):
    me = lax.axis_index("sp")
    tp_me = lax.axis_index("tp")
    length = y_c.shape[0]
    own_rows, width = out_ref.shape
    conv_width, ssd_width = y_c.shape[1], y_s.shape[1]
    state_width = reads.shape[1]
    pairs = ssd_width // (2 * HEAD_DIM)
    cw, pw, sw = conv_width // pairs, 2 * HEAD_DIM, 2 * STATE
    at_gate = 3 * conv_width
    at_x = at_gate + ssd_width
    at_b = at_x + ssd_width
    at_c = at_b + state_width

    barrier = pltpu.get_barrier_semaphore()
    for other in [{"sp": (me + k) % n} for k in range(1, n)] + [{"tp": 1 - tp_me}]:
        pl.semaphore_signal(
            barrier, inc=1, device_id=other, device_id_type=pl.DeviceIdType.MESH
        )
    pl.semaphore_wait(barrier, n)
    chips, start, advance, finish = exit_ring(
        n, c_ref, x_ref, c_all, x_all, own_sems, (ring_send, ring_recv, mate_send, mate_recv)
    )
    start()

    def log_copy(k, incoming=False):
        there = (me + n - k) % n if incoming else (me + k) % n
        slot = there if incoming else me
        return send_to(ends_ref, logs.at[slot], l_out.at[k], l_in.at[k], {"sp": there})

    for k in range(1, n):
        log_copy(k).start()
    logs[me] = ends_ref[...]

    t_at = lax.broadcasted_iota(jnp.int32, (length, length), 0)
    s_at = lax.broadcasted_iota(jnp.int32, (length, length), 1)
    below, above = t_at > s_at, t_at < s_at
    here = slice(HALO, HALO + length)

    def rows_f32(ref, j, wide, base):
        return ref[:, base + j * wide : base + (j + 1) * wide].astype(F32)

    def state_copy(owner):
        return send_to(
            states.at[owner], got.at[me], s_out.at[owner], s_in.at[me], {"sp": owner}
        )

    def mix_pair(j):
        taps = ct_ref[:, j * cw : (j + 1) * cw].astype(F32)
        gated = rows_f32(proj_ref, j, cw, conv_width) * rows_f32(proj_ref, j, cw, 2 * conv_width)
        conv = tap_sum(
            gated.astype(BF16).astype(F32), [taps[k : k + 1] for k in range(taps.shape[0])], length
        )
        og = proj_ref[here, j * cw : (j + 1) * cw].astype(F32)
        y_c[:, j * cw : (j + 1) * cw] = (og * conv).astype(BF16)
        taps = xt_ref[:, j * pw : (j + 1) * pw].astype(F32)
        xs = silu(
            tap_sum(
                rows_f32(proj_ref, j, pw, at_x), [taps[k : k + 1] for k in range(taps.shape[0])], length
            )
        ).astype(BF16)
        taps = [lt_ref[k, :, j * sw : (j + 1) * sw].astype(F32) for k in range(lt_ref.shape[0])]
        bs = silu(
            tap_sum(rows_f32(proj_ref, j, sw, at_b), [tap[0:1] for tap in taps], length)
        ).astype(BF16)
        cs = silu(
            tap_sum(rows_f32(proj_ref, j, sw, at_c), [tap[1:2] for tap in taps], length)
        ).astype(BF16)
        reads[:, j * sw : (j + 1) * sw] = cs
        outs = []
        for h in range(2):
            c_h = cs[:, h * STATE : (h + 1) * STATE]
            b_h = bs[:, h * STATE : (h + 1) * STATE]
            x_h = xs[:, h * HEAD_DIM : (h + 1) * HEAD_DIM]
            head = 2 * j + h
            cols = table_ref[:, 4 * head : 4 * head + 4]
            rows = turned_ref[4 * head : 4 * head + 4, :]
            scores = lax.dot_general(
                c_h, b_h, (((1,), (1,)), ((), ())), preferred_element_type=F32
            )
            gap = jnp.where(above, cols[:, 3:4] - rows[3:4], cols[:, 2:3] - rows[2:3])
            d_f, d_b = rows[0:1], rows[1:2]
            scale = jnp.where(below, d_f, jnp.where(above, d_b, d_f + d_b))
            w = (scores * jnp.exp(gap) * scale).astype(BF16)
            outs.append(jnp.dot(w, x_h, preferred_element_type=F32))
            x32 = x_h.astype(F32)
            end_f = jnp.exp(rows[2:3, length - 1 : length] - cols[:, 2:3])
            end_b = jnp.exp(rows[3:4, 0:1] - cols[:, 3:4])
            both = jnp.concatenate(
                [x32 * (end_f * cols[:, 0:1]), x32 * (end_b * cols[:, 1:2])], axis=1
            ).astype(BF16)
            state = lax.dot_general(
                both, b_h, (((0,), (0,)), ((), ())), preferred_element_type=F32
            ).astype(BF16)
            for d in range(2):
                states[2 * head + d] = state[d * HEAD_DIM : (d + 1) * HEAD_DIM]
        within[:, j * pw : (j + 1) * pw] = jnp.concatenate(outs, axis=1)

    def send_states(j):
        for owner in range(4 * j, 4 * j + 4):
            @pl.when(me != owner)
            def _():
                state_copy(owner).start()

            @pl.when(me == owner)
            def _():
                got[owner] = states[owner]

    for j in range(pairs):
        mix_pair(j)
        advance(j)
        send_states(j)

    for k in range(1, n):
        log_copy(k, True).wait_recv()
    lane = 4 * (me // 2) + 2 + me % 2
    lane_at = lax.broadcasted_iota(jnp.int32, (1, STATE), 1)
    for k in range(1, n):
        other = (me + k) % n
        send_to(
            states.at[other], got.at[other], s_out.at[other], s_in.at[other], {"sp": other}
        ).wait_recv()
    back = me % 2
    acc = jnp.zeros(got.shape[1:], F32)
    for i in range(n):
        j = back * (n - 1 - i) + (1 - back) * i
        enter[j] = acc.astype(BF16)
        log = jnp.sum(
            jnp.where(lane_at == lane, logs[j][0:1, :], 0.0), axis=1, keepdims=True
        )
        acc = acc * jnp.exp(log) + got[j].astype(F32)
    entered[me] = enter[me]

    def enter_copy(k, incoming=False):
        there = (me + n - k) % n if incoming else (me + k) % n
        slot = there if incoming else me
        return send_to(enter.at[there], entered.at[slot], e_out.at[k], e_in.at[k], {"sp": there})

    for k in range(1, n):
        enter_copy(k).start()
    for step in range(pairs, chips - 1):
        advance(step)
    for k in range(1, n):
        enter_copy(k, True).wait_recv()

    for j in range(pairs):
        outs = []
        gate = silu(rows_f32(proj_ref, j, pw, at_gate)[here])
        for h in range(2):
            head = 2 * j + h
            cols = table_ref[:, 4 * head : 4 * head + 4]
            wide = jnp.concatenate([entered[2 * head], entered[2 * head + 1]], axis=0)
            both = lax.dot_general(
                reads[:, head * STATE : (head + 1) * STATE], wide,
                (((1,), (1,)), ((), ())), preferred_element_type=F32,
            )
            mine = slice(h * HEAD_DIM, (h + 1) * HEAD_DIM)
            y = within[:, head * HEAD_DIM : (head + 1) * HEAD_DIM]
            y = y + both[:, :HEAD_DIM] * jnp.exp(cols[:, 2:3])
            y = y + both[:, HEAD_DIM:] * jnp.exp(cols[:, 3:4])
            g = y * gate[:, mine]
            g = g * lax.rsqrt(jnp.mean(g * g, axis=-1, keepdims=True) + epsilon)
            gain = gain_ref[:, head * HEAD_DIM : (head + 1) * HEAD_DIM].astype(F32)
            outs.append(g * gain)
        y_s[:, j * pw : (j + 1) * pw] = jnp.concatenate(outs, axis=1).astype(BF16)
    finish()

    part = width // BLOCKS

    def partial(owner, block):
        rows = pl.ds(pl.multiple_of(owner * own_rows, HALO), own_rows)
        cols = slice(block * part, (block + 1) * part)
        return jnp.dot(
            y_c[rows, :], c_all[:, cols], preferred_element_type=F32
        ) + jnp.dot(y_s[rows, :], x_all[:, cols], preferred_element_type=F32)

    def partial_copy(block):
        return send_to(
            away.at[block], came.at[block], p_out.at[block], p_in.at[block], {"tp": 1 - tp_me}
        )

    for block in range(BLOCKS):
        away[block] = partial(1 - tp_me, block).astype(BF16)
        partial_copy(block).start()
    for block in range(BLOCKS):
        kept = partial(tp_me, block)
        partial_copy(block).wait_recv()
        cols = slice(block * part, (block + 1) * part)
        out_ref[:, cols] = (kept + came[block].astype(F32)).astype(BF16)
    for block in range(BLOCKS):
        partial_copy(block).wait_send()
    for k in range(1, n):
        log_copy(k).wait_send()
        enter_copy(k).wait_send()
        other = (me + k) % n
        state_copy(other).wait_send()


def tail(proj, table, turned, ends, conv_taps, x_taps, latent_taps, gain, exit_c, exit_s, own_rows):
    n = lax.axis_size("sp")
    chips = n // 2
    length = table.shape[0]
    conv_width, ssd_width = exit_c.shape[0], exit_s.shape[0]
    state_width = latent_taps.shape[2]
    width = exit_c.shape[1] * n
    pairs = ssd_width // (2 * HEAD_DIM)
    assert 4 * pairs == n and pairs < chips - 1 and conv_width == ssd_width
    vmem = pl.BlockSpec(memory_space=pltpu.VMEM)
    spans = (n, HEAD_DIM, STATE)
    blocks = (BLOCKS, own_rows, width // BLOCKS)
    return pl.pallas_call(
        functools.partial(tail_kernel, n),
        out_shape=jax.ShapeDtypeStruct((own_rows, width), BF16),
        in_specs=[vmem] * 10,
        out_specs=vmem,
        scratch_shapes=[
            pltpu.VMEM((conv_width, width), BF16),
            pltpu.VMEM((ssd_width, width), BF16),
            pltpu.VMEM((length, conv_width), BF16),
            pltpu.VMEM((length, ssd_width), BF16),
            pltpu.VMEM((length, ssd_width), F32),
            pltpu.VMEM((length, state_width), BF16),
            pltpu.VMEM(spans, BF16),
            pltpu.VMEM(spans, BF16),
            pltpu.VMEM((n, 8, STATE), F32),
            pltpu.VMEM(spans, BF16),
            pltpu.VMEM(spans, BF16),
            pltpu.VMEM(blocks, BF16),
            pltpu.VMEM(blocks, BF16),
        ]
        + [pltpu.SemaphoreType.DMA((n,))] * 6
        + [pltpu.SemaphoreType.DMA((BLOCKS,))] * 2
        + [pltpu.SemaphoreType.DMA((2,))]
        + [pltpu.SemaphoreType.DMA((chips - 1, 2, CHUNKS))] * 2
        + [pltpu.SemaphoreType.DMA((chips, 2, CHUNKS))] * 2,
        compiler_params=pltpu.CompilerParams(
            collective_id=3, has_side_effects=True, vmem_limit_bytes=48 * 2**20
        ),
        cost_estimate=pl.CostEstimate(
            flops=4 * length * conv_width * width, bytes_accessed=2**24, transcendentals=0
        ),
    )(proj, table, turned, ends, conv_taps, x_taps, latent_taps, gain, exit_c, exit_s)


def project_kernel(r_ref, w_ref, o_ref):
    o_ref[...] = jnp.dot(r_ref[...], w_ref[...], preferred_element_type=F32).astype(BF16)


def project(rows, weights):
    count, width = rows.shape
    cols = weights.shape[1]
    tile = cols // 9
    return pl.pallas_call(
        project_kernel,
        grid=(9,),
        in_specs=[
            pl.BlockSpec((count, width), lambda j: (0, 0)),
            pl.BlockSpec((width, tile), lambda j: (0, j)),
        ],
        out_specs=pl.BlockSpec((count, tile), lambda j: (0, j)),
        out_shape=jax.ShapeDtypeStruct((count, cols), BF16),
        cost_estimate=pl.CostEstimate(
            flops=2 * count * width * cols, bytes_accessed=2 * width * cols, transcendentals=0
        ),
    )(rows, weights)


def finish_kernel(within_ref, reads_ref, enter_ref, gate_ref, gain_ref, col_ref, y_ref):
    length = y_ref.shape[0]
    cols = col_ref[0]
    outs = []
    for h in range(2):
        o = 4 * h
        both = lax.dot_general(
            reads_ref[:, h * STATE : (h + 1) * STATE],
            enter_ref[h * STATE : (h + 1) * STATE],
            (((1,), (1,)), ((), ())),
            preferred_element_type=F32,
        )
        here = slice(h * HEAD_DIM, (h + 1) * HEAD_DIM)
        y = within_ref[:, here]
        y = y + both[:, :HEAD_DIM] * jnp.exp(cols[:, o + 2 : o + 3])
        y = y + both[:, HEAD_DIM:] * jnp.exp(cols[:, o + 3 : o + 4])
        g = y * silu(gate_ref[pl.ds(HALO, length), :].astype(F32)[:, here])
        g = g * lax.rsqrt(jnp.mean(g * g, axis=-1, keepdims=True) + epsilon)
        outs.append(g * gain_ref[:, here].astype(F32))
    y_ref[...] = jnp.concatenate(outs, axis=1).astype(BF16)


def local(
    layer_source_rows, entry_rescale_factor, sliding_mixer_entry_matrix,
    recurrent_mixer_entry_matrix, latent_write_read_matrix, timestep_matrix,
    sliding_kernel_coefficients, recurrent_kernel_coefficients, latent_kernel_coefficients,
    lane_forgetting_rate, spike_forgetting_rate, lane_rescale_factor,
    sliding_mixer_exit_matrix, recurrent_mixer_exit_matrix,
):
    n = lax.axis_size("sp")
    tp = lax.axis_size("tp")
    own_rows, width = layer_source_rows.shape
    length = own_rows * tp
    full = length + 2 * HALO
    conv_width = sliding_mixer_entry_matrix.shape[2]
    ssd_width = recurrent_mixer_entry_matrix.shape[2]
    state_width = latent_write_read_matrix.shape[2]
    heads = timestep_matrix.shape[2]
    pairs = heads // 2
    cw = conv_width // pairs

    share = heads * 2 * HEAD_DIM // n
    if tp == 2 and 2 * heads == n:
        proj, table, turned, ends = front(
            layer_source_rows, entry_rescale_factor, sliding_mixer_entry_matrix,
            recurrent_mixer_entry_matrix, latent_write_read_matrix,
            timestep_matrix.transpose(1, 2, 0).reshape(2 * heads, width),
            lane_forgetting_rate, spike_forgetting_rate.T,
        )
        return tail(
            proj, table, turned, ends, sliding_kernel_coefficients,
            recurrent_kernel_coefficients, latent_kernel_coefficients,
            lane_rescale_factor.reshape(1, -1), sliding_mixer_exit_matrix,
            recurrent_mixer_exit_matrix, own_rows,
        )

    block = jnp.concatenate(
        [sliding_mixer_entry_matrix[i] for i in range(3)]
        + [recurrent_mixer_entry_matrix[i] for i in range(2)]
        + [latent_write_read_matrix[i] for i in range(2)],
        axis=1,
    )
    gathered = gather_rows(block)
    weights = gathered.reshape(n * block.shape[0], block.shape[1])

    x32 = layer_source_rows.astype(F32)
    normed = (
        x32
        * lax.rsqrt(jnp.mean(x32 * x32, axis=-1, keepdims=True) + epsilon)
        * entry_rescale_factor.astype(F32)
    ).astype(BF16)
    up = [(i, i + 1) for i in range(n - 1)]
    down = [(i + 1, i) for i in range(n - 1)]
    before = lax.ppermute(normed[own_rows - HALO :], "sp", up)
    after = lax.ppermute(normed[:HALO], "sp", down)
    shared = lax.all_gather(jnp.concatenate([before, normed, after], axis=0), "tp", axis=0)
    rows = jnp.concatenate(
        [shared[tp - 1, :HALO]]
        + [shared[i, HALO : HALO + own_rows] for i in range(tp)]
        + [shared[0, HALO + own_rows :]],
        axis=0,
    )

    step_weight = timestep_matrix.reshape(width, 2 * heads)
    raw = jnp.dot(rows, step_weight, preferred_element_type=F32).astype(BF16)
    raw = raw[HALO : HALO + length].astype(F32).reshape(length, 2, heads)
    deltas = jax.nn.softplus(raw)
    logs = -deltas * lane_forgetting_rate[None] + spike_forgetting_rate[:, None, :]
    tri = (jnp.arange(length)[:, None] >= jnp.arange(length)[None, :]).astype(F32)
    run_f = jnp.dot(tri, logs[:, 0], precision=HIGHEST)
    run_b = jnp.dot(tri.T, logs[:, 1], precision=HIGHEST)
    table = jnp.stack([deltas[:, 0], deltas[:, 1], run_f, run_b], axis=2)
    col_table = table.reshape(length, pairs, 8).transpose(1, 0, 2)
    row_table = table.reshape(length, pairs, 8).transpose(1, 2, 0)
    span_log = jnp.stack([run_f[length - 1], run_b[0]], axis=1)
    exit_c, exit_s, weights = lax.optimization_barrier(
        (sliding_mixer_exit_matrix, recurrent_mixer_exit_matrix, weights)
    )
    proj = project(rows, weights)
    exit_c = lax.all_gather(exit_c, "sp", axis=1, tiled=True)
    exit_s = lax.all_gather(exit_s, "sp", axis=1, tiled=True)

    latent = latent_kernel_coefficients
    pw, sw = 2 * HEAD_DIM, 2 * STATE
    g0 = 3 * conv_width
    at_gate, at_x = g0 // pw, (g0 + ssd_width) // pw
    at_b = (g0 + 2 * ssd_width) // sw
    at_c = at_b + pairs
    y_conv, within, reads, states = pl.pallas_call(
        mix_kernel,
        grid=(pairs,),
        in_specs=[
            pl.BlockSpec((full, cw), lambda j: (0, j)),
            pl.BlockSpec((full, cw), lambda j: (0, pairs + j)),
            pl.BlockSpec((full, cw), lambda j: (0, 2 * pairs + j)),
            pl.BlockSpec((full, pw), lambda j: (0, at_x + j)),
            pl.BlockSpec((full, sw), lambda j: (0, at_b + j)),
            pl.BlockSpec((full, sw), lambda j: (0, at_c + j)),
            pl.BlockSpec((3, cw), lambda j: (0, j)),
            pl.BlockSpec((5, pw), lambda j: (0, j)),
            pl.BlockSpec((5, sw), lambda j: (0, j)),
            pl.BlockSpec((5, sw), lambda j: (0, pairs + j)),
            pl.BlockSpec((1, length, 8), lambda j: (j, 0, 0)),
            pl.BlockSpec((1, 8, length), lambda j: (j, 0, 0)),
        ],
        out_specs=[
            pl.BlockSpec((length, cw), lambda j: (0, j)),
            pl.BlockSpec((length, pw), lambda j: (0, j)),
            pl.BlockSpec((length, sw), lambda j: (0, j)),
            pl.BlockSpec((sw, STATE), lambda j: (j, 0)),
        ],
        out_shape=[
            jax.ShapeDtypeStruct((length, conv_width), BF16),
            jax.ShapeDtypeStruct((length, ssd_width), F32),
            jax.ShapeDtypeStruct((length, state_width), BF16),
            jax.ShapeDtypeStruct((pairs * sw, STATE), BF16),
        ],
        cost_estimate=pl.CostEstimate(
            flops=8 * length * length * heads * STATE, bytes_accessed=2**24, transcendentals=0
        ),
    )(
        proj, proj, proj, proj, proj, proj,
        sliding_kernel_coefficients, recurrent_kernel_coefficients,
        latent.reshape(latent.shape[0], -1), latent.reshape(latent.shape[0], -1),
        col_table, row_table,
    )

    entering = exchange_states(states.reshape(n, share, STATE), span_log)
    entering = entering.reshape(pairs * sw, STATE)

    y_ssd = pl.pallas_call(
        finish_kernel,
        grid=(pairs,),
        in_specs=[
            pl.BlockSpec((length, pw), lambda j: (0, j)),
            pl.BlockSpec((length, sw), lambda j: (0, j)),
            pl.BlockSpec((sw, STATE), lambda j: (j, 0)),
            pl.BlockSpec((full, pw), lambda j: (0, at_gate + j)),
            pl.BlockSpec((1, pw), lambda j: (0, j)),
            pl.BlockSpec((1, length, 8), lambda j: (j, 0, 0)),
        ],
        out_specs=pl.BlockSpec((length, pw), lambda j: (0, j)),
        out_shape=jax.ShapeDtypeStruct((length, ssd_width), BF16),
    )(within, reads, entering, proj, lane_rescale_factor.reshape(1, -1), col_table)

    def partial(y_c, y_s):
        return (
            jnp.dot(y_c, exit_c, preferred_element_type=F32)
            + jnp.dot(y_s, exit_s, preferred_element_type=F32)
        ).astype(BF16)

    if tp != 2:
        return lax.psum_scatter(
            partial(y_conv, y_ssd), "tp", scatter_dimension=0, tiled=True
        )
    tp_me = lax.axis_index("tp")

    def rows_of(owner, y):
        return lax.dynamic_slice_in_dim(y, owner * own_rows, own_rows, axis=0)

    away = partial(rows_of(1 - tp_me, y_conv), rows_of(1 - tp_me, y_ssd))
    arrived = lax.ppermute(away, "tp", [(0, 1), (1, 0)])
    kept = partial(rows_of(tp_me, y_conv), rows_of(tp_me, y_ssd))
    return (kept.astype(F32) + arrived.astype(F32)).astype(BF16)


def solution(mesh):
    placed = (
        P(("sp", "tp"), None),
        P(),
        P(None, "sp", "tp"),
        P(None, "sp", "tp"),
        P(None, "sp", "tp"),
        P(None, None, "tp"),
        P(None, "tp"),
        P(None, "tp"),
        P(None, None, "tp"),
        P(None, "tp"),
        P("sp", "tp"),
        P("tp"),
        P("tp", "sp"),
        P("tp", "sp"),
    )
    return jax.shard_map(
        local, mesh=mesh, in_specs=placed, out_specs=P(("sp", "tp"), None), check_vma=False
    )
```

```python
import functools

import jax
import jax.numpy as jnp
from jax import lax
from jax.experimental import pallas as pl
from jax.experimental.pallas import tpu as pltpu
from jax.sharding import PartitionSpec as P

HEAD_DIM = 64
STATE = 128
HALO = 16
CHUNKS = 2
LAG = 2
SKEW = 2
BLOCKS = 4
epsilon = 1e-05
F32 = jnp.float32
BF16 = jnp.bfloat16
HIGHEST = lax.Precision.HIGHEST


def ring_kernel(n, w_ref, out_ref, own_sem, ring_send, ring_recv, mate_send, mate_recv):
    chips = n // 2
    me = lax.axis_index("sp")
    core, chip = me % 2, me // 2
    odd = chip % 2
    spot = (1 - odd) * (chip // 2) + odd * (chips - 1 - chip // 2)

    def device(position):
        position = (position + 2 * chips) % chips
        half = (chips + 1) // 2
        late = position // half
        late_chip = 2 * (chips - 1 - position) + 1
        return 2 * ((1 - late) * 2 * position + late * late_chip) + core

    mate = me + 1 - 2 * core
    ways = (device(spot + 1), device(spot - 1))
    rows = w_ref.shape[0] // (2 * CHUNKS)

    barrier = pltpu.get_barrier_semaphore()
    for other in (mate,) + ways:
        pl.semaphore_signal(
            barrier, inc=1, device_id={"sp": other}, device_id_type=pl.DeviceIdType.MESH
        )
    pl.semaphore_wait(barrier, 3)

    def piece(way, chunk):
        return pl.ds((way * CHUNKS + chunk) * rows, rows)

    def ring_copy(step, way, chunk):
        owner = device(spot - step if way == 0 else spot + step)
        part = piece(way, chunk)
        return pltpu.make_async_remote_copy(
            src_ref=w_ref.at[part] if step == 0 else out_ref.at[owner, part],
            dst_ref=out_ref.at[owner, part],
            send_sem=ring_send.at[step, way, chunk],
            recv_sem=ring_recv.at[step, way, chunk],
            device_id={"sp": ways[way]},
            device_id_type=pl.DeviceIdType.MESH,
        )

    def arrival(step, way, chunk):
        owner = device(spot - step - 1 if way == 0 else spot + step + 1)
        part = piece(way, chunk)
        return pltpu.make_async_remote_copy(
            src_ref=out_ref.at[owner, part],
            dst_ref=out_ref.at[owner, part],
            send_sem=ring_send.at[step, way, chunk],
            recv_sem=ring_recv.at[step, way, chunk],
            device_id={"sp": ways[way]},
            device_id_type=pl.DeviceIdType.MESH,
        )

    def mate_copy(step, way, chunk, incoming=False):
        owner = device(spot - step if way == 0 else spot + step)
        if incoming:
            owner = owner + 1 - 2 * core
        part = piece(way, chunk)
        return pltpu.make_async_remote_copy(
            src_ref=w_ref.at[part] if step == 0 else out_ref.at[owner, part],
            dst_ref=out_ref.at[owner, part],
            send_sem=mate_send.at[step, way, chunk],
            recv_sem=mate_recv.at[step, way, chunk],
            device_id={"sp": mate},
            device_id_type=pl.DeviceIdType.MESH,
        )

    parts = [(way, chunk) for chunk in range(CHUNKS) for way in range(2)]
    for way, chunk in parts:
        ring_copy(0, way, chunk).start()
    for way, chunk in parts:
        mate_copy(0, way, chunk).start()
    own = pltpu.make_async_copy(w_ref, out_ref.at[me], own_sem)
    own.start()
    for step in range(chips - 1):
        for way, chunk in parts:
            arrival(step, way, chunk).wait_recv()
            if step < chips - 2:
                ring_copy(step + 1, way, chunk).start()
            mate_copy(step + 1, way, chunk).start()
    own.wait()
    for step in range(chips):
        for way, chunk in parts:
            if step < chips - 1:
                ring_copy(step, way, chunk).wait_send()
            mate_copy(step, way, chunk).wait_send()
            mate_copy(step, way, chunk, True).wait_recv()


def gather_rows(block):
    n = lax.axis_size("sp")
    chips = n // 2
    rows, cols = block.shape
    return pl.pallas_call(
        functools.partial(ring_kernel, n),
        out_shape=jax.ShapeDtypeStruct((n, rows, cols), block.dtype),
        in_specs=[pl.BlockSpec(memory_space=pltpu.VMEM)],
        out_specs=pl.BlockSpec(memory_space=pl.ANY),
        scratch_shapes=[
            pltpu.SemaphoreType.DMA,
            pltpu.SemaphoreType.DMA((chips - 1, 2, CHUNKS)),
            pltpu.SemaphoreType.DMA((chips - 1, 2, CHUNKS)),
            pltpu.SemaphoreType.DMA((chips, 2, CHUNKS)),
            pltpu.SemaphoreType.DMA((chips, 2, CHUNKS)),
        ],
        compiler_params=pltpu.CompilerParams(
            collective_id=0, has_side_effects=True, vmem_limit_bytes=16 * 2**20
        ),
        cost_estimate=pl.CostEstimate(
            flops=0, bytes_accessed=n * rows * cols * 16, transcendentals=0
        ),
    )(block)


def taps_of(padded, table, length):
    full = padded.shape[0]
    half = table.shape[0] // 2
    total = None
    for k in range(table.shape[0]):
        moved = padded if k == half else pltpu.roll(padded, (half - k) % full, 0)
        term = moved[HALO : HALO + length] * table[k : k + 1].astype(F32)
        total = term if total is None else total + term
    return total


def silu(v):
    return v * jax.nn.sigmoid(v)


def mix_kernel(
    og_ref, ig_ref, va_ref, x_ref, b_ref, c_ref, ct_ref, xt_ref, bt_ref, rt_ref,
    col_ref, row_ref, yconv_ref, within_ref, reads_ref, state_ref,
):
    length = yconv_ref.shape[0]
    gated = (ig_ref[...].astype(F32) * va_ref[...].astype(F32)).astype(BF16).astype(F32)
    conv = taps_of(gated, ct_ref[...], length)
    yconv_ref[...] = (og_ref[pl.ds(HALO, length), :].astype(F32) * conv).astype(BF16)
    xs = silu(taps_of(x_ref[...].astype(F32), xt_ref[...], length)).astype(BF16)
    bs = silu(taps_of(b_ref[...].astype(F32), bt_ref[...], length)).astype(BF16)
    cs = silu(taps_of(c_ref[...].astype(F32), rt_ref[...], length)).astype(BF16)
    reads_ref[...] = cs
    cols = col_ref[0]
    rows = row_ref[0]
    t_at = lax.broadcasted_iota(jnp.int32, (length, length), 0)
    s_at = lax.broadcasted_iota(jnp.int32, (length, length), 1)
    outs, weighted = [], []
    for h in range(2):
        c_h = cs[:, h * STATE : (h + 1) * STATE]
        b_h = bs[:, h * STATE : (h + 1) * STATE]
        x_h = xs[:, h * HEAD_DIM : (h + 1) * HEAD_DIM]
        o = 4 * h
        scores = lax.dot_general(
            c_h, b_h, (((1,), (1,)), ((), ())), preferred_element_type=F32
        )
        gap = jnp.where(
            t_at >= s_at,
            cols[:, o + 2 : o + 3] - rows[o + 2 : o + 3],
            cols[:, o + 3 : o + 4] - rows[o + 3 : o + 4],
        )
        d_f, d_b = rows[o : o + 1], rows[o + 1 : o + 2]
        scale = jnp.where(t_at > s_at, d_f, jnp.where(t_at < s_at, d_b, d_f + d_b))
        w = (scores * jnp.exp(gap) * scale).astype(BF16)
        outs.append(jnp.dot(w, x_h, preferred_element_type=F32))
        x32 = x_h.astype(F32)
        end_f = jnp.exp(rows[o + 2 : o + 3, length - 1 : length] - cols[:, o + 2 : o + 3])
        end_b = jnp.exp(rows[o + 3 : o + 4, 0:1] - cols[:, o + 3 : o + 4])
        both = jnp.concatenate(
            [x32 * (end_f * cols[:, o : o + 1]), x32 * (end_b * cols[:, o + 1 : o + 2])], axis=1
        ).astype(BF16)
        state_ref[h * STATE : (h + 1) * STATE] = lax.dot_general(
            both, b_h, (((0,), (0,)), ((), ())), preferred_element_type=F32
        ).astype(BF16)
    within_ref[...] = jnp.concatenate(outs, axis=1)


def exchange_kernel(
    n, share, s_ref, l_ref, out_ref, got, logs, enter, s_out, s_in, l_out, l_in, e_out, e_in
):
    me = lax.axis_index("sp")
    barrier = pltpu.get_barrier_semaphore()
    for k in range(1, n):
        pl.semaphore_signal(
            barrier,
            inc=1,
            device_id={"sp": (me + k) % n},
            device_id_type=pl.DeviceIdType.MESH,
        )
    pl.semaphore_wait(barrier, n - 1)

    def copy(src, dst, out_sem, in_sem, k, there, slot):
        return pltpu.make_async_remote_copy(
            src_ref=src.at[there],
            dst_ref=dst.at[slot],
            send_sem=out_sem.at[k],
            recv_sem=in_sem.at[k],
            device_id={"sp": there},
            device_id_type=pl.DeviceIdType.MESH,
        )

    for k in range(1, n):
        there = (me + k) % n
        copy(s_ref, got, s_out, s_in, k, there, me).start()
        copy(l_ref, logs, l_out, l_in, k, there, me).start()
    got[me] = s_ref[me]
    logs[me] = l_ref[me]
    for k in range(1, n):
        here = (me + n - k) % n
        copy(s_ref, got, s_out, s_in, k, here, here).wait_recv()
        copy(l_ref, logs, l_out, l_in, k, here, here).wait_recv()
    back = (me * share // HEAD_DIM) % 2
    acc = jnp.zeros(s_ref.shape[1:], F32)
    for i in range(n):
        j = back * (n - 1 - i) + (1 - back) * i
        enter[j] = acc.astype(BF16)
        acc = acc * jnp.exp(logs[j][0:1, :]) + got[j].astype(F32)
    out_ref[me] = enter[me]
    for k in range(1, n):
        copy(enter, out_ref, e_out, e_in, k, (me + k) % n, me).start()
    for k in range(1, n):
        here = (me + n - k) % n
        copy(enter, out_ref, e_out, e_in, k, here, here).wait_recv()
    for k in range(1, n):
        there = (me + k) % n
        copy(s_ref, got, s_out, s_in, k, there, me).wait_send()
        copy(l_ref, logs, l_out, l_in, k, there, me).wait_send()
        copy(enter, out_ref, e_out, e_in, k, there, me).wait_send()


def exchange_states(states, span_log):
    n, share, _ = states.shape
    assert HEAD_DIM % share == 0
    tables = jnp.repeat(span_log.reshape(-1), HEAD_DIM // share)
    tables = jnp.broadcast_to(tables[:, None, None], (n, 8, STATE))
    return pl.pallas_call(
        functools.partial(exchange_kernel, n, share),
        out_shape=jax.ShapeDtypeStruct(states.shape, BF16),
        in_specs=[pl.BlockSpec(memory_space=pltpu.VMEM)] * 2,
        out_specs=pl.BlockSpec(memory_space=pltpu.VMEM),
        scratch_shapes=[
            pltpu.VMEM(states.shape, BF16),
            pltpu.VMEM(tables.shape, F32),
            pltpu.VMEM(states.shape, BF16),
        ]
        + [pltpu.SemaphoreType.DMA((n,))] * 6,
        compiler_params=pltpu.CompilerParams(collective_id=1, has_side_effects=True),
        cost_estimate=pl.CostEstimate(flops=0, bytes_accessed=2**25, transcendentals=0),
    )(states, tables)


def ring_spot(n):
    chips = n // 2
    me = lax.axis_index("sp")
    core, chip = me % 2, me // 2
    odd = chip % 2
    spot = (1 - odd) * (chip // 2) + odd * (chips - 1 - chip // 2)

    def device(position):
        position = (position + 2 * chips) % chips
        half = (chips + 1) // 2
        late = position // half
        late_chip = 2 * (chips - 1 - position) + 1
        return 2 * ((1 - late) * 2 * position + late * late_chip) + core

    return me, core, spot, device


def send_to(src, dst, out_sem, in_sem, target):
    return pltpu.make_async_remote_copy(
        src_ref=src,
        dst_ref=dst,
        send_sem=out_sem,
        recv_sem=in_sem,
        device_id=target,
        device_id_type=pl.DeviceIdType.MESH,
    )


def softplus(v):
    return jnp.maximum(v, 0.0) + jnp.log1p(jnp.exp(-jnp.abs(v)))


def tap_sum(padded, taps, length):
    full = padded.shape[0]
    half = len(taps) // 2
    total = None
    for k, tap in enumerate(taps):
        moved = padded if k == half else pltpu.roll(padded, (half - k) % full, 0)
        term = moved[HALO : HALO + length] * tap
        total = term if total is None else total + term
    return total


def mixer_kernel(
    n, x_ref, gain_ref, conv_ref, rec_ref, lat_ref, step_ref, rate_ref, spike_ref,
    ct_ref, xt_ref, lt_ref, head_gain_ref, exit_c_ref, exit_s_ref, out_ref,
    w_buf, raw, normed, proj, table_ref, turned_ref, ends_ref,
    c_all, s_all, y_c, y_s, within, reads, states, got, logs, enter, entered, away, came,
    own_sems, exit_own, x_own, x_send, x_recv,
    ring_send, ring_recv, mate_send, mate_recv,
    exit_send, exit_recv, pass_send, pass_recv,
    s_out, s_in, l_out, l_in, e_out, e_in, p_out, p_in,
):
    chips = n // 2
    hops = chips - 1
    me, core, spot, device = ring_spot(n)
    tp_me = lax.axis_index("tp")
    mate = me + 1 - 2 * core
    ways = (device(spot + 1), device(spot - 1))
    own_rows, width = x_ref.shape
    length = 2 * own_rows
    pairs, _, group_cols = w_buf.shape
    depth = w_buf.shape[1] // n
    half = depth // 2
    cw, pw, sw = conv_ref.shape[2] // pairs, 2 * HEAD_DIM, 2 * STATE

    def block_rows(owner):
        return pl.ds(pl.multiple_of(owner * depth, depth), depth)

    own = []
    for g in range(pairs):
        offset = 0
        for ref, wide in ((conv_ref, cw), (rec_ref, pw), (lat_ref, sw)):
            for i in range(ref.shape[0]):
                own.append(
                    pltpu.make_async_copy(
                        ref.at[i, :, pl.ds(g * wide, wide)],
                        w_buf.at[g, block_rows(me), pl.ds(offset, wide)],
                        own_sems.at[len(own)],
                    )
                )
                offset += wide
    per_group = len(own) // pairs
    for copy in own:
        copy.start()

    up, down = (me + 1) % n, (me + n - 1) % n
    barrier = pltpu.get_barrier_semaphore()
    greeted = [{"sp": (me + k) % n} for k in range(1, n)]
    greeted += [{"sp": other, "tp": 1 - tp_me} for other in (me, up, down)]
    for other in greeted:
        pl.semaphore_signal(
            barrier, inc=1, device_id=other, device_id_type=pl.DeviceIdType.MESH
        )
    pl.semaphore_wait(barrier, len(greeted))

    def owner_of(step, way):
        return device(spot - step if way == 0 else spot + step)

    def part_of(g, owner, way):
        return w_buf.at[g, pl.ds(pl.multiple_of(owner * depth + way * half, half), half), :]

    def ring_copy(g, step, way, shift=0):
        part = part_of(g, owner_of(step + shift, way), way)
        at = (g, step, way)
        return send_to(part, part, ring_send.at[at], ring_recv.at[at], {"sp": ways[way]})

    def mate_copy(g, step, way, incoming=False):
        owner = owner_of(step, way)
        part = part_of(g, owner + 1 - 2 * core if incoming else owner, way)
        at = (g, step, way)
        return send_to(part, part, mate_send.at[at], mate_recv.at[at], {"sp": mate})

    def start_group(g):
        for copy in own[g * per_group : (g + 1) * per_group]:
            copy.wait()
        for way in range(2):
            ring_copy(g, 0, way).start()
        for way in range(2):
            mate_copy(g, 0, way).start()

    def advance_group(g, step):
        for way in range(2):
            ring_copy(g, step, way, 1).wait_recv()
            if step < hops - 1:
                ring_copy(g, step + 1, way).start()
            mate_copy(g, step + 1, way).start()

    turn = 1 - 2 * core
    exit_refs, exit_alls = (exit_c_ref, exit_s_ref), (c_all, s_all)
    exit_wide = exit_c_ref.shape[1]

    def exit_cols(which, owner):
        return exit_alls[which].at[:, pl.ds(pl.multiple_of(owner * exit_wide, exit_wide), exit_wide)]

    def exit_source(which, step):
        if step == 0:
            return exit_refs[which]
        return exit_cols(which, device(spot - turn * step))

    def exit_copy(which, step, shift=0):
        there = exit_cols(which, device(spot - turn * (step + shift)))
        src = there if shift else exit_source(which, step)
        at = (step, which)
        return send_to(
            src, there, exit_send.at[at], exit_recv.at[at], {"sp": device(spot + turn)}
        )

    def pass_copy(which, step, incoming=False):
        if incoming:
            there = exit_cols(which, device(spot + turn * step) + 1 - 2 * core)
            src = there
        else:
            there = exit_cols(which, device(spot - turn * step))
            src = exit_source(which, step)
        at = (step, which)
        return send_to(src, there, pass_send.at[at], pass_recv.at[at], {"sp": mate})

    exit_own_copies = [
        pltpu.make_async_copy(exit_refs[which], exit_cols(which, me), exit_own.at[which])
        for which in range(2)
    ]

    def start_exit():
        for which in range(2):
            exit_copy(which, 0).start()
        for which in range(2):
            pass_copy(which, 0).start()
            exit_own_copies[which].start()

    def advance_exit(step):
        for which in range(2):
            exit_copy(which, step, 1).wait_recv()
            if step < hops - 1:
                exit_copy(which, step + 1).start()
            pass_copy(which, step + 1).start()

    start_group(0)
    mine = pl.ds(pl.multiple_of(HALO + own_rows * tp_me, HALO), own_rows)
    across = send_to(x_ref, raw.at[mine], x_send.at[0], x_recv.at[0], {"tp": 1 - tp_me})
    across.start()
    here = pltpu.make_async_copy(x_ref, raw.at[mine], x_own)
    here.start()
    before, after = pl.ds(0, HALO), pl.ds(HALO + length, HALO)

    def halo(t, low):
        if low:
            return send_to(
                x_ref.at[pl.ds(own_rows - HALO, HALO)], raw.at[before],
                x_send.at[1 + t], x_recv.at[1], {"sp": up, "tp": t},
            )
        return send_to(
            x_ref.at[pl.ds(0, HALO)], raw.at[after],
            x_send.at[1 + t], x_recv.at[2], {"sp": down, "tp": t},
        )

    sends_up = jnp.logical_and(tp_me == 1, me < n - 1)
    sends_down = jnp.logical_and(tp_me == 0, me > 0)

    @pl.when(sends_up)
    def _():
        for t in range(2):
            halo(t, True).start()

    @pl.when(sends_down)
    def _():
        for t in range(2):
            halo(t, False).start()

    @pl.when(me == 0)
    def _():
        raw[0:HALO, :] = jnp.zeros((HALO, width), BF16)

    @pl.when(me == n - 1)
    def _():
        raw[HALO + length :, :] = jnp.zeros((HALO, width), BF16)

    def make_normed():
        here.wait()
        across.wait()

        @pl.when(me > 0)
        def _():
            halo(0, True).wait_recv()

        @pl.when(me < n - 1)
        def _():
            halo(0, False).wait_recv()

        @pl.when(sends_up)
        def _():
            for t in range(2):
                halo(t, True).wait_send()

        @pl.when(sends_down)
        def _():
            for t in range(2):
                halo(t, False).wait_send()

        gain = gain_ref[...].astype(F32)
        tall = 2 * HALO

        def norm_block(i, _):
            at = pl.ds(pl.multiple_of(i * tall, tall), tall)
            x32 = raw[at, :].astype(F32)
            scale = lax.rsqrt(jnp.mean(x32 * x32, axis=-1, keepdims=True) + epsilon)
            normed[at, :] = (x32 * scale * gain).astype(BF16)
            return 0

        lax.fori_loop(0, raw.shape[0] // tall, norm_block, 0)

    def make_tables():
        heads = spike_ref.shape[0]
        raw_step = lax.dot_general(
            normed[HALO : HALO + length, :], step_ref[...],
            (((1,), (1,)), ((), ())), preferred_element_type=F32,
        ).astype(BF16)
        lanes = table_ref.shape[1]
        row = lax.broadcasted_iota(jnp.int32, (2 * heads, lanes), 0)
        col = lax.broadcasted_iota(jnp.int32, (2 * heads, lanes), 1)
        pick = jnp.where((row % heads == col // 4) & (row // heads == col % 2), 1.0, 0.0)
        head_row = lax.broadcasted_iota(jnp.int32, (heads, lanes), 0)
        head_col = lax.broadcasted_iota(jnp.int32, (heads, lanes), 1)
        spread = jnp.where(head_row == head_col // 4, 1.0, 0.0).astype(F32)
        deltas = softplus(jnp.dot(raw_step, pick.astype(BF16), preferred_element_type=F32))
        rates = jnp.dot(rate_ref[...], spread, precision=HIGHEST, preferred_element_type=F32)
        side = lax.broadcasted_iota(jnp.int32, (2, lanes), 0)
        kind2 = lax.broadcasted_iota(jnp.int32, (2, lanes), 1) % 2
        rates = jnp.sum(jnp.where(side == kind2, rates, 0.0), axis=0, keepdims=True)
        spikes = lax.dot_general(
            spike_ref[...], spread, (((0,), (0,)), ((), ())),
            precision=HIGHEST, preferred_element_type=F32,
        )
        logs = spikes - deltas * rates
        t_at = lax.broadcasted_iota(jnp.int32, (length, length), 0)
        s_at = lax.broadcasted_iota(jnp.int32, (length, length), 1)
        tri = jnp.where(t_at >= s_at, 1.0, 0.0).astype(F32)
        run_f = jnp.dot(tri, logs, precision=HIGHEST, preferred_element_type=F32)
        tri = jnp.where(t_at <= s_at, 1.0, 0.0).astype(F32)
        run_b = jnp.dot(tri, logs, precision=HIGHEST, preferred_element_type=F32)
        kind = lax.broadcasted_iota(jnp.int32, (length, lanes), 1) % 4
        table = jnp.where(kind < 2, deltas, jnp.where(kind == 2, run_f, run_b))
        table_ref[...] = table
        turned_ref[...] = table.T
        ends = jnp.where(kind[0:1] == 2, run_f[length - 1 : length], run_b[0:1])
        ends_ref[...] = jnp.broadcast_to(ends, ends_ref.shape)

    def project_group(g):
        def arrived(step, _):
            for way in range(2):
                mate_copy(g, step, way, True).wait_recv()
            return 0

        lax.fori_loop(0, chips, arrived, 0)
        tile = group_cols // 3

        def project_tile(i, _):
            cols = pl.ds(pl.multiple_of(i * tile, STATE), tile)
            proj[g, :, cols] = jnp.dot(
                normed[...], w_buf[g, :, cols], preferred_element_type=F32
            ).astype(BF16)
            return 0

        lax.fori_loop(0, 3, project_tile, 0)

    def log_copy(k, incoming=False):
        there = (me + n - k) % n if incoming else (me + k) % n
        slot = there if incoming else me
        return send_to(ends_ref, logs.at[slot], l_out.at[k], l_in.at[k], {"sp": there})

    inner = slice(HALO, HALO + length)
    at_ig, at_va, at_gate = cw, 2 * cw, 3 * cw
    at_x = at_gate + pw
    at_b = at_x + pw
    at_c = at_b + sw

    def rows_f32(j, wide, base):
        return proj[j, :, base : base + wide].astype(F32)

    def state_copy(owner):
        return send_to(
            states.at[owner], got.at[me], s_out.at[owner], s_in.at[me], {"sp": owner}
        )

    def mix_pair(j):
        t_at = lax.broadcasted_iota(jnp.int32, (length, length), 0)
        s_at = lax.broadcasted_iota(jnp.int32, (length, length), 1)
        below, above = t_at > s_at, t_at < s_at
        taps = ct_ref[:, j * cw : (j + 1) * cw].astype(F32)
        gated = rows_f32(j, cw, at_ig) * rows_f32(j, cw, at_va)
        conv = tap_sum(
            gated.astype(BF16).astype(F32), [taps[k : k + 1] for k in range(taps.shape[0])], length
        )
        og = proj[j, inner, 0:cw].astype(F32)
        y_c[:, j * cw : (j + 1) * cw] = (og * conv).astype(BF16)
        taps = xt_ref[:, j * pw : (j + 1) * pw].astype(F32)
        xs = silu(
            tap_sum(
                rows_f32(j, pw, at_x), [taps[k : k + 1] for k in range(taps.shape[0])], length
            )
        ).astype(BF16)
        taps = [lt_ref[k, :, j * sw : (j + 1) * sw].astype(F32) for k in range(lt_ref.shape[0])]
        bs = silu(
            tap_sum(rows_f32(j, sw, at_b), [tap[0:1] for tap in taps], length)
        ).astype(BF16)
        cs = silu(
            tap_sum(rows_f32(j, sw, at_c), [tap[1:2] for tap in taps], length)
        ).astype(BF16)
        reads[:, j * sw : (j + 1) * sw] = cs
        outs = []
        for h in range(2):
            c_h = cs[:, h * STATE : (h + 1) * STATE]
            b_h = bs[:, h * STATE : (h + 1) * STATE]
            x_h = xs[:, h * HEAD_DIM : (h + 1) * HEAD_DIM]
            head = 2 * j + h
            cols = table_ref[:, 4 * head : 4 * head + 4]
            rows = turned_ref[4 * head : 4 * head + 4, :]
            scores = lax.dot_general(
                c_h, b_h, (((1,), (1,)), ((), ())), preferred_element_type=F32
            )
            gap = jnp.where(above, cols[:, 3:4] - rows[3:4], cols[:, 2:3] - rows[2:3])
            d_f, d_b = rows[0:1], rows[1:2]
            scale = jnp.where(below, d_f, jnp.where(above, d_b, d_f + d_b))
            w = (scores * jnp.exp(gap) * scale).astype(BF16)
            outs.append(jnp.dot(w, x_h, preferred_element_type=F32))
            x32 = x_h.astype(F32)
            end_f = jnp.exp(rows[2:3, length - 1 : length] - cols[:, 2:3])
            end_b = jnp.exp(rows[3:4, 0:1] - cols[:, 3:4])
            both = jnp.concatenate(
                [x32 * (end_f * cols[:, 0:1]), x32 * (end_b * cols[:, 1:2])], axis=1
            ).astype(BF16)
            state = lax.dot_general(
                both, b_h, (((0,), (0,)), ((), ())), preferred_element_type=F32
            ).astype(BF16)
            for d in range(2):
                states[2 * head + d] = state[d * HEAD_DIM : (d + 1) * HEAD_DIM]
        within[:, j * pw : (j + 1) * pw] = jnp.concatenate(outs, axis=1)

    def send_states(j):
        for owner in range(4 * j, 4 * j + 4):
            @pl.when(me != owner)
            def _():
                state_copy(owner).start()

            @pl.when(me == owner)
            def _():
                got[owner] = states[owner]

    def send_logs():
        for k in range(1, n):
            log_copy(k).start()
        logs[me] = ends_ref[...]

    def project_then(g):
        return lambda: project_group(g)

    def mix_then(g):
        def run():
            mix_pair(g)
            send_states(g)

        return run

    units = {LAG + 1: make_normed, LAG + 2: make_tables, LAG + 3: send_logs}
    for g in range(pairs):
        units[SKEW * g + hops] = project_then(g)
        units[SKEW * g + hops + 1] = mix_then(g)
    exit_slot = SKEW * (pairs - 1) + hops - 1
    last_mix = SKEW * (pairs - 1) + hops + 1

    def slot(t):
        for g in range(pairs):
            if g > 0 and t == SKEW * g - 1:
                start_group(g)
            if 0 <= t - SKEW * g < hops:
                advance_group(g, t - SKEW * g)
        if t == exit_slot - 1:
            start_exit()
        if 0 <= t - exit_slot < hops:
            advance_exit(t - exit_slot)
        if t in units:
            units[t]()

    for t in range(last_mix + 2):
        slot(t)

    for k in range(1, n):
        log_copy(k, True).wait_recv()
    lane = 4 * (me // 2) + 2 + me % 2
    lane_at = lax.broadcasted_iota(jnp.int32, (1, STATE), 1)
    for k in range(1, n):
        other = (me + k) % n
        send_to(
            states.at[other], got.at[other], s_out.at[other], s_in.at[other], {"sp": other}
        ).wait_recv()
    back = me % 2
    acc = jnp.zeros(got.shape[1:], F32)
    for i in range(n):
        j = back * (n - 1 - i) + (1 - back) * i
        enter[j] = acc.astype(BF16)
        log = jnp.sum(
            jnp.where(lane_at == lane, logs[j][0:1, :], 0.0), axis=1, keepdims=True
        )
        acc = acc * jnp.exp(log) + got[j].astype(F32)
    entered[me] = enter[me]

    def enter_copy(k, incoming=False):
        there = (me + n - k) % n if incoming else (me + k) % n
        slot = there if incoming else me
        return send_to(enter.at[there], entered.at[slot], e_out.at[k], e_in.at[k], {"sp": there})

    for k in range(1, n):
        enter_copy(k).start()
    for t in range(last_mix + 2, exit_slot + hops):
        slot(t)
    for k in range(1, n):
        enter_copy(k, True).wait_recv()

    for j in range(pairs):
        outs = []
        gate = silu(rows_f32(j, pw, at_gate)[inner])
        for h in range(2):
            head = 2 * j + h
            cols = table_ref[:, 4 * head : 4 * head + 4]
            wide = jnp.concatenate([entered[2 * head], entered[2 * head + 1]], axis=0)
            both = lax.dot_general(
                reads[:, head * STATE : (head + 1) * STATE], wide,
                (((1,), (1,)), ((), ())), preferred_element_type=F32,
            )
            mine = slice(h * HEAD_DIM, (h + 1) * HEAD_DIM)
            y = within[:, head * HEAD_DIM : (head + 1) * HEAD_DIM]
            y = y + both[:, :HEAD_DIM] * jnp.exp(cols[:, 2:3])
            y = y + both[:, HEAD_DIM:] * jnp.exp(cols[:, 3:4])
            g = y * gate[:, mine]
            g = g * lax.rsqrt(jnp.mean(g * g, axis=-1, keepdims=True) + epsilon)
            gain = head_gain_ref[:, head * HEAD_DIM : (head + 1) * HEAD_DIM].astype(F32)
            outs.append(g * gain)
        y_s[:, j * pw : (j + 1) * pw] = jnp.concatenate(outs, axis=1).astype(BF16)
    for which in range(2):
        exit_own_copies[which].wait()
        for step in range(chips):
            pass_copy(which, step, True).wait_recv()

    part = width // BLOCKS

    def partial(owner, block):
        rows = pl.ds(pl.multiple_of(owner * own_rows, HALO), own_rows)
        cols = slice(block * part, (block + 1) * part)
        return jnp.dot(
            y_c[rows, :], c_all[:, cols], preferred_element_type=F32
        ) + jnp.dot(y_s[rows, :], s_all[:, cols], preferred_element_type=F32)

    def partial_copy(block):
        return send_to(
            away.at[block], came.at[block], p_out.at[block], p_in.at[block], {"tp": 1 - tp_me}
        )

    for block in range(BLOCKS):
        away[block] = partial(1 - tp_me, block).astype(BF16)
        partial_copy(block).start()
    for block in range(BLOCKS):
        kept = partial(tp_me, block)
        partial_copy(block).wait_recv()
        cols = slice(block * part, (block + 1) * part)
        out_ref[:, cols] = (kept + came[block].astype(F32)).astype(BF16)
    for block in range(BLOCKS):
        partial_copy(block).wait_send()
    for k in range(1, n):
        log_copy(k).wait_send()
        enter_copy(k).wait_send()
        other = (me + k) % n
        state_copy(other).wait_send()
    for step in range(chips):
        for which in range(2):
            if step < hops:
                exit_copy(which, step).wait_send()
            pass_copy(which, step).wait_send()

    def drain(step, _):
        for g in range(pairs):
            for way in range(2):
                @pl.when(step < hops)
                def _():
                    ring_copy(g, step, way).wait_send()

                mate_copy(g, step, way).wait_send()
        return 0

    lax.fori_loop(0, chips, drain, 0)


def mixer(
    rows, gain, conv_w, rec_w, lat_w, step_w, rate, spike,
    conv_taps, x_taps, latent_taps, head_gain, exit_c, exit_s,
):
    n = lax.axis_size("sp")
    chips = n // 2
    hops = chips - 1
    own_rows, width = rows.shape
    length = 2 * own_rows
    full = length + 2 * HALO
    depth = conv_w.shape[1]
    blocks = sum(w.shape[0] for w in (conv_w, rec_w, lat_w))
    cols = sum(w.shape[0] * w.shape[2] for w in (conv_w, rec_w, lat_w))
    heads = spike.shape[0]
    pairs = heads // 2
    conv_width, ssd_width = exit_c.shape[0], exit_s.shape[0]
    state_width = latent_taps.shape[2]
    assert 4 * heads <= STATE and 2 * heads == n and conv_width == ssd_width
    vmem = pl.BlockSpec(memory_space=pltpu.VMEM)
    hbm = pl.BlockSpec(memory_space=pl.ANY)
    spans = (n, HEAD_DIM, STATE)
    parts = (BLOCKS, own_rows, width // BLOCKS)
    dma = pltpu.SemaphoreType.DMA
    return pl.pallas_call(
        functools.partial(mixer_kernel, n),
        out_shape=jax.ShapeDtypeStruct((own_rows, width), BF16),
        in_specs=[vmem, vmem, hbm, hbm, hbm] + [vmem] * 9,
        out_specs=vmem,
        scratch_shapes=[
            pltpu.VMEM((pairs, n * depth, cols // pairs), BF16),
            pltpu.VMEM((full, width), BF16),
            pltpu.VMEM((full, width), BF16),
            pltpu.VMEM((pairs, full, cols // pairs), BF16),
            pltpu.VMEM((length, STATE), F32),
            pltpu.VMEM((STATE, length), F32),
            pltpu.VMEM((8, STATE), F32),
            pltpu.VMEM((conv_width, width), BF16),
            pltpu.VMEM((ssd_width, width), BF16),
            pltpu.VMEM((length, conv_width), BF16),
            pltpu.VMEM((length, ssd_width), BF16),
            pltpu.VMEM((length, ssd_width), F32),
            pltpu.VMEM((length, state_width), BF16),
            pltpu.VMEM(spans, BF16),
            pltpu.VMEM(spans, BF16),
            pltpu.VMEM((n, 8, STATE), F32),
            pltpu.VMEM(spans, BF16),
            pltpu.VMEM(spans, BF16),
            pltpu.VMEM(parts, BF16),
            pltpu.VMEM(parts, BF16),
            dma((pairs * blocks,)), dma((2,)), dma, dma((3,)), dma((3,)),
            dma((pairs, hops, 2)), dma((pairs, hops, 2)),
            dma((pairs, chips, 2)), dma((pairs, chips, 2)),
            dma((hops, 2)), dma((hops, 2)), dma((chips, 2)), dma((chips, 2)),
        ]
        + [dma((n,))] * 6
        + [dma((BLOCKS,))] * 2,
        compiler_params=pltpu.CompilerParams(
            collective_id=2, has_side_effects=True, vmem_limit_bytes=58 * 2**20
        ),
        cost_estimate=pl.CostEstimate(
            flops=2 * full * width * cols, bytes_accessed=2 * width * cols, transcendentals=0
        ),
    )(
        rows, gain.reshape(1, -1), conv_w, rec_w, lat_w, step_w, rate, spike,
        conv_taps, x_taps, latent_taps, head_gain.reshape(1, -1), exit_c, exit_s,
    )


def project_kernel(r_ref, w_ref, o_ref):
    o_ref[...] = jnp.dot(r_ref[...], w_ref[...], preferred_element_type=F32).astype(BF16)


def project(rows, weights):
    count, width = rows.shape
    cols = weights.shape[1]
    tile = cols // 9
    return pl.pallas_call(
        project_kernel,
        grid=(9,),
        in_specs=[
            pl.BlockSpec((count, width), lambda j: (0, 0)),
            pl.BlockSpec((width, tile), lambda j: (0, j)),
        ],
        out_specs=pl.BlockSpec((count, tile), lambda j: (0, j)),
        out_shape=jax.ShapeDtypeStruct((count, cols), BF16),
        cost_estimate=pl.CostEstimate(
            flops=2 * count * width * cols, bytes_accessed=2 * width * cols, transcendentals=0
        ),
    )(rows, weights)


def finish_kernel(within_ref, reads_ref, enter_ref, gate_ref, gain_ref, col_ref, y_ref):
    length = y_ref.shape[0]
    cols = col_ref[0]
    outs = []
    for h in range(2):
        o = 4 * h
        both = lax.dot_general(
            reads_ref[:, h * STATE : (h + 1) * STATE],
            enter_ref[h * STATE : (h + 1) * STATE],
            (((1,), (1,)), ((), ())),
            preferred_element_type=F32,
        )
        here = slice(h * HEAD_DIM, (h + 1) * HEAD_DIM)
        y = within_ref[:, here]
        y = y + both[:, :HEAD_DIM] * jnp.exp(cols[:, o + 2 : o + 3])
        y = y + both[:, HEAD_DIM:] * jnp.exp(cols[:, o + 3 : o + 4])
        g = y * silu(gate_ref[pl.ds(HALO, length), :].astype(F32)[:, here])
        g = g * lax.rsqrt(jnp.mean(g * g, axis=-1, keepdims=True) + epsilon)
        outs.append(g * gain_ref[:, here].astype(F32))
    y_ref[...] = jnp.concatenate(outs, axis=1).astype(BF16)


def local(
    layer_source_rows, entry_rescale_factor, sliding_mixer_entry_matrix,
    recurrent_mixer_entry_matrix, latent_write_read_matrix, timestep_matrix,
    sliding_kernel_coefficients, recurrent_kernel_coefficients, latent_kernel_coefficients,
    lane_forgetting_rate, spike_forgetting_rate, lane_rescale_factor,
    sliding_mixer_exit_matrix, recurrent_mixer_exit_matrix,
):
    n = lax.axis_size("sp")
    tp = lax.axis_size("tp")
    own_rows, width = layer_source_rows.shape
    length = own_rows * tp
    full = length + 2 * HALO
    conv_width = sliding_mixer_entry_matrix.shape[2]
    ssd_width = recurrent_mixer_entry_matrix.shape[2]
    state_width = latent_write_read_matrix.shape[2]
    heads = timestep_matrix.shape[2]
    pairs = heads // 2
    cw = conv_width // pairs

    share = heads * 2 * HEAD_DIM // n
    if tp == 2 and 2 * heads == n:
        return mixer(
            layer_source_rows, entry_rescale_factor, sliding_mixer_entry_matrix,
            recurrent_mixer_entry_matrix, latent_write_read_matrix,
            timestep_matrix.transpose(1, 2, 0).reshape(2 * heads, width),
            lane_forgetting_rate, spike_forgetting_rate.T, sliding_kernel_coefficients,
            recurrent_kernel_coefficients, latent_kernel_coefficients, lane_rescale_factor,
            sliding_mixer_exit_matrix, recurrent_mixer_exit_matrix,
        )

    block = jnp.concatenate(
        [sliding_mixer_entry_matrix[i] for i in range(3)]
        + [recurrent_mixer_entry_matrix[i] for i in range(2)]
        + [latent_write_read_matrix[i] for i in range(2)],
        axis=1,
    )
    gathered = gather_rows(block)
    weights = gathered.reshape(n * block.shape[0], block.shape[1])

    x32 = layer_source_rows.astype(F32)
    normed = (
        x32
        * lax.rsqrt(jnp.mean(x32 * x32, axis=-1, keepdims=True) + epsilon)
        * entry_rescale_factor.astype(F32)
    ).astype(BF16)
    up = [(i, i + 1) for i in range(n - 1)]
    down = [(i + 1, i) for i in range(n - 1)]
    before = lax.ppermute(normed[own_rows - HALO :], "sp", up)
    after = lax.ppermute(normed[:HALO], "sp", down)
    shared = lax.all_gather(jnp.concatenate([before, normed, after], axis=0), "tp", axis=0)
    rows = jnp.concatenate(
        [shared[tp - 1, :HALO]]
        + [shared[i, HALO : HALO + own_rows] for i in range(tp)]
        + [shared[0, HALO + own_rows :]],
        axis=0,
    )

    step_weight = timestep_matrix.reshape(width, 2 * heads)
    raw = jnp.dot(rows, step_weight, preferred_element_type=F32).astype(BF16)
    raw = raw[HALO : HALO + length].astype(F32).reshape(length, 2, heads)
    deltas = jax.nn.softplus(raw)
    logs = -deltas * lane_forgetting_rate[None] + spike_forgetting_rate[:, None, :]
    tri = (jnp.arange(length)[:, None] >= jnp.arange(length)[None, :]).astype(F32)
    run_f = jnp.dot(tri, logs[:, 0], precision=HIGHEST)
    run_b = jnp.dot(tri.T, logs[:, 1], precision=HIGHEST)
    table = jnp.stack([deltas[:, 0], deltas[:, 1], run_f, run_b], axis=2)
    col_table = table.reshape(length, pairs, 8).transpose(1, 0, 2)
    row_table = table.reshape(length, pairs, 8).transpose(1, 2, 0)
    span_log = jnp.stack([run_f[length - 1], run_b[0]], axis=1)
    exit_c, exit_s, weights = lax.optimization_barrier(
        (sliding_mixer_exit_matrix, recurrent_mixer_exit_matrix, weights)
    )
    proj = project(rows, weights)
    exit_c = lax.all_gather(exit_c, "sp", axis=1, tiled=True)
    exit_s = lax.all_gather(exit_s, "sp", axis=1, tiled=True)

    latent = latent_kernel_coefficients
    pw, sw = 2 * HEAD_DIM, 2 * STATE
    g0 = 3 * conv_width
    at_gate, at_x = g0 // pw, (g0 + ssd_width) // pw
    at_b = (g0 + 2 * ssd_width) // sw
    at_c = at_b + pairs
    y_conv, within, reads, states = pl.pallas_call(
        mix_kernel,
        grid=(pairs,),
        in_specs=[
            pl.BlockSpec((full, cw), lambda j: (0, j)),
            pl.BlockSpec((full, cw), lambda j: (0, pairs + j)),
            pl.BlockSpec((full, cw), lambda j: (0, 2 * pairs + j)),
            pl.BlockSpec((full, pw), lambda j: (0, at_x + j)),
            pl.BlockSpec((full, sw), lambda j: (0, at_b + j)),
            pl.BlockSpec((full, sw), lambda j: (0, at_c + j)),
            pl.BlockSpec((3, cw), lambda j: (0, j)),
            pl.BlockSpec((5, pw), lambda j: (0, j)),
            pl.BlockSpec((5, sw), lambda j: (0, j)),
            pl.BlockSpec((5, sw), lambda j: (0, pairs + j)),
            pl.BlockSpec((1, length, 8), lambda j: (j, 0, 0)),
            pl.BlockSpec((1, 8, length), lambda j: (j, 0, 0)),
        ],
        out_specs=[
            pl.BlockSpec((length, cw), lambda j: (0, j)),
            pl.BlockSpec((length, pw), lambda j: (0, j)),
            pl.BlockSpec((length, sw), lambda j: (0, j)),
            pl.BlockSpec((sw, STATE), lambda j: (j, 0)),
        ],
        out_shape=[
            jax.ShapeDtypeStruct((length, conv_width), BF16),
            jax.ShapeDtypeStruct((length, ssd_width), F32),
            jax.ShapeDtypeStruct((length, state_width), BF16),
            jax.ShapeDtypeStruct((pairs * sw, STATE), BF16),
        ],
        cost_estimate=pl.CostEstimate(
            flops=8 * length * length * heads * STATE, bytes_accessed=2**24, transcendentals=0
        ),
    )(
        proj, proj, proj, proj, proj, proj,
        sliding_kernel_coefficients, recurrent_kernel_coefficients,
        latent.reshape(latent.shape[0], -1), latent.reshape(latent.shape[0], -1),
        col_table, row_table,
    )

    entering = exchange_states(states.reshape(n, share, STATE), span_log)
    entering = entering.reshape(pairs * sw, STATE)

    y_ssd = pl.pallas_call(
        finish_kernel,
        grid=(pairs,),
        in_specs=[
            pl.BlockSpec((length, pw), lambda j: (0, j)),
            pl.BlockSpec((length, sw), lambda j: (0, j)),
            pl.BlockSpec((sw, STATE), lambda j: (j, 0)),
            pl.BlockSpec((full, pw), lambda j: (0, at_gate + j)),
            pl.BlockSpec((1, pw), lambda j: (0, j)),
            pl.BlockSpec((1, length, 8), lambda j: (j, 0, 0)),
        ],
        out_specs=pl.BlockSpec((length, pw), lambda j: (0, j)),
        out_shape=jax.ShapeDtypeStruct((length, ssd_width), BF16),
    )(within, reads, entering, proj, lane_rescale_factor.reshape(1, -1), col_table)

    def partial(y_c, y_s):
        return (
            jnp.dot(y_c, exit_c, preferred_element_type=F32)
            + jnp.dot(y_s, exit_s, preferred_element_type=F32)
        ).astype(BF16)

    if tp != 2:
        return lax.psum_scatter(
            partial(y_conv, y_ssd), "tp", scatter_dimension=0, tiled=True
        )
    tp_me = lax.axis_index("tp")

    def rows_of(owner, y):
        return lax.dynamic_slice_in_dim(y, owner * own_rows, own_rows, axis=0)

    away = partial(rows_of(1 - tp_me, y_conv), rows_of(1 - tp_me, y_ssd))
    arrived = lax.ppermute(away, "tp", [(0, 1), (1, 0)])
    kept = partial(rows_of(tp_me, y_conv), rows_of(tp_me, y_ssd))
    return (kept.astype(F32) + arrived.astype(F32)).astype(BF16)


def solution(mesh):
    placed = (
        P(("sp", "tp"), None),
        P(),
        P(None, "sp", "tp"),
        P(None, "sp", "tp"),
        P(None, "sp", "tp"),
        P(None, None, "tp"),
        P(None, "tp"),
        P(None, "tp"),
        P(None, None, "tp"),
        P(None, "tp"),
        P("sp", "tp"),
        P("tp"),
        P("tp", "sp"),
        P("tp", "sp"),
    )
    return jax.shard_map(
        local, mesh=mesh, in_specs=placed, out_specs=P(("sp", "tp"), None), check_vma=False
    )
```

```python
import functools

import jax
import jax.numpy as jnp
from jax import lax
from jax.experimental import pallas as pl
from jax.experimental.pallas import tpu as pltpu
from jax.sharding import PartitionSpec as P

HEAD_DIM = 64
STATE = 128
HALO = 16
CHUNKS = 2
LAG = 2
SKEW = 1
EXIT_LAG = 6
AHEAD = 1
AWAIT = 2
epsilon = 1e-05
F32 = jnp.float32
BF16 = jnp.bfloat16
HIGHEST = lax.Precision.HIGHEST


def ring_kernel(n, w_ref, out_ref, own_sem, ring_send, ring_recv, mate_send, mate_recv):
    chips = n // 2
    me = lax.axis_index("sp")
    core, chip = me % 2, me // 2
    odd = chip % 2
    spot = (1 - odd) * (chip // 2) + odd * (chips - 1 - chip // 2)

    def device(position):
        position = (position + 2 * chips) % chips
        half = (chips + 1) // 2
        late = position // half
        late_chip = 2 * (chips - 1 - position) + 1
        return 2 * ((1 - late) * 2 * position + late * late_chip) + core

    mate = me + 1 - 2 * core
    ways = (device(spot + 1), device(spot - 1))
    rows = w_ref.shape[0] // (2 * CHUNKS)

    barrier = pltpu.get_barrier_semaphore()
    for other in (mate,) + ways:
        pl.semaphore_signal(
            barrier, inc=1, device_id={"sp": other}, device_id_type=pl.DeviceIdType.MESH
        )
    pl.semaphore_wait(barrier, 3)

    def piece(way, chunk):
        return pl.ds((way * CHUNKS + chunk) * rows, rows)

    def ring_copy(step, way, chunk):
        owner = device(spot - step if way == 0 else spot + step)
        part = piece(way, chunk)
        return pltpu.make_async_remote_copy(
            src_ref=w_ref.at[part] if step == 0 else out_ref.at[owner, part],
            dst_ref=out_ref.at[owner, part],
            send_sem=ring_send.at[step, way, chunk],
            recv_sem=ring_recv.at[step, way, chunk],
            device_id={"sp": ways[way]},
            device_id_type=pl.DeviceIdType.MESH,
        )

    def arrival(step, way, chunk):
        owner = device(spot - step - 1 if way == 0 else spot + step + 1)
        part = piece(way, chunk)
        return pltpu.make_async_remote_copy(
            src_ref=out_ref.at[owner, part],
            dst_ref=out_ref.at[owner, part],
            send_sem=ring_send.at[step, way, chunk],
            recv_sem=ring_recv.at[step, way, chunk],
            device_id={"sp": ways[way]},
            device_id_type=pl.DeviceIdType.MESH,
        )

    def mate_copy(step, way, chunk, incoming=False):
        owner = device(spot - step if way == 0 else spot + step)
        if incoming:
            owner = owner + 1 - 2 * core
        part = piece(way, chunk)
        return pltpu.make_async_remote_copy(
            src_ref=w_ref.at[part] if step == 0 else out_ref.at[owner, part],
            dst_ref=out_ref.at[owner, part],
            send_sem=mate_send.at[step, way, chunk],
            recv_sem=mate_recv.at[step, way, chunk],
            device_id={"sp": mate},
            device_id_type=pl.DeviceIdType.MESH,
        )

    parts = [(way, chunk) for chunk in range(CHUNKS) for way in range(2)]
    for way, chunk in parts:
        ring_copy(0, way, chunk).start()
    for way, chunk in parts:
        mate_copy(0, way, chunk).start()
    own = pltpu.make_async_copy(w_ref, out_ref.at[me], own_sem)
    own.start()
    for step in range(chips - 1):
        for way, chunk in parts:
            arrival(step, way, chunk).wait_recv()
            if step < chips - 2:
                ring_copy(step + 1, way, chunk).start()
            mate_copy(step + 1, way, chunk).start()
    own.wait()
    for step in range(chips):
        for way, chunk in parts:
            if step < chips - 1:
                ring_copy(step, way, chunk).wait_send()
            mate_copy(step, way, chunk).wait_send()
            mate_copy(step, way, chunk, True).wait_recv()


def gather_rows(block):
    n = lax.axis_size("sp")
    chips = n // 2
    rows, cols = block.shape
    return pl.pallas_call(
        functools.partial(ring_kernel, n),
        out_shape=jax.ShapeDtypeStruct((n, rows, cols), block.dtype),
        in_specs=[pl.BlockSpec(memory_space=pltpu.VMEM)],
        out_specs=pl.BlockSpec(memory_space=pl.ANY),
        scratch_shapes=[
            pltpu.SemaphoreType.DMA,
            pltpu.SemaphoreType.DMA((chips - 1, 2, CHUNKS)),
            pltpu.SemaphoreType.DMA((chips - 1, 2, CHUNKS)),
            pltpu.SemaphoreType.DMA((chips, 2, CHUNKS)),
            pltpu.SemaphoreType.DMA((chips, 2, CHUNKS)),
        ],
        compiler_params=pltpu.CompilerParams(
            collective_id=0, has_side_effects=True, vmem_limit_bytes=16 * 2**20
        ),
        cost_estimate=pl.CostEstimate(
            flops=0, bytes_accessed=n * rows * cols * 16, transcendentals=0
        ),
    )(block)


def taps_of(padded, table, length):
    full = padded.shape[0]
    half = table.shape[0] // 2
    total = None
    for k in range(table.shape[0]):
        moved = padded if k == half else pltpu.roll(padded, (half - k) % full, 0)
        term = moved[HALO : HALO + length] * table[k : k + 1].astype(F32)
        total = term if total is None else total + term
    return total


def silu(v):
    return v * jax.nn.sigmoid(v)


def mix_kernel(
    og_ref, ig_ref, va_ref, x_ref, b_ref, c_ref, ct_ref, xt_ref, bt_ref, rt_ref,
    col_ref, row_ref, yconv_ref, within_ref, reads_ref, state_ref,
):
    length = yconv_ref.shape[0]
    gated = (ig_ref[...].astype(F32) * va_ref[...].astype(F32)).astype(BF16).astype(F32)
    conv = taps_of(gated, ct_ref[...], length)
    yconv_ref[...] = (og_ref[pl.ds(HALO, length), :].astype(F32) * conv).astype(BF16)
    xs = silu(taps_of(x_ref[...].astype(F32), xt_ref[...], length)).astype(BF16)
    bs = silu(taps_of(b_ref[...].astype(F32), bt_ref[...], length)).astype(BF16)
    cs = silu(taps_of(c_ref[...].astype(F32), rt_ref[...], length)).astype(BF16)
    reads_ref[...] = cs
    cols = col_ref[0]
    rows = row_ref[0]
    t_at = lax.broadcasted_iota(jnp.int32, (length, length), 0)
    s_at = lax.broadcasted_iota(jnp.int32, (length, length), 1)
    outs, weighted = [], []
    for h in range(2):
        c_h = cs[:, h * STATE : (h + 1) * STATE]
        b_h = bs[:, h * STATE : (h + 1) * STATE]
        x_h = xs[:, h * HEAD_DIM : (h + 1) * HEAD_DIM]
        o = 4 * h
        scores = lax.dot_general(
            c_h, b_h, (((1,), (1,)), ((), ())), preferred_element_type=F32
        )
        gap = jnp.where(
            t_at >= s_at,
            cols[:, o + 2 : o + 3] - rows[o + 2 : o + 3],
            cols[:, o + 3 : o + 4] - rows[o + 3 : o + 4],
        )
        d_f, d_b = rows[o : o + 1], rows[o + 1 : o + 2]
        scale = jnp.where(t_at > s_at, d_f, jnp.where(t_at < s_at, d_b, d_f + d_b))
        w = (scores * jnp.exp(gap) * scale).astype(BF16)
        outs.append(jnp.dot(w, x_h, preferred_element_type=F32))
        x32 = x_h.astype(F32)
        end_f = jnp.exp(rows[o + 2 : o + 3, length - 1 : length] - cols[:, o + 2 : o + 3])
        end_b = jnp.exp(rows[o + 3 : o + 4, 0:1] - cols[:, o + 3 : o + 4])
        both = jnp.concatenate(
            [x32 * (end_f * cols[:, o : o + 1]), x32 * (end_b * cols[:, o + 1 : o + 2])], axis=1
        ).astype(BF16)
        state_ref[h * STATE : (h + 1) * STATE] = lax.dot_general(
            both, b_h, (((0,), (0,)), ((), ())), preferred_element_type=F32
        ).astype(BF16)
    within_ref[...] = jnp.concatenate(outs, axis=1)


def exchange_kernel(
    n, share, s_ref, l_ref, out_ref, got, logs, enter, s_out, s_in, l_out, l_in, e_out, e_in
):
    me = lax.axis_index("sp")
    barrier = pltpu.get_barrier_semaphore()
    for k in range(1, n):
        pl.semaphore_signal(
            barrier,
            inc=1,
            device_id={"sp": (me + k) % n},
            device_id_type=pl.DeviceIdType.MESH,
        )
    pl.semaphore_wait(barrier, n - 1)

    def copy(src, dst, out_sem, in_sem, k, there, slot):
        return pltpu.make_async_remote_copy(
            src_ref=src.at[there],
            dst_ref=dst.at[slot],
            send_sem=out_sem.at[k],
            recv_sem=in_sem.at[k],
            device_id={"sp": there},
            device_id_type=pl.DeviceIdType.MESH,
        )

    for k in range(1, n):
        there = (me + k) % n
        copy(s_ref, got, s_out, s_in, k, there, me).start()
        copy(l_ref, logs, l_out, l_in, k, there, me).start()
    got[me] = s_ref[me]
    logs[me] = l_ref[me]
    for k in range(1, n):
        here = (me + n - k) % n
        copy(s_ref, got, s_out, s_in, k, here, here).wait_recv()
        copy(l_ref, logs, l_out, l_in, k, here, here).wait_recv()
    back = (me * share // HEAD_DIM) % 2
    acc = jnp.zeros(s_ref.shape[1:], F32)
    for i in range(n):
        j = back * (n - 1 - i) + (1 - back) * i
        enter[j] = acc.astype(BF16)
        acc = acc * jnp.exp(logs[j][0:1, :]) + got[j].astype(F32)
    out_ref[me] = enter[me]
    for k in range(1, n):
        copy(enter, out_ref, e_out, e_in, k, (me + k) % n, me).start()
    for k in range(1, n):
        here = (me + n - k) % n
        copy(enter, out_ref, e_out, e_in, k, here, here).wait_recv()
    for k in range(1, n):
        there = (me + k) % n
        copy(s_ref, got, s_out, s_in, k, there, me).wait_send()
        copy(l_ref, logs, l_out, l_in, k, there, me).wait_send()
        copy(enter, out_ref, e_out, e_in, k, there, me).wait_send()


def exchange_states(states, span_log):
    n, share, _ = states.shape
    assert HEAD_DIM % share == 0
    tables = jnp.repeat(span_log.reshape(-1), HEAD_DIM // share)
    tables = jnp.broadcast_to(tables[:, None, None], (n, 8, STATE))
    return pl.pallas_call(
        functools.partial(exchange_kernel, n, share),
        out_shape=jax.ShapeDtypeStruct(states.shape, BF16),
        in_specs=[pl.BlockSpec(memory_space=pltpu.VMEM)] * 2,
        out_specs=pl.BlockSpec(memory_space=pltpu.VMEM),
        scratch_shapes=[
            pltpu.VMEM(states.shape, BF16),
            pltpu.VMEM(tables.shape, F32),
            pltpu.VMEM(states.shape, BF16),
        ]
        + [pltpu.SemaphoreType.DMA((n,))] * 6,
        compiler_params=pltpu.CompilerParams(collective_id=1, has_side_effects=True),
        cost_estimate=pl.CostEstimate(flops=0, bytes_accessed=2**25, transcendentals=0),
    )(states, tables)


def ring_spot(n):
    chips = n // 2
    me = lax.axis_index("sp")
    core, chip = me % 2, me // 2
    odd = chip % 2
    spot = (1 - odd) * (chip // 2) + odd * (chips - 1 - chip // 2)

    def device(position):
        position = (position + 2 * chips) % chips
        half = (chips + 1) // 2
        late = position // half
        late_chip = 2 * (chips - 1 - position) + 1
        return 2 * ((1 - late) * 2 * position + late * late_chip) + core

    return me, core, spot, device


def send_to(src, dst, out_sem, in_sem, target):
    return pltpu.make_async_remote_copy(
        src_ref=src,
        dst_ref=dst,
        send_sem=out_sem,
        recv_sem=in_sem,
        device_id=target,
        device_id_type=pl.DeviceIdType.MESH,
    )


def softplus(v):
    return jnp.maximum(v, 0.0) + jnp.log1p(jnp.exp(-jnp.abs(v)))


def tap_sum(padded, taps, length):
    full = padded.shape[0]
    half = len(taps) // 2
    total = None
    for k, tap in enumerate(taps):
        moved = padded if k == half else pltpu.roll(padded, (half - k) % full, 0)
        term = moved[HALO : HALO + length] * tap
        total = term if total is None else total + term
    return total


def mixer_kernel(
    n, x_ref, gain_ref, conv_ref, rec_ref, lat_ref, step_ref, rate_ref, spike_ref,
    ct_ref, xt_ref, lt_ref, head_gain_ref, exit_c_ref, exit_s_ref, out_ref,
    w_buf, raw, normed, proj, table_ref, turned_ref, ends_ref,
    c_all, s_all, y_c, y_s, within, reads, states, got, logs, enter, entered, away, came,
    own_sems, exit_own, x_own, x_send, x_recv,
    ring_send, ring_recv, mate_send, mate_recv,
    exit_send, exit_recv, pass_send, pass_recv,
    s_out, s_in, l_out, l_in, e_out, e_in, p_out, p_in,
):
    chips = n // 2
    hops = chips - 1
    me, core, spot, device = ring_spot(n)
    tp_me = lax.axis_index("tp")
    mate = me + 1 - 2 * core
    ways = (device(spot + 1), device(spot - 1))
    own_rows, width = x_ref.shape
    length = 2 * own_rows
    pairs, _, group_cols = w_buf.shape
    depth = w_buf.shape[1] // n
    half = depth // 2
    cw, pw, sw = conv_ref.shape[2] // pairs, 2 * HEAD_DIM, 2 * STATE

    def block_rows(owner):
        return pl.ds(pl.multiple_of(owner * depth, depth), depth)

    own = []
    for g in range(pairs):
        offset = 0
        for ref, wide in ((conv_ref, cw), (rec_ref, pw), (lat_ref, sw)):
            for i in range(ref.shape[0]):
                own.append(
                    pltpu.make_async_copy(
                        ref.at[i, :, pl.ds(g * wide, wide)],
                        w_buf.at[g, block_rows(me), pl.ds(offset, wide)],
                        own_sems.at[len(own)],
                    )
                )
                offset += wide
    per_group = len(own) // pairs
    for copy in own:
        copy.start()

    up, down = (me + 1) % n, (me + n - 1) % n
    barrier = pltpu.get_barrier_semaphore()
    greeted = [{"sp": (me + k) % n} for k in range(1, n)]
    greeted += [{"sp": other, "tp": 1 - tp_me} for other in (me, up, down)]
    for other in greeted:
        pl.semaphore_signal(
            barrier, inc=1, device_id=other, device_id_type=pl.DeviceIdType.MESH
        )
    pl.semaphore_wait(barrier, len(greeted))

    def owner_of(step, way):
        return device(spot - step if way == 0 else spot + step)

    def part_of(g, owner, way):
        return w_buf.at[g, pl.ds(pl.multiple_of(owner * depth + way * half, half), half), :]

    def ring_copy(g, step, way, shift=0):
        part = part_of(g, owner_of(step + shift, way), way)
        at = (g, step, way)
        return send_to(part, part, ring_send.at[at], ring_recv.at[at], {"sp": ways[way]})

    def mate_copy(g, step, way, incoming=False):
        owner = owner_of(step, way)
        part = part_of(g, owner + 1 - 2 * core if incoming else owner, way)
        at = (g, step, way)
        return send_to(part, part, mate_send.at[at], mate_recv.at[at], {"sp": mate})

    def start_group(g):
        for copy in own[g * per_group : (g + 1) * per_group]:
            copy.wait()
        for way in range(2):
            ring_copy(g, 0, way).start()
        for way in range(2):
            mate_copy(g, 0, way).start()

    def advance_group(g, step):
        for way in range(2):
            ring_copy(g, step, way, 1).wait_recv()
            if step < hops - 1:
                ring_copy(g, step + 1, way).start()
            mate_copy(g, step + 1, way).start()

    turn = 1 - 2 * core
    exit_refs, exit_alls = (exit_c_ref, exit_s_ref), (c_all, s_all)
    exit_wide = exit_c_ref.shape[1]

    def exit_cols(which, owner):
        return exit_alls[which].at[:, pl.ds(pl.multiple_of(owner * exit_wide, exit_wide), exit_wide)]

    def exit_source(which, step):
        if step == 0:
            return exit_refs[which]
        return exit_cols(which, device(spot - turn * step))

    def exit_copy(which, step, shift=0):
        there = exit_cols(which, device(spot - turn * (step + shift)))
        src = there if shift else exit_source(which, step)
        at = (step, which)
        return send_to(
            src, there, exit_send.at[at], exit_recv.at[at], {"sp": device(spot + turn)}
        )

    def pass_copy(which, step, incoming=False):
        if incoming:
            there = exit_cols(which, device(spot + turn * step) + 1 - 2 * core)
            src = there
        else:
            there = exit_cols(which, device(spot - turn * step))
            src = exit_source(which, step)
        at = (step, which)
        return send_to(src, there, pass_send.at[at], pass_recv.at[at], {"sp": mate})

    exit_own_copies = [
        pltpu.make_async_copy(exit_refs[which], exit_cols(which, me), exit_own.at[which])
        for which in range(2)
    ]

    def start_exit():
        for which in range(2):
            exit_copy(which, 0).start()
        for which in range(2):
            pass_copy(which, 0).start()
            exit_own_copies[which].start()

    def advance_exit(step):
        for which in range(2):
            exit_copy(which, step, 1).wait_recv()
            if step < hops - 1:
                exit_copy(which, step + 1).start()
            pass_copy(which, step + 1).start()

    start_group(0)
    mine = pl.ds(pl.multiple_of(HALO + own_rows * tp_me, HALO), own_rows)
    across = send_to(x_ref, raw.at[mine], x_send.at[0], x_recv.at[0], {"tp": 1 - tp_me})
    across.start()
    here = pltpu.make_async_copy(x_ref, raw.at[mine], x_own)
    here.start()
    before, after = pl.ds(0, HALO), pl.ds(HALO + length, HALO)

    def halo(t, low):
        if low:
            return send_to(
                x_ref.at[pl.ds(own_rows - HALO, HALO)], raw.at[before],
                x_send.at[1 + t], x_recv.at[1], {"sp": up, "tp": t},
            )
        return send_to(
            x_ref.at[pl.ds(0, HALO)], raw.at[after],
            x_send.at[1 + t], x_recv.at[2], {"sp": down, "tp": t},
        )

    sends_up = jnp.logical_and(tp_me == 1, me < n - 1)
    sends_down = jnp.logical_and(tp_me == 0, me > 0)

    @pl.when(sends_up)
    def _():
        for t in range(2):
            halo(t, True).start()

    @pl.when(sends_down)
    def _():
        for t in range(2):
            halo(t, False).start()

    @pl.when(me == 0)
    def _():
        raw[0:HALO, :] = jnp.zeros((HALO, width), BF16)

    @pl.when(me == n - 1)
    def _():
        raw[HALO + length :, :] = jnp.zeros((HALO, width), BF16)

    def make_normed():
        here.wait()
        across.wait()

        @pl.when(me > 0)
        def _():
            halo(0, True).wait_recv()

        @pl.when(me < n - 1)
        def _():
            halo(0, False).wait_recv()

        @pl.when(sends_up)
        def _():
            for t in range(2):
                halo(t, True).wait_send()

        @pl.when(sends_down)
        def _():
            for t in range(2):
                halo(t, False).wait_send()

        gain = gain_ref[...].astype(F32).reshape(1, -1)
        tall = 2 * HALO

        def norm_block(i, _):
            at = pl.ds(pl.multiple_of(i * tall, tall), tall)
            x32 = raw[at, :].astype(F32)
            scale = lax.rsqrt(jnp.mean(x32 * x32, axis=-1, keepdims=True) + epsilon)
            normed[at, :] = (x32 * scale * gain).astype(BF16)
            return 0

        lax.fori_loop(0, raw.shape[0] // tall, norm_block, 0)

    def make_tables():
        heads = spike_ref.shape[0]
        raw_step = lax.dot_general(
            normed[HALO : HALO + length, :], step_ref[...],
            (((1,), (1,)), ((), ())), preferred_element_type=F32,
        ).astype(BF16)
        lanes = table_ref.shape[1]
        row = lax.broadcasted_iota(jnp.int32, (2 * heads, lanes), 0)
        col = lax.broadcasted_iota(jnp.int32, (2 * heads, lanes), 1)
        pick = jnp.where((row % heads == col // 4) & (row // heads == col % 2), 1.0, 0.0)
        head_row = lax.broadcasted_iota(jnp.int32, (heads, lanes), 0)
        head_col = lax.broadcasted_iota(jnp.int32, (heads, lanes), 1)
        spread = jnp.where(head_row == head_col // 4, 1.0, 0.0).astype(F32)
        deltas = softplus(jnp.dot(raw_step, pick.astype(BF16), preferred_element_type=F32))
        rates = jnp.dot(rate_ref[...], spread, precision=HIGHEST, preferred_element_type=F32)
        side = lax.broadcasted_iota(jnp.int32, (2, lanes), 0)
        kind2 = lax.broadcasted_iota(jnp.int32, (2, lanes), 1) % 2
        rates = jnp.sum(jnp.where(side == kind2, rates, 0.0), axis=0, keepdims=True)
        spikes = lax.dot_general(
            spike_ref[...], spread, (((0,), (0,)), ((), ())),
            precision=HIGHEST, preferred_element_type=F32,
        )
        logs = spikes - deltas * rates
        t_at = lax.broadcasted_iota(jnp.int32, (length, length), 0)
        s_at = lax.broadcasted_iota(jnp.int32, (length, length), 1)
        tri = jnp.where(t_at >= s_at, 1.0, 0.0).astype(F32)
        run_f = jnp.dot(tri, logs, precision=HIGHEST, preferred_element_type=F32)
        tri = jnp.where(t_at <= s_at, 1.0, 0.0).astype(F32)
        run_b = jnp.dot(tri, logs, precision=HIGHEST, preferred_element_type=F32)
        kind = lax.broadcasted_iota(jnp.int32, (length, lanes), 1) % 4
        table = jnp.where(kind < 2, deltas, jnp.where(kind == 2, run_f, run_b))
        table_ref[...] = table
        turned_ref[...] = table.T
        ends = jnp.where(kind[0:1] == 2, run_f[length - 1 : length], run_b[0:1])
        ends_ref[...] = jnp.broadcast_to(ends, ends_ref.shape)

    def project_group(g):
        def arrived(step, _):
            for way in range(2):
                mate_copy(g, step, way, True).wait_recv()
            return 0

        lax.fori_loop(0, chips, arrived, 0)
        tile = group_cols // 3

        def project_tile(i, _):
            cols = pl.ds(pl.multiple_of(i * tile, STATE), tile)
            proj[g, :, cols] = jnp.dot(
                normed[...], w_buf[g, :, cols], preferred_element_type=F32
            ).astype(BF16)
            return 0

        lax.fori_loop(0, 3, project_tile, 0)

    def log_copy(k, incoming=False):
        there = (me + n - k) % n if incoming else (me + k) % n
        slot = there if incoming else me
        return send_to(ends_ref, logs.at[slot], l_out.at[k], l_in.at[k], {"sp": there})

    inner = slice(HALO, HALO + length)
    at_ig, at_va, at_gate = cw, 2 * cw, 3 * cw
    at_x = at_gate + pw
    at_b = at_x + pw
    at_c = at_b + sw

    def rows_f32(j, wide, base):
        return proj[j, :, base : base + wide].astype(F32)

    def state_copy(owner):
        return send_to(
            states.at[owner], got.at[me], s_out.at[owner], s_in.at[me], {"sp": owner}
        )

    def mix_pair(j):
        t_at = lax.broadcasted_iota(jnp.int32, (length, length), 0)
        s_at = lax.broadcasted_iota(jnp.int32, (length, length), 1)
        below, above = t_at > s_at, t_at < s_at
        taps = ct_ref[:, j * cw : (j + 1) * cw].astype(F32)
        gated = rows_f32(j, cw, at_ig) * rows_f32(j, cw, at_va)
        conv = tap_sum(
            gated.astype(BF16).astype(F32), [taps[k : k + 1] for k in range(taps.shape[0])], length
        )
        og = proj[j, inner, 0:cw].astype(F32)
        y_c[:, j * cw : (j + 1) * cw] = (og * conv).astype(BF16)
        taps = xt_ref[:, j * pw : (j + 1) * pw].astype(F32)
        xs = silu(
            tap_sum(
                rows_f32(j, pw, at_x), [taps[k : k + 1] for k in range(taps.shape[0])], length
            )
        ).astype(BF16)
        taps = [lt_ref[k, :, j * sw : (j + 1) * sw].astype(F32) for k in range(lt_ref.shape[0])]
        bs = silu(
            tap_sum(rows_f32(j, sw, at_b), [tap[0:1] for tap in taps], length)
        ).astype(BF16)
        cs = silu(
            tap_sum(rows_f32(j, sw, at_c), [tap[1:2] for tap in taps], length)
        ).astype(BF16)
        reads[:, j * sw : (j + 1) * sw] = cs
        outs = []
        for h in range(2):
            c_h = cs[:, h * STATE : (h + 1) * STATE]
            b_h = bs[:, h * STATE : (h + 1) * STATE]
            x_h = xs[:, h * HEAD_DIM : (h + 1) * HEAD_DIM]
            head = 2 * j + h
            cols = table_ref[:, 4 * head : 4 * head + 4]
            rows = turned_ref[4 * head : 4 * head + 4, :]
            scores = lax.dot_general(
                c_h, b_h, (((1,), (1,)), ((), ())), preferred_element_type=F32
            )
            gap = jnp.where(above, cols[:, 3:4] - rows[3:4], cols[:, 2:3] - rows[2:3])
            d_f, d_b = rows[0:1], rows[1:2]
            scale = jnp.where(below, d_f, jnp.where(above, d_b, d_f + d_b))
            w = (scores * jnp.exp(gap) * scale).astype(BF16)
            outs.append(jnp.dot(w, x_h, preferred_element_type=F32))
            x32 = x_h.astype(F32)
            end_f = jnp.exp(rows[2:3, length - 1 : length] - cols[:, 2:3])
            end_b = jnp.exp(rows[3:4, 0:1] - cols[:, 3:4])
            both = jnp.concatenate(
                [x32 * (end_f * cols[:, 0:1]), x32 * (end_b * cols[:, 1:2])], axis=1
            ).astype(BF16)
            state = lax.dot_general(
                both, b_h, (((0,), (0,)), ((), ())), preferred_element_type=F32
            ).astype(BF16)
            for d in range(2):
                states[2 * head + d] = state[d * HEAD_DIM : (d + 1) * HEAD_DIM]
        within[:, j * pw : (j + 1) * pw] = jnp.concatenate(outs, axis=1)

    def send_states(j):
        for owner in range(4 * j, 4 * j + 4):
            @pl.when(me != owner)
            def _():
                state_copy(owner).start()

            @pl.when(me == owner)
            def _():
                got[owner] = states[owner]

    def send_logs():
        for k in range(1, n):
            log_copy(k).start()
        logs[me] = ends_ref[...]

    def project_then(g):
        return lambda: project_group(g)

    def mix_then(g):
        def run():
            mix_pair(g)
            send_states(g)

        return run

    late = 4 * (pairs - 1)

    def enter_copy(there, owner):
        return send_to(
            enter.at[there], entered.at[owner], e_out.at[there], e_in.at[owner], {"sp": there}
        )

    def scan_states():
        for k in range(1, n):
            log_copy(k, True).wait_recv()
        for k in range(1, n):
            other = (me + k) % n
            send_to(
                states.at[other], got.at[other], s_out.at[other], s_in.at[other], {"sp": other}
            ).wait_recv()
        lane = 4 * (me // 2) + 2 + me % 2
        lane_at = lax.broadcasted_iota(jnp.int32, (1, STATE), 1)
        back = me % 2

        def scan_one(i, acc):
            j = back * (n - 1 - i) + (1 - back) * i
            enter[j] = acc.astype(BF16)
            log = jnp.sum(
                jnp.where(lane_at == lane, logs[j][0:1, :], 0.0), axis=1, keepdims=True
            )
            return acc * jnp.exp(log) + got[j].astype(F32)

        acc = jnp.zeros(got.shape[1:], F32)
        for i in range(n):
            acc = scan_one(i, acc)
        entered[me] = enter[me]
        for k in range(1, n):
            enter_copy((me + k) % n, me).start()

    def scan_early():
        pl.when(me < late)(scan_states)

    def scan_late():
        pl.when(me >= late)(scan_states)

    def finish_pair(j):
        for owner in range(4 * j, 4 * j + 4):
            @pl.when(me != owner)
            def _():
                enter_copy(me, owner).wait_recv()

        outs = []
        gains = head_gain_ref[...].astype(F32).reshape(1, -1)
        gate = silu(rows_f32(j, pw, at_gate)[inner])
        for h in range(2):
            head = 2 * j + h
            cols = table_ref[:, 4 * head : 4 * head + 4]
            wide = jnp.concatenate([entered[2 * head], entered[2 * head + 1]], axis=0)
            both = lax.dot_general(
                reads[:, head * STATE : (head + 1) * STATE], wide,
                (((1,), (1,)), ((), ())), preferred_element_type=F32,
            )
            mine = slice(h * HEAD_DIM, (h + 1) * HEAD_DIM)
            y = within[:, head * HEAD_DIM : (head + 1) * HEAD_DIM]
            y = y + both[:, :HEAD_DIM] * jnp.exp(cols[:, 2:3])
            y = y + both[:, HEAD_DIM:] * jnp.exp(cols[:, 3:4])
            g = y * gate[:, mine]
            g = g * lax.rsqrt(jnp.mean(g * g, axis=-1, keepdims=True) + epsilon)
            gain = gains[:, head * HEAD_DIM : (head + 1) * HEAD_DIM]
            outs.append(g * gain)
        y_s[:, j * pw : (j + 1) * pw] = jnp.concatenate(outs, axis=1).astype(BF16)
    def finish_then(j):
        return lambda: finish_pair(j)

    units = {LAG + 1: [make_normed], LAG + 2: [make_tables], LAG + 3: [send_logs]}
    for g in range(pairs):
        units.setdefault(SKEW * g + hops, []).append(project_then(g))
        units.setdefault(SKEW * g + hops + 1, []).insert(0, mix_then(g))
    exit_slot = SKEW * (pairs - 1) + EXIT_LAG
    last_mix = SKEW * (pairs - 1) + hops + 1

    def slot(t):
        for g in range(pairs):
            if g > 0 and t == max(SKEW * g - AHEAD, 0):
                start_group(g)
            if 0 <= t - SKEW * g < hops:
                advance_group(g, t - SKEW * g)
        if t == exit_slot - 1:
            start_exit()
        if 0 <= t - exit_slot < hops:
            advance_exit(t - exit_slot)
        for unit in units.get(t, []):
            unit()

    scan_slot = SKEW * (pairs - 1) + hops
    units[scan_slot].append(scan_early)
    for j in range(pairs - 1):
        units.setdefault(last_mix + 1, []).append(finish_then(j))
    for t in range(last_mix + 2):
        slot(t)
    scan_late()
    def partial(owner, place):
        rows = pl.ds(pl.multiple_of(owner * own_rows, HALO), own_rows)
        cols = pl.ds(pl.multiple_of(place * exit_wide, exit_wide), exit_wide)
        return jnp.dot(
            y_c[rows, :], c_all[:, cols], preferred_element_type=F32
        ) + jnp.dot(y_s[rows, :], s_all[:, cols], preferred_element_type=F32)

    def place_of(step, passed):
        if passed:
            return device(spot + turn * step) + 1 - 2 * core
        return device(spot - turn * step)

    def partial_copy(step, passed):
        at = 2 * step + passed
        return send_to(
            away.at[at], came.at[at], p_out.at[at], p_in.at[at], {"tp": 1 - tp_me}
        )

    def send_blocks(step):
        for passed in range(2):
            for which in range(2):
                if passed:
                    pass_copy(which, step, True).wait_recv()
                elif step == 0:
                    exit_own_copies[which].wait()
            away[2 * step + passed] = partial(1 - tp_me, place_of(step, passed)).astype(BF16)
            partial_copy(step, passed).start()

    rest = list(range(last_mix + 2, exit_slot + hops))
    for t in rest[:AWAIT]:
        slot(t)
    finish_pair(pairs - 1)
    done = min(hops, max(exit_slot + hops - len(rest[AWAIT:]) - exit_slot, 0))
    for step in range(done):
        send_blocks(step)
    for t in rest[AWAIT:]:
        slot(t)
        send_blocks(t - exit_slot)
    send_blocks(hops)
    for step in range(chips):
        for passed in range(2):
            place = place_of(step, passed)
            kept = partial(tp_me, place)
            partial_copy(step, passed).wait_recv()
            cols = pl.ds(pl.multiple_of(place * exit_wide, exit_wide), exit_wide)
            out_ref[:, cols] = (kept + came[2 * step + passed].astype(F32)).astype(BF16)
    for step in range(chips):
        for passed in range(2):
            partial_copy(step, passed).wait_send()
    for k in range(1, n):
        log_copy(k).wait_send()
        other = (me + k) % n
        enter_copy(other, me).wait_send()
        state_copy(other).wait_send()
    for step in range(chips):
        for which in range(2):
            if step < hops:
                exit_copy(which, step).wait_send()
            pass_copy(which, step).wait_send()

    def drain(step, _):
        for g in range(pairs):
            for way in range(2):
                @pl.when(step < hops)
                def _():
                    ring_copy(g, step, way).wait_send()

                mate_copy(g, step, way).wait_send()
        return 0

    lax.fori_loop(0, chips, drain, 0)


def mixer(
    rows, gain, conv_w, rec_w, lat_w, step_w, rate, spike,
    conv_taps, x_taps, latent_taps, head_gain, exit_c, exit_s,
):
    n = lax.axis_size("sp")
    chips = n // 2
    hops = chips - 1
    own_rows, width = rows.shape
    length = 2 * own_rows
    full = length + 2 * HALO
    depth = conv_w.shape[1]
    blocks = sum(w.shape[0] for w in (conv_w, rec_w, lat_w))
    cols = sum(w.shape[0] * w.shape[2] for w in (conv_w, rec_w, lat_w))
    heads = spike.shape[0]
    pairs = heads // 2
    conv_width, ssd_width = exit_c.shape[0], exit_s.shape[0]
    state_width = latent_taps.shape[2]
    assert 4 * heads <= STATE and 2 * heads == n and conv_width == ssd_width
    vmem = pl.BlockSpec(memory_space=pltpu.VMEM)
    hbm = pl.BlockSpec(memory_space=pl.ANY)
    spans = (n, HEAD_DIM, STATE)
    parts = (n, own_rows, width // n)
    dma = pltpu.SemaphoreType.DMA
    return pl.pallas_call(
        functools.partial(mixer_kernel, n),
        out_shape=jax.ShapeDtypeStruct((own_rows, width), BF16),
        in_specs=[hbm, vmem, hbm, hbm, hbm] + [vmem] * 7 + [hbm] * 2,
        out_specs=vmem,
        scratch_shapes=[
            pltpu.VMEM((pairs, n * depth, cols // pairs), BF16),
            pltpu.VMEM((full, width), BF16),
            pltpu.VMEM((full, width), BF16),
            pltpu.VMEM((pairs, full, cols // pairs), BF16),
            pltpu.VMEM((length, STATE), F32),
            pltpu.VMEM((STATE, length), F32),
            pltpu.VMEM((8, STATE), F32),
            pltpu.VMEM((conv_width, width), BF16),
            pltpu.VMEM((ssd_width, width), BF16),
            pltpu.VMEM((length, conv_width), BF16),
            pltpu.VMEM((length, ssd_width), BF16),
            pltpu.VMEM((length, ssd_width), F32),
            pltpu.VMEM((length, state_width), BF16),
            pltpu.VMEM(spans, BF16),
            pltpu.VMEM(spans, BF16),
            pltpu.VMEM((n, 8, STATE), F32),
            pltpu.VMEM(spans, BF16),
            pltpu.VMEM(spans, BF16),
            pltpu.VMEM(parts, BF16),
            pltpu.VMEM(parts, BF16),
            dma((pairs * blocks,)), dma((2,)), dma, dma((3,)), dma((3,)),
            dma((pairs, hops, 2)), dma((pairs, hops, 2)),
            dma((pairs, chips, 2)), dma((pairs, chips, 2)),
            dma((hops, 2)), dma((hops, 2)), dma((chips, 2)), dma((chips, 2)),
        ]
        + [dma((n,))] * 6
        + [dma((n,))] * 2,
        compiler_params=pltpu.CompilerParams(
            collective_id=2, has_side_effects=True, vmem_limit_bytes=58 * 2**20
        ),
        cost_estimate=pl.CostEstimate(
            flops=2 * full * width * cols, bytes_accessed=2 * width * cols, transcendentals=0
        ),
    )(
        rows, gain, conv_w, rec_w, lat_w, step_w, rate, spike,
        conv_taps, x_taps, latent_taps, head_gain, exit_c, exit_s,
    )


def project_kernel(r_ref, w_ref, o_ref):
    o_ref[...] = jnp.dot(r_ref[...], w_ref[...], preferred_element_type=F32).astype(BF16)


def project(rows, weights):
    count, width = rows.shape
    cols = weights.shape[1]
    tile = cols // 9
    return pl.pallas_call(
        project_kernel,
        grid=(9,),
        in_specs=[
            pl.BlockSpec((count, width), lambda j: (0, 0)),
            pl.BlockSpec((width, tile), lambda j: (0, j)),
        ],
        out_specs=pl.BlockSpec((count, tile), lambda j: (0, j)),
        out_shape=jax.ShapeDtypeStruct((count, cols), BF16),
        cost_estimate=pl.CostEstimate(
            flops=2 * count * width * cols, bytes_accessed=2 * width * cols, transcendentals=0
        ),
    )(rows, weights)


def finish_kernel(within_ref, reads_ref, enter_ref, gate_ref, gain_ref, col_ref, y_ref):
    length = y_ref.shape[0]
    cols = col_ref[0]
    outs = []
    for h in range(2):
        o = 4 * h
        both = lax.dot_general(
            reads_ref[:, h * STATE : (h + 1) * STATE],
            enter_ref[h * STATE : (h + 1) * STATE],
            (((1,), (1,)), ((), ())),
            preferred_element_type=F32,
        )
        here = slice(h * HEAD_DIM, (h + 1) * HEAD_DIM)
        y = within_ref[:, here]
        y = y + both[:, :HEAD_DIM] * jnp.exp(cols[:, o + 2 : o + 3])
        y = y + both[:, HEAD_DIM:] * jnp.exp(cols[:, o + 3 : o + 4])
        g = y * silu(gate_ref[pl.ds(HALO, length), :].astype(F32)[:, here])
        g = g * lax.rsqrt(jnp.mean(g * g, axis=-1, keepdims=True) + epsilon)
        outs.append(g * gain_ref[:, here].astype(F32))
    y_ref[...] = jnp.concatenate(outs, axis=1).astype(BF16)


def local(
    layer_source_rows, entry_rescale_factor, sliding_mixer_entry_matrix,
    recurrent_mixer_entry_matrix, latent_write_read_matrix, timestep_matrix,
    sliding_kernel_coefficients, recurrent_kernel_coefficients, latent_kernel_coefficients,
    lane_forgetting_rate, spike_forgetting_rate, lane_rescale_factor,
    sliding_mixer_exit_matrix, recurrent_mixer_exit_matrix,
):
    n = lax.axis_size("sp")
    tp = lax.axis_size("tp")
    own_rows, width = layer_source_rows.shape
    length = own_rows * tp
    full = length + 2 * HALO
    conv_width = sliding_mixer_entry_matrix.shape[2]
    ssd_width = recurrent_mixer_entry_matrix.shape[2]
    state_width = latent_write_read_matrix.shape[2]
    heads = timestep_matrix.shape[2]
    pairs = heads // 2
    cw = conv_width // pairs

    share = heads * 2 * HEAD_DIM // n
    if tp == 2 and 2 * heads == n:
        return mixer(
            layer_source_rows, entry_rescale_factor, sliding_mixer_entry_matrix,
            recurrent_mixer_entry_matrix, latent_write_read_matrix,
            timestep_matrix.transpose(1, 2, 0).reshape(2 * heads, width),
            lane_forgetting_rate, spike_forgetting_rate.T, sliding_kernel_coefficients,
            recurrent_kernel_coefficients, latent_kernel_coefficients, lane_rescale_factor,
            sliding_mixer_exit_matrix, recurrent_mixer_exit_matrix,
        )

    block = jnp.concatenate(
        [sliding_mixer_entry_matrix[i] for i in range(3)]
        + [recurrent_mixer_entry_matrix[i] for i in range(2)]
        + [latent_write_read_matrix[i] for i in range(2)],
        axis=1,
    )
    gathered = gather_rows(block)
    weights = gathered.reshape(n * block.shape[0], block.shape[1])

    x32 = layer_source_rows.astype(F32)
    normed = (
        x32
        * lax.rsqrt(jnp.mean(x32 * x32, axis=-1, keepdims=True) + epsilon)
        * entry_rescale_factor.astype(F32)
    ).astype(BF16)
    up = [(i, i + 1) for i in range(n - 1)]
    down = [(i + 1, i) for i in range(n - 1)]
    before = lax.ppermute(normed[own_rows - HALO :], "sp", up)
    after = lax.ppermute(normed[:HALO], "sp", down)
    shared = lax.all_gather(jnp.concatenate([before, normed, after], axis=0), "tp", axis=0)
    rows = jnp.concatenate(
        [shared[tp - 1, :HALO]]
        + [shared[i, HALO : HALO + own_rows] for i in range(tp)]
        + [shared[0, HALO + own_rows :]],
        axis=0,
    )

    step_weight = timestep_matrix.reshape(width, 2 * heads)
    raw = jnp.dot(rows, step_weight, preferred_element_type=F32).astype(BF16)
    raw = raw[HALO : HALO + length].astype(F32).reshape(length, 2, heads)
    deltas = jax.nn.softplus(raw)
    logs = -deltas * lane_forgetting_rate[None] + spike_forgetting_rate[:, None, :]
    tri = (jnp.arange(length)[:, None] >= jnp.arange(length)[None, :]).astype(F32)
    run_f = jnp.dot(tri, logs[:, 0], precision=HIGHEST)
    run_b = jnp.dot(tri.T, logs[:, 1], precision=HIGHEST)
    table = jnp.stack([deltas[:, 0], deltas[:, 1], run_f, run_b], axis=2)
    col_table = table.reshape(length, pairs, 8).transpose(1, 0, 2)
    row_table = table.reshape(length, pairs, 8).transpose(1, 2, 0)
    span_log = jnp.stack([run_f[length - 1], run_b[0]], axis=1)
    exit_c, exit_s, weights = lax.optimization_barrier(
        (sliding_mixer_exit_matrix, recurrent_mixer_exit_matrix, weights)
    )
    proj = project(rows, weights)
    exit_c = lax.all_gather(exit_c, "sp", axis=1, tiled=True)
    exit_s = lax.all_gather(exit_s, "sp", axis=1, tiled=True)

    latent = latent_kernel_coefficients
    pw, sw = 2 * HEAD_DIM, 2 * STATE
    g0 = 3 * conv_width
    at_gate, at_x = g0 // pw, (g0 + ssd_width) // pw
    at_b = (g0 + 2 * ssd_width) // sw
    at_c = at_b + pairs
    y_conv, within, reads, states = pl.pallas_call(
        mix_kernel,
        grid=(pairs,),
        in_specs=[
            pl.BlockSpec((full, cw), lambda j: (0, j)),
            pl.BlockSpec((full, cw), lambda j: (0, pairs + j)),
            pl.BlockSpec((full, cw), lambda j: (0, 2 * pairs + j)),
            pl.BlockSpec((full, pw), lambda j: (0, at_x + j)),
            pl.BlockSpec((full, sw), lambda j: (0, at_b + j)),
            pl.BlockSpec((full, sw), lambda j: (0, at_c + j)),
            pl.BlockSpec((3, cw), lambda j: (0, j)),
            pl.BlockSpec((5, pw), lambda j: (0, j)),
            pl.BlockSpec((5, sw), lambda j: (0, j)),
            pl.BlockSpec((5, sw), lambda j: (0, pairs + j)),
            pl.BlockSpec((1, length, 8), lambda j: (j, 0, 0)),
            pl.BlockSpec((1, 8, length), lambda j: (j, 0, 0)),
        ],
        out_specs=[
            pl.BlockSpec((length, cw), lambda j: (0, j)),
            pl.BlockSpec((length, pw), lambda j: (0, j)),
            pl.BlockSpec((length, sw), lambda j: (0, j)),
            pl.BlockSpec((sw, STATE), lambda j: (j, 0)),
        ],
        out_shape=[
            jax.ShapeDtypeStruct((length, conv_width), BF16),
            jax.ShapeDtypeStruct((length, ssd_width), F32),
            jax.ShapeDtypeStruct((length, state_width), BF16),
            jax.ShapeDtypeStruct((pairs * sw, STATE), BF16),
        ],
        cost_estimate=pl.CostEstimate(
            flops=8 * length * length * heads * STATE, bytes_accessed=2**24, transcendentals=0
        ),
    )(
        proj, proj, proj, proj, proj, proj,
        sliding_kernel_coefficients, recurrent_kernel_coefficients,
        latent.reshape(latent.shape[0], -1), latent.reshape(latent.shape[0], -1),
        col_table, row_table,
    )

    entering = exchange_states(states.reshape(n, share, STATE), span_log)
    entering = entering.reshape(pairs * sw, STATE)

    y_ssd = pl.pallas_call(
        finish_kernel,
        grid=(pairs,),
        in_specs=[
            pl.BlockSpec((length, pw), lambda j: (0, j)),
            pl.BlockSpec((length, sw), lambda j: (0, j)),
            pl.BlockSpec((sw, STATE), lambda j: (j, 0)),
            pl.BlockSpec((full, pw), lambda j: (0, at_gate + j)),
            pl.BlockSpec((1, pw), lambda j: (0, j)),
            pl.BlockSpec((1, length, 8), lambda j: (j, 0, 0)),
        ],
        out_specs=pl.BlockSpec((length, pw), lambda j: (0, j)),
        out_shape=jax.ShapeDtypeStruct((length, ssd_width), BF16),
    )(within, reads, entering, proj, lane_rescale_factor.reshape(1, -1), col_table)

    def partial(y_c, y_s):
        return (
            jnp.dot(y_c, exit_c, preferred_element_type=F32)
            + jnp.dot(y_s, exit_s, preferred_element_type=F32)
        ).astype(BF16)

    if tp != 2:
        return lax.psum_scatter(
            partial(y_conv, y_ssd), "tp", scatter_dimension=0, tiled=True
        )
    tp_me = lax.axis_index("tp")

    def rows_of(owner, y):
        return lax.dynamic_slice_in_dim(y, owner * own_rows, own_rows, axis=0)

    away = partial(rows_of(1 - tp_me, y_conv), rows_of(1 - tp_me, y_ssd))
    arrived = lax.ppermute(away, "tp", [(0, 1), (1, 0)])
    kept = partial(rows_of(tp_me, y_conv), rows_of(tp_me, y_ssd))
    return (kept.astype(F32) + arrived.astype(F32)).astype(BF16)


def solution(mesh):
    placed = (
        P(("sp", "tp"), None),
        P(),
        P(None, "sp", "tp"),
        P(None, "sp", "tp"),
        P(None, "sp", "tp"),
        P(None, None, "tp"),
        P(None, "tp"),
        P(None, "tp"),
        P(None, None, "tp"),
        P(None, "tp"),
        P("sp", "tp"),
        P("tp"),
        P("tp", "sp"),
        P("tp", "sp"),
    )
    return jax.shard_map(
        local, mesh=mesh, in_specs=placed, out_specs=P(("sp", "tp"), None), check_vma=False
    )
```

```python
import functools

import jax
import jax.numpy as jnp
from jax import lax
from jax.experimental import pallas as pl
from jax.experimental.pallas import tpu as pltpu
from jax.sharding import PartitionSpec as P

HEAD_DIM = 64
STATE = 128
HALO = 16
CHUNKS = 2
LAG = 2
SKEW = 1
EXIT_LAG = 7
AHEAD = 1
AWAIT = 2
epsilon = 1e-05
F32 = jnp.float32
BF16 = jnp.bfloat16
HIGHEST = lax.Precision.HIGHEST


def ring_kernel(n, w_ref, out_ref, own_sem, ring_send, ring_recv, mate_send, mate_recv):
    chips = n // 2
    me = lax.axis_index("sp")
    core, chip = me % 2, me // 2
    odd = chip % 2
    spot = (1 - odd) * (chip // 2) + odd * (chips - 1 - chip // 2)

    def device(position):
        position = (position + 2 * chips) % chips
        half = (chips + 1) // 2
        late = position // half
        late_chip = 2 * (chips - 1 - position) + 1
        return 2 * ((1 - late) * 2 * position + late * late_chip) + core

    mate = me + 1 - 2 * core
    ways = (device(spot + 1), device(spot - 1))
    rows = w_ref.shape[0] // (2 * CHUNKS)

    barrier = pltpu.get_barrier_semaphore()
    for other in (mate,) + ways:
        pl.semaphore_signal(
            barrier, inc=1, device_id={"sp": other}, device_id_type=pl.DeviceIdType.MESH
        )
    pl.semaphore_wait(barrier, 3)

    def piece(way, chunk):
        return pl.ds((way * CHUNKS + chunk) * rows, rows)

    def ring_copy(step, way, chunk):
        owner = device(spot - step if way == 0 else spot + step)
        part = piece(way, chunk)
        return pltpu.make_async_remote_copy(
            src_ref=w_ref.at[part] if step == 0 else out_ref.at[owner, part],
            dst_ref=out_ref.at[owner, part],
            send_sem=ring_send.at[step, way, chunk],
            recv_sem=ring_recv.at[step, way, chunk],
            device_id={"sp": ways[way]},
            device_id_type=pl.DeviceIdType.MESH,
        )

    def arrival(step, way, chunk):
        owner = device(spot - step - 1 if way == 0 else spot + step + 1)
        part = piece(way, chunk)
        return pltpu.make_async_remote_copy(
            src_ref=out_ref.at[owner, part],
            dst_ref=out_ref.at[owner, part],
            send_sem=ring_send.at[step, way, chunk],
            recv_sem=ring_recv.at[step, way, chunk],
            device_id={"sp": ways[way]},
            device_id_type=pl.DeviceIdType.MESH,
        )

    def mate_copy(step, way, chunk, incoming=False):
        owner = device(spot - step if way == 0 else spot + step)
        if incoming:
            owner = owner + 1 - 2 * core
        part = piece(way, chunk)
        return pltpu.make_async_remote_copy(
            src_ref=w_ref.at[part] if step == 0 else out_ref.at[owner, part],
            dst_ref=out_ref.at[owner, part],
            send_sem=mate_send.at[step, way, chunk],
            recv_sem=mate_recv.at[step, way, chunk],
            device_id={"sp": mate},
            device_id_type=pl.DeviceIdType.MESH,
        )

    parts = [(way, chunk) for chunk in range(CHUNKS) for way in range(2)]
    for way, chunk in parts:
        ring_copy(0, way, chunk).start()
    for way, chunk in parts:
        mate_copy(0, way, chunk).start()
    own = pltpu.make_async_copy(w_ref, out_ref.at[me], own_sem)
    own.start()
    for step in range(chips - 1):
        for way, chunk in parts:
            arrival(step, way, chunk).wait_recv()
            if step < chips - 2:
                ring_copy(step + 1, way, chunk).start()
            mate_copy(step + 1, way, chunk).start()
    own.wait()
    for step in range(chips):
        for way, chunk in parts:
            if step < chips - 1:
                ring_copy(step, way, chunk).wait_send()
            mate_copy(step, way, chunk).wait_send()
            mate_copy(step, way, chunk, True).wait_recv()


def gather_rows(block):
    n = lax.axis_size("sp")
    chips = n // 2
    rows, cols = block.shape
    return pl.pallas_call(
        functools.partial(ring_kernel, n),
        out_shape=jax.ShapeDtypeStruct((n, rows, cols), block.dtype),
        in_specs=[pl.BlockSpec(memory_space=pltpu.VMEM)],
        out_specs=pl.BlockSpec(memory_space=pl.ANY),
        scratch_shapes=[
            pltpu.SemaphoreType.DMA,
            pltpu.SemaphoreType.DMA((chips - 1, 2, CHUNKS)),
            pltpu.SemaphoreType.DMA((chips - 1, 2, CHUNKS)),
            pltpu.SemaphoreType.DMA((chips, 2, CHUNKS)),
            pltpu.SemaphoreType.DMA((chips, 2, CHUNKS)),
        ],
        compiler_params=pltpu.CompilerParams(
            collective_id=0, has_side_effects=True, vmem_limit_bytes=16 * 2**20
        ),
        cost_estimate=pl.CostEstimate(
            flops=0, bytes_accessed=n * rows * cols * 16, transcendentals=0
        ),
    )(block)


def taps_of(padded, table, length):
    full = padded.shape[0]
    half = table.shape[0] // 2
    total = None
    for k in range(table.shape[0]):
        moved = padded if k == half else pltpu.roll(padded, (half - k) % full, 0)
        term = moved[HALO : HALO + length] * table[k : k + 1].astype(F32)
        total = term if total is None else total + term
    return total


def silu(v):
    return v * jax.nn.sigmoid(v)


def mix_kernel(
    og_ref, ig_ref, va_ref, x_ref, b_ref, c_ref, ct_ref, xt_ref, bt_ref, rt_ref,
    col_ref, row_ref, yconv_ref, within_ref, reads_ref, state_ref,
):
    length = yconv_ref.shape[0]
    gated = (ig_ref[...].astype(F32) * va_ref[...].astype(F32)).astype(BF16).astype(F32)
    conv = taps_of(gated, ct_ref[...], length)
    yconv_ref[...] = (og_ref[pl.ds(HALO, length), :].astype(F32) * conv).astype(BF16)
    xs = silu(taps_of(x_ref[...].astype(F32), xt_ref[...], length)).astype(BF16)
    bs = silu(taps_of(b_ref[...].astype(F32), bt_ref[...], length)).astype(BF16)
    cs = silu(taps_of(c_ref[...].astype(F32), rt_ref[...], length)).astype(BF16)
    reads_ref[...] = cs
    cols = col_ref[0]
    rows = row_ref[0]
    t_at = lax.broadcasted_iota(jnp.int32, (length, length), 0)
    s_at = lax.broadcasted_iota(jnp.int32, (length, length), 1)
    outs, weighted = [], []
    for h in range(2):
        c_h = cs[:, h * STATE : (h + 1) * STATE]
        b_h = bs[:, h * STATE : (h + 1) * STATE]
        x_h = xs[:, h * HEAD_DIM : (h + 1) * HEAD_DIM]
        o = 4 * h
        scores = lax.dot_general(
            c_h, b_h, (((1,), (1,)), ((), ())), preferred_element_type=F32
        )
        gap = jnp.where(
            t_at >= s_at,
            cols[:, o + 2 : o + 3] - rows[o + 2 : o + 3],
            cols[:, o + 3 : o + 4] - rows[o + 3 : o + 4],
        )
        d_f, d_b = rows[o : o + 1], rows[o + 1 : o + 2]
        scale = jnp.where(t_at > s_at, d_f, jnp.where(t_at < s_at, d_b, d_f + d_b))
        w = (scores * jnp.exp(gap) * scale).astype(BF16)
        outs.append(jnp.dot(w, x_h, preferred_element_type=F32))
        x32 = x_h.astype(F32)
        end_f = jnp.exp(rows[o + 2 : o + 3, length - 1 : length] - cols[:, o + 2 : o + 3])
        end_b = jnp.exp(rows[o + 3 : o + 4, 0:1] - cols[:, o + 3 : o + 4])
        both = jnp.concatenate(
            [x32 * (end_f * cols[:, o : o + 1]), x32 * (end_b * cols[:, o + 1 : o + 2])], axis=1
        ).astype(BF16)
        state_ref[h * STATE : (h + 1) * STATE] = lax.dot_general(
            both, b_h, (((0,), (0,)), ((), ())), preferred_element_type=F32
        ).astype(BF16)
    within_ref[...] = jnp.concatenate(outs, axis=1)


def exchange_kernel(
    n, share, s_ref, l_ref, out_ref, got, logs, enter, s_out, s_in, l_out, l_in, e_out, e_in
):
    me = lax.axis_index("sp")
    barrier = pltpu.get_barrier_semaphore()
    for k in range(1, n):
        pl.semaphore_signal(
            barrier,
            inc=1,
            device_id={"sp": (me + k) % n},
            device_id_type=pl.DeviceIdType.MESH,
        )
    pl.semaphore_wait(barrier, n - 1)

    def copy(src, dst, out_sem, in_sem, k, there, slot):
        return pltpu.make_async_remote_copy(
            src_ref=src.at[there],
            dst_ref=dst.at[slot],
            send_sem=out_sem.at[k],
            recv_sem=in_sem.at[k],
            device_id={"sp": there},
            device_id_type=pl.DeviceIdType.MESH,
        )

    for k in range(1, n):
        there = (me + k) % n
        copy(s_ref, got, s_out, s_in, k, there, me).start()
        copy(l_ref, logs, l_out, l_in, k, there, me).start()
    got[me] = s_ref[me]
    logs[me] = l_ref[me]
    for k in range(1, n):
        here = (me + n - k) % n
        copy(s_ref, got, s_out, s_in, k, here, here).wait_recv()
        copy(l_ref, logs, l_out, l_in, k, here, here).wait_recv()
    back = (me * share // HEAD_DIM) % 2
    acc = jnp.zeros(s_ref.shape[1:], F32)
    for i in range(n):
        j = back * (n - 1 - i) + (1 - back) * i
        enter[j] = acc.astype(BF16)
        acc = acc * jnp.exp(logs[j, 0:1]) + got[j].astype(F32)
    out_ref[me] = enter[me]
    for k in range(1, n):
        copy(enter, out_ref, e_out, e_in, k, (me + k) % n, me).start()
    for k in range(1, n):
        here = (me + n - k) % n
        copy(enter, out_ref, e_out, e_in, k, here, here).wait_recv()
    for k in range(1, n):
        there = (me + k) % n
        copy(s_ref, got, s_out, s_in, k, there, me).wait_send()
        copy(l_ref, logs, l_out, l_in, k, there, me).wait_send()
        copy(enter, out_ref, e_out, e_in, k, there, me).wait_send()


def exchange_states(states, span_log):
    n, share, _ = states.shape
    assert HEAD_DIM % share == 0
    tables = jnp.repeat(span_log.reshape(-1), HEAD_DIM // share)
    tables = jnp.broadcast_to(tables[:, None, None], (n, 8, STATE))
    return pl.pallas_call(
        functools.partial(exchange_kernel, n, share),
        out_shape=jax.ShapeDtypeStruct(states.shape, BF16),
        in_specs=[pl.BlockSpec(memory_space=pltpu.VMEM)] * 2,
        out_specs=pl.BlockSpec(memory_space=pltpu.VMEM),
        scratch_shapes=[
            pltpu.VMEM(states.shape, BF16),
            pltpu.VMEM(tables.shape, F32),
            pltpu.VMEM(states.shape, BF16),
        ]
        + [pltpu.SemaphoreType.DMA((n,))] * 6,
        compiler_params=pltpu.CompilerParams(collective_id=1, has_side_effects=True),
        cost_estimate=pl.CostEstimate(flops=0, bytes_accessed=2**25, transcendentals=0),
    )(states, tables)


def ring_spot(n):
    chips = n // 2
    me = lax.axis_index("sp")
    core, chip = me % 2, me // 2
    odd = chip % 2
    spot = (1 - odd) * (chip // 2) + odd * (chips - 1 - chip // 2)

    def device(position):
        position = (position + 2 * chips) % chips
        half = (chips + 1) // 2
        late = position // half
        late_chip = 2 * (chips - 1 - position) + 1
        return 2 * ((1 - late) * 2 * position + late * late_chip) + core

    return me, core, spot, device


def send_to(src, dst, out_sem, in_sem, target):
    return pltpu.make_async_remote_copy(
        src_ref=src,
        dst_ref=dst,
        send_sem=out_sem,
        recv_sem=in_sem,
        device_id=target,
        device_id_type=pl.DeviceIdType.MESH,
    )


def softplus(v):
    return jnp.maximum(v, 0.0) + jnp.log1p(jnp.exp(-jnp.abs(v)))


def tap_sum(padded, taps, length):
    full = padded.shape[0]
    half = len(taps) // 2
    total = None
    for k, tap in enumerate(taps):
        moved = padded if k == half else pltpu.roll(padded, (half - k) % full, 0)
        term = moved[HALO : HALO + length] * tap
        total = term if total is None else total + term
    return total


def mixer_kernel(
    n, x_ref, gain_ref, conv_ref, rec_ref, lat_ref, step_ref, rate_ref, spike_ref,
    ct_ref, xt_ref, lt_ref, head_gain_ref, exit_c_ref, exit_s_ref, out_ref,
    w_buf, raw, normed, proj, table_ref, turned_ref, ends_ref,
    c_all, s_all, y_c, y_s, within, reads, states, got, logs, enter, entered, away, came,
    own_sems, exit_own, x_own, x_send, x_recv,
    ring_send, ring_recv, mate_send, mate_recv,
    exit_send, exit_recv, pass_send, pass_recv,
    s_out, s_in, l_out, l_in, e_out, e_in, p_out, p_in,
):
    chips = n // 2
    hops = chips - 1
    me, core, spot, device = ring_spot(n)
    tp_me = lax.axis_index("tp")
    mate = me + 1 - 2 * core
    ways = (device(spot + 1), device(spot - 1))
    own_rows, width = x_ref.shape
    length = 2 * own_rows
    pairs, _, group_cols = w_buf.shape
    depth = w_buf.shape[1] // n
    half = depth // 2
    cw, pw, sw = conv_ref.shape[2] // pairs, 2 * HEAD_DIM, 2 * STATE

    def block_rows(owner):
        return pl.ds(pl.multiple_of(owner * depth, depth), depth)

    own = []
    for g in range(pairs):
        offset = 0
        for ref, wide in ((conv_ref, cw), (rec_ref, pw), (lat_ref, sw)):
            for i in range(ref.shape[0]):
                own.append(
                    pltpu.make_async_copy(
                        ref.at[i, :, pl.ds(g * wide, wide)],
                        w_buf.at[g, block_rows(me), pl.ds(offset, wide)],
                        own_sems.at[len(own)],
                    )
                )
                offset += wide
    per_group = len(own) // pairs
    for copy in own:
        copy.start()

    up, down = (me + 1) % n, (me + n - 1) % n
    barrier = pltpu.get_barrier_semaphore()
    greeted = [{"sp": (me + k) % n} for k in range(1, n)]
    greeted += [{"sp": other, "tp": 1 - tp_me} for other in (me, up, down)]
    for other in greeted:
        pl.semaphore_signal(
            barrier, inc=1, device_id=other, device_id_type=pl.DeviceIdType.MESH
        )
    pl.semaphore_wait(barrier, len(greeted))

    def owner_of(step, way):
        return device(spot - step if way == 0 else spot + step)

    def part_of(g, owner, way):
        return w_buf.at[g, pl.ds(pl.multiple_of(owner * depth + way * half, half), half), :]

    def ring_copy(g, step, way, shift=0):
        part = part_of(g, owner_of(step + shift, way), way)
        at = (g, step, way)
        return send_to(part, part, ring_send.at[at], ring_recv.at[at], {"sp": ways[way]})

    def mate_copy(g, step, way, incoming=False):
        owner = owner_of(step, way)
        part = part_of(g, owner + 1 - 2 * core if incoming else owner, way)
        at = (g, step, way)
        return send_to(part, part, mate_send.at[at], mate_recv.at[at], {"sp": mate})

    def start_group(g):
        for copy in own[g * per_group : (g + 1) * per_group]:
            copy.wait()
        for way in range(2):
            ring_copy(g, 0, way).start()
        for way in range(2):
            mate_copy(g, 0, way).start()

    def advance_group(g, step):
        for way in range(2):
            ring_copy(g, step, way, 1).wait_recv()
            if step < hops - 1:
                ring_copy(g, step + 1, way).start()
            mate_copy(g, step + 1, way).start()

    turn = 1 - 2 * core
    exit_refs, exit_alls = (exit_c_ref, exit_s_ref), (c_all, s_all)
    exit_wide = exit_c_ref.shape[1]

    def exit_cols(which, owner):
        return exit_alls[which].at[:, pl.ds(pl.multiple_of(owner * exit_wide, exit_wide), exit_wide)]

    def exit_source(which, step):
        if step == 0:
            return exit_refs[which]
        return exit_cols(which, device(spot - turn * step))

    def exit_copy(which, step, shift=0):
        there = exit_cols(which, device(spot - turn * (step + shift)))
        src = there if shift else exit_source(which, step)
        at = (step, which)
        return send_to(
            src, there, exit_send.at[at], exit_recv.at[at], {"sp": device(spot + turn)}
        )

    def pass_copy(which, step, incoming=False):
        if incoming:
            there = exit_cols(which, device(spot + turn * step) + 1 - 2 * core)
            src = there
        else:
            there = exit_cols(which, device(spot - turn * step))
            src = exit_source(which, step)
        at = (step, which)
        return send_to(src, there, pass_send.at[at], pass_recv.at[at], {"sp": mate})

    exit_own_copies = [
        pltpu.make_async_copy(exit_refs[which], exit_cols(which, me), exit_own.at[which])
        for which in range(2)
    ]

    def start_exit():
        for which in range(2):
            exit_copy(which, 0).start()
        for which in range(2):
            pass_copy(which, 0).start()
            exit_own_copies[which].start()

    def advance_exit(step):
        for which in range(2):
            exit_copy(which, step, 1).wait_recv()
            if step < hops - 1:
                exit_copy(which, step + 1).start()
            pass_copy(which, step + 1).start()

    start_group(0)
    mine = pl.ds(pl.multiple_of(HALO + own_rows * tp_me, HALO), own_rows)
    across = send_to(x_ref, raw.at[mine], x_send.at[0], x_recv.at[0], {"tp": 1 - tp_me})
    across.start()
    here = pltpu.make_async_copy(x_ref, raw.at[mine], x_own)
    here.start()
    before, after = pl.ds(0, HALO), pl.ds(HALO + length, HALO)

    def halo(t, low):
        if low:
            return send_to(
                x_ref.at[pl.ds(own_rows - HALO, HALO)], raw.at[before],
                x_send.at[1 + t], x_recv.at[1], {"sp": up, "tp": t},
            )
        return send_to(
            x_ref.at[pl.ds(0, HALO)], raw.at[after],
            x_send.at[1 + t], x_recv.at[2], {"sp": down, "tp": t},
        )

    sends_up = jnp.logical_and(tp_me == 1, me < n - 1)
    sends_down = jnp.logical_and(tp_me == 0, me > 0)

    @pl.when(sends_up)
    def _():
        for t in range(2):
            halo(t, True).start()

    @pl.when(sends_down)
    def _():
        for t in range(2):
            halo(t, False).start()

    @pl.when(me == 0)
    def _():
        raw[0:HALO, :] = jnp.zeros((HALO, width), BF16)

    @pl.when(me == n - 1)
    def _():
        raw[HALO + length :, :] = jnp.zeros((HALO, width), BF16)

    def make_normed():
        here.wait()
        across.wait()

        @pl.when(me > 0)
        def _():
            halo(0, True).wait_recv()

        @pl.when(me < n - 1)
        def _():
            halo(0, False).wait_recv()

        @pl.when(sends_up)
        def _():
            for t in range(2):
                halo(t, True).wait_send()

        @pl.when(sends_down)
        def _():
            for t in range(2):
                halo(t, False).wait_send()

        gain = gain_ref[...].astype(F32).reshape(1, -1)
        tall = 2 * HALO

        def norm_block(i, _):
            at = pl.ds(pl.multiple_of(i * tall, tall), tall)
            x32 = raw[at, :].astype(F32)
            scale = lax.rsqrt(jnp.mean(x32 * x32, axis=-1, keepdims=True) + epsilon)
            normed[at, :] = (x32 * scale * gain).astype(BF16)
            return 0

        lax.fori_loop(0, raw.shape[0] // tall, norm_block, 0)

    def make_tables():
        heads = spike_ref.shape[0]
        raw_step = lax.dot_general(
            normed[HALO : HALO + length, :], step_ref[...],
            (((1,), (1,)), ((), ())), preferred_element_type=F32,
        ).astype(BF16)
        lanes = table_ref.shape[1]
        row = lax.broadcasted_iota(jnp.int32, (2 * heads, lanes), 0)
        col = lax.broadcasted_iota(jnp.int32, (2 * heads, lanes), 1)
        pick = jnp.where((row % heads == col // 4) & (row // heads == col % 2), 1.0, 0.0)
        head_row = lax.broadcasted_iota(jnp.int32, (heads, lanes), 0)
        head_col = lax.broadcasted_iota(jnp.int32, (heads, lanes), 1)
        spread = jnp.where(head_row == head_col // 4, 1.0, 0.0).astype(F32)
        deltas = softplus(jnp.dot(raw_step, pick.astype(BF16), preferred_element_type=F32))
        rates = jnp.dot(rate_ref[...], spread, precision=HIGHEST, preferred_element_type=F32)
        side = lax.broadcasted_iota(jnp.int32, (2, lanes), 0)
        kind2 = lax.broadcasted_iota(jnp.int32, (2, lanes), 1) % 2
        rates = jnp.sum(jnp.where(side == kind2, rates, 0.0), axis=0, keepdims=True)
        spikes = lax.dot_general(
            spike_ref[...], spread, (((0,), (0,)), ((), ())),
            precision=HIGHEST, preferred_element_type=F32,
        )
        logs = spikes - deltas * rates
        t_at = lax.broadcasted_iota(jnp.int32, (length, length), 0)
        s_at = lax.broadcasted_iota(jnp.int32, (length, length), 1)
        tri = jnp.where(t_at >= s_at, 1.0, 0.0).astype(F32)
        run_f = jnp.dot(tri, logs, precision=HIGHEST, preferred_element_type=F32)
        tri = jnp.where(t_at <= s_at, 1.0, 0.0).astype(F32)
        run_b = jnp.dot(tri, logs, precision=HIGHEST, preferred_element_type=F32)
        kind = lax.broadcasted_iota(jnp.int32, (length, lanes), 1) % 4
        table = jnp.where(kind < 2, deltas, jnp.where(kind == 2, run_f, run_b))
        table_ref[...] = table
        turned_ref[...] = table.T
        ends = jnp.where(kind[0:1] == 2, run_f[length - 1 : length], run_b[0:1])
        ends_ref[...] = jnp.broadcast_to(ends, ends_ref.shape)

    def project_group(g):
        def arrived(step, _):
            for way in range(2):
                mate_copy(g, step, way, True).wait_recv()
            return 0

        lax.fori_loop(0, chips, arrived, 0)
        tile = group_cols // 3

        def project_tile(i, _):
            cols = pl.ds(pl.multiple_of(i * tile, STATE), tile)
            proj[g, :, cols] = jnp.dot(
                normed[...], w_buf[g, :, cols], preferred_element_type=F32
            ).astype(BF16)
            return 0

        lax.fori_loop(0, 3, project_tile, 0)

    def log_copy(k, incoming=False):
        there = (me + n - k) % n if incoming else (me + k) % n
        slot = there if incoming else me
        return send_to(
            ends_ref.at[pl.ds(0, 1)], logs.at[slot, pl.ds(0, 1)], l_out.at[k], l_in.at[k], {"sp": there}
        )

    inner = slice(HALO, HALO + length)
    at_ig, at_va, at_gate = cw, 2 * cw, 3 * cw
    at_x = at_gate + pw
    at_b = at_x + pw
    at_c = at_b + sw

    def rows_f32(j, wide, base):
        return proj[j, :, base : base + wide].astype(F32)

    def state_copy(owner):
        return send_to(
            states.at[owner], got.at[me], s_out.at[owner], s_in.at[me], {"sp": owner}
        )

    def mix_pair(j):
        t_at = lax.broadcasted_iota(jnp.int32, (length, length), 0)
        s_at = lax.broadcasted_iota(jnp.int32, (length, length), 1)
        below, above = t_at > s_at, t_at < s_at
        taps = ct_ref[:, j * cw : (j + 1) * cw].astype(F32)
        gated = rows_f32(j, cw, at_ig) * rows_f32(j, cw, at_va)
        conv = tap_sum(
            gated.astype(BF16).astype(F32), [taps[k : k + 1] for k in range(taps.shape[0])], length
        )
        og = proj[j, inner, 0:cw].astype(F32)
        y_c[:, j * cw : (j + 1) * cw] = (og * conv).astype(BF16)
        taps = xt_ref[:, j * pw : (j + 1) * pw].astype(F32)
        xs = silu(
            tap_sum(
                rows_f32(j, pw, at_x), [taps[k : k + 1] for k in range(taps.shape[0])], length
            )
        ).astype(BF16)
        taps = [lt_ref[k, :, j * sw : (j + 1) * sw].astype(F32) for k in range(lt_ref.shape[0])]
        bs = silu(
            tap_sum(rows_f32(j, sw, at_b), [tap[0:1] for tap in taps], length)
        ).astype(BF16)
        cs = silu(
            tap_sum(rows_f32(j, sw, at_c), [tap[1:2] for tap in taps], length)
        ).astype(BF16)
        reads[:, j * sw : (j + 1) * sw] = cs
        outs = []
        for h in range(2):
            c_h = cs[:, h * STATE : (h + 1) * STATE]
            b_h = bs[:, h * STATE : (h + 1) * STATE]
            x_h = xs[:, h * HEAD_DIM : (h + 1) * HEAD_DIM]
            head = 2 * j + h
            cols = table_ref[:, 4 * head : 4 * head + 4]
            rows = turned_ref[4 * head : 4 * head + 4, :]
            scores = lax.dot_general(
                c_h, b_h, (((1,), (1,)), ((), ())), preferred_element_type=F32
            )
            gap = jnp.where(above, cols[:, 3:4] - rows[3:4], cols[:, 2:3] - rows[2:3])
            d_f, d_b = rows[0:1], rows[1:2]
            scale = jnp.where(below, d_f, jnp.where(above, d_b, d_f + d_b))
            w = (scores * jnp.exp(gap) * scale).astype(BF16)
            outs.append(jnp.dot(w, x_h, preferred_element_type=F32))
            x32 = x_h.astype(F32)
            end_f = jnp.exp(rows[2:3, length - 1 : length] - cols[:, 2:3])
            end_b = jnp.exp(rows[3:4, 0:1] - cols[:, 3:4])
            both = jnp.concatenate(
                [x32 * (end_f * cols[:, 0:1]), x32 * (end_b * cols[:, 1:2])], axis=1
            ).astype(BF16)
            state = lax.dot_general(
                both, b_h, (((0,), (0,)), ((), ())), preferred_element_type=F32
            ).astype(BF16)
            for d in range(2):
                states[2 * head + d] = state[d * HEAD_DIM : (d + 1) * HEAD_DIM]
        within[:, j * pw : (j + 1) * pw] = jnp.concatenate(outs, axis=1)

    def send_states(j):
        for owner in range(4 * j, 4 * j + 4):
            @pl.when(me != owner)
            def _():
                state_copy(owner).start()

            @pl.when(me == owner)
            def _():
                got[owner] = states[owner]

    def send_logs():
        for k in range(1, n):
            log_copy(k).start()
        logs[me, 0:1] = ends_ref[0:1, :]

    def project_then(g):
        return lambda: project_group(g)

    def mix_then(g):
        def run():
            mix_pair(g)
            send_states(g)

        return run

    late = 4 * (pairs - 1)

    def enter_copy(there, owner):
        return send_to(
            enter.at[there], entered.at[owner], e_out.at[there], e_in.at[owner], {"sp": there}
        )

    def scan_states():
        for k in range(1, n):
            log_copy(k, True).wait_recv()
        for k in range(1, n):
            other = (me + k) % n
            send_to(
                states.at[other], got.at[other], s_out.at[other], s_in.at[other], {"sp": other}
            ).wait_recv()
        lane = 4 * (me // 2) + 2 + me % 2
        lane_at = lax.broadcasted_iota(jnp.int32, (1, STATE), 1)
        back = me % 2

        def scan_one(i, acc):
            j = back * (n - 1 - i) + (1 - back) * i
            enter[j] = acc.astype(BF16)
            log = jnp.sum(
                jnp.where(lane_at == lane, logs[j, 0:1], 0.0), axis=1, keepdims=True
            )
            return acc * jnp.exp(log) + got[j].astype(F32)

        acc = jnp.zeros(got.shape[1:], F32)
        for i in range(n):
            acc = scan_one(i, acc)
        entered[me] = enter[me]
        for k in range(1, n):
            enter_copy((me + k) % n, me).start()

    def scan_early():
        pl.when(me < late)(scan_states)

    def scan_late():
        pl.when(me >= late)(scan_states)

    def finish_pair(j):
        for owner in range(4 * j, 4 * j + 4):
            @pl.when(me != owner)
            def _():
                enter_copy(me, owner).wait_recv()

        outs = []
        gains = head_gain_ref[...].astype(F32).reshape(1, -1)
        gate = silu(rows_f32(j, pw, at_gate)[inner])
        for h in range(2):
            head = 2 * j + h
            cols = table_ref[:, 4 * head : 4 * head + 4]
            wide = jnp.concatenate([entered[2 * head], entered[2 * head + 1]], axis=0)
            both = lax.dot_general(
                reads[:, head * STATE : (head + 1) * STATE], wide,
                (((1,), (1,)), ((), ())), preferred_element_type=F32,
            )
            mine = slice(h * HEAD_DIM, (h + 1) * HEAD_DIM)
            y = within[:, head * HEAD_DIM : (head + 1) * HEAD_DIM]
            y = y + both[:, :HEAD_DIM] * jnp.exp(cols[:, 2:3])
            y = y + both[:, HEAD_DIM:] * jnp.exp(cols[:, 3:4])
            g = y * gate[:, mine]
            g = g * lax.rsqrt(jnp.mean(g * g, axis=-1, keepdims=True) + epsilon)
            gain = gains[:, head * HEAD_DIM : (head + 1) * HEAD_DIM]
            outs.append(g * gain)
        y_s[:, j * pw : (j + 1) * pw] = jnp.concatenate(outs, axis=1).astype(BF16)
    def finish_then(j):
        return lambda: finish_pair(j)

    units = {LAG + 1: [make_normed], LAG + 2: [make_tables], LAG + 3: [send_logs]}
    for g in range(pairs):
        units.setdefault(SKEW * g + hops, []).append(project_then(g))
        units.setdefault(SKEW * g + hops + 1, []).insert(0, mix_then(g))
    exit_slot = SKEW * (pairs - 1) + EXIT_LAG
    last_mix = SKEW * (pairs - 1) + hops + 1

    def slot(t):
        for g in range(pairs):
            if g > 0 and t == max(SKEW * g - AHEAD, 0):
                start_group(g)
            if 0 <= t - SKEW * g < hops:
                advance_group(g, t - SKEW * g)
        if t == exit_slot - 1:
            start_exit()
        if 0 <= t - exit_slot < hops:
            advance_exit(t - exit_slot)
        for unit in units.get(t, []):
            unit()

    scan_slot = SKEW * (pairs - 1) + hops
    units[scan_slot].append(scan_early)
    for j in range(pairs - 1):
        units.setdefault(last_mix + 1, []).append(finish_then(j))
    for t in range(last_mix + 2):
        slot(t)
    scan_late()
    def partial(owner, place):
        rows = pl.ds(pl.multiple_of(owner * own_rows, HALO), own_rows)
        cols = pl.ds(pl.multiple_of(place * exit_wide, exit_wide), exit_wide)
        return jnp.dot(
            y_c[rows, :], c_all[:, cols], preferred_element_type=F32
        ) + jnp.dot(y_s[rows, :], s_all[:, cols], preferred_element_type=F32)

    def place_of(step, passed):
        if passed:
            return device(spot + turn * step) + 1 - 2 * core
        return device(spot - turn * step)

    def partial_copy(step, passed):
        at = 2 * step + passed
        return send_to(
            away.at[at], came.at[at], p_out.at[at], p_in.at[at], {"tp": 1 - tp_me}
        )

    def send_blocks(step):
        for passed in range(2):
            for which in range(2):
                if passed:
                    pass_copy(which, step, True).wait_recv()
                elif step == 0:
                    exit_own_copies[which].wait()
            away[2 * step + passed] = partial(1 - tp_me, place_of(step, passed)).astype(BF16)
            partial_copy(step, passed).start()

    rest = list(range(last_mix + 2, exit_slot + hops))
    for t in rest[:AWAIT]:
        slot(t)
    finish_pair(pairs - 1)
    done = min(hops, max(exit_slot + hops - len(rest[AWAIT:]) - exit_slot, 0))
    for step in range(done):
        send_blocks(step)
    for t in rest[AWAIT:]:
        slot(t)
        send_blocks(t - exit_slot)
    send_blocks(hops)
    for step in range(chips):
        for passed in range(2):
            place = place_of(step, passed)
            kept = partial(tp_me, place)
            partial_copy(step, passed).wait_recv()
            cols = pl.ds(pl.multiple_of(place * exit_wide, exit_wide), exit_wide)
            out_ref[:, cols] = (kept + came[2 * step + passed].astype(F32)).astype(BF16)
    for step in range(chips):
        for passed in range(2):
            partial_copy(step, passed).wait_send()
    for k in range(1, n):
        log_copy(k).wait_send()
        other = (me + k) % n
        enter_copy(other, me).wait_send()
        state_copy(other).wait_send()
    for step in range(chips):
        for which in range(2):
            if step < hops:
                exit_copy(which, step).wait_send()
            pass_copy(which, step).wait_send()

    def drain(step, _):
        for g in range(pairs):
            for way in range(2):
                @pl.when(step < hops)
                def _():
                    ring_copy(g, step, way).wait_send()

                mate_copy(g, step, way).wait_send()
        return 0

    lax.fori_loop(0, chips, drain, 0)


def mixer(
    rows, gain, conv_w, rec_w, lat_w, step_w, rate, spike,
    conv_taps, x_taps, latent_taps, head_gain, exit_c, exit_s,
):
    n = lax.axis_size("sp")
    chips = n // 2
    hops = chips - 1
    own_rows, width = rows.shape
    length = 2 * own_rows
    full = length + 2 * HALO
    depth = conv_w.shape[1]
    blocks = sum(w.shape[0] for w in (conv_w, rec_w, lat_w))
    cols = sum(w.shape[0] * w.shape[2] for w in (conv_w, rec_w, lat_w))
    heads = spike.shape[0]
    pairs = heads // 2
    conv_width, ssd_width = exit_c.shape[0], exit_s.shape[0]
    state_width = latent_taps.shape[2]
    assert 4 * heads <= STATE and 2 * heads == n and conv_width == ssd_width
    vmem = pl.BlockSpec(memory_space=pltpu.VMEM)
    hbm = pl.BlockSpec(memory_space=pl.ANY)
    spans = (n, HEAD_DIM, STATE)
    parts = (n, own_rows, width // n)
    dma = pltpu.SemaphoreType.DMA
    return pl.pallas_call(
        functools.partial(mixer_kernel, n),
        out_shape=jax.ShapeDtypeStruct((own_rows, width), BF16),
        in_specs=[hbm, vmem, hbm, hbm, hbm] + [vmem] * 7 + [hbm] * 2,
        out_specs=vmem,
        scratch_shapes=[
            pltpu.VMEM((pairs, n * depth, cols // pairs), BF16),
            pltpu.VMEM((full, width), BF16),
            pltpu.VMEM((full, width), BF16),
            pltpu.VMEM((pairs, full, cols // pairs), BF16),
            pltpu.VMEM((length, STATE), F32),
            pltpu.VMEM((STATE, length), F32),
            pltpu.VMEM((8, STATE), F32),
            pltpu.VMEM((conv_width, width), BF16),
            pltpu.VMEM((ssd_width, width), BF16),
            pltpu.VMEM((length, conv_width), BF16),
            pltpu.VMEM((length, ssd_width), BF16),
            pltpu.VMEM((length, ssd_width), F32),
            pltpu.VMEM((length, state_width), BF16),
            pltpu.VMEM(spans, BF16),
            pltpu.VMEM(spans, BF16),
            pltpu.VMEM((n, 8, STATE), F32),
            pltpu.VMEM(spans, BF16),
            pltpu.VMEM(spans, BF16),
            pltpu.VMEM(parts, BF16),
            pltpu.VMEM(parts, BF16),
            dma((pairs * blocks,)), dma((2,)), dma, dma((3,)), dma((3,)),
            dma((pairs, hops, 2)), dma((pairs, hops, 2)),
            dma((pairs, chips, 2)), dma((pairs, chips, 2)),
            dma((hops, 2)), dma((hops, 2)), dma((chips, 2)), dma((chips, 2)),
        ]
        + [dma((n,))] * 6
        + [dma((n,))] * 2,
        compiler_params=pltpu.CompilerParams(
            collective_id=2, has_side_effects=True, vmem_limit_bytes=58 * 2**20
        ),
        cost_estimate=pl.CostEstimate(
            flops=2 * full * width * cols, bytes_accessed=2 * width * cols, transcendentals=0
        ),
    )(
        rows, gain, conv_w, rec_w, lat_w, step_w, rate, spike,
        conv_taps, x_taps, latent_taps, head_gain, exit_c, exit_s,
    )


def project_kernel(r_ref, w_ref, o_ref):
    o_ref[...] = jnp.dot(r_ref[...], w_ref[...], preferred_element_type=F32).astype(BF16)


def project(rows, weights):
    count, width = rows.shape
    cols = weights.shape[1]
    tile = cols // 9
    return pl.pallas_call(
        project_kernel,
        grid=(9,),
        in_specs=[
            pl.BlockSpec((count, width), lambda j: (0, 0)),
            pl.BlockSpec((width, tile), lambda j: (0, j)),
        ],
        out_specs=pl.BlockSpec((count, tile), lambda j: (0, j)),
        out_shape=jax.ShapeDtypeStruct((count, cols), BF16),
        cost_estimate=pl.CostEstimate(
            flops=2 * count * width * cols, bytes_accessed=2 * width * cols, transcendentals=0
        ),
    )(rows, weights)


def finish_kernel(within_ref, reads_ref, enter_ref, gate_ref, gain_ref, col_ref, y_ref):
    length = y_ref.shape[0]
    cols = col_ref[0]
    outs = []
    for h in range(2):
        o = 4 * h
        both = lax.dot_general(
            reads_ref[:, h * STATE : (h + 1) * STATE],
            enter_ref[h * STATE : (h + 1) * STATE],
            (((1,), (1,)), ((), ())),
            preferred_element_type=F32,
        )
        here = slice(h * HEAD_DIM, (h + 1) * HEAD_DIM)
        y = within_ref[:, here]
        y = y + both[:, :HEAD_DIM] * jnp.exp(cols[:, o + 2 : o + 3])
        y = y + both[:, HEAD_DIM:] * jnp.exp(cols[:, o + 3 : o + 4])
        g = y * silu(gate_ref[pl.ds(HALO, length), :].astype(F32)[:, here])
        g = g * lax.rsqrt(jnp.mean(g * g, axis=-1, keepdims=True) + epsilon)
        outs.append(g * gain_ref[:, here].astype(F32))
    y_ref[...] = jnp.concatenate(outs, axis=1).astype(BF16)


def local(
    layer_source_rows, entry_rescale_factor, sliding_mixer_entry_matrix,
    recurrent_mixer_entry_matrix, latent_write_read_matrix, timestep_matrix,
    sliding_kernel_coefficients, recurrent_kernel_coefficients, latent_kernel_coefficients,
    lane_forgetting_rate, spike_forgetting_rate, lane_rescale_factor,
    sliding_mixer_exit_matrix, recurrent_mixer_exit_matrix,
):
    n = lax.axis_size("sp")
    tp = lax.axis_size("tp")
    own_rows, width = layer_source_rows.shape
    length = own_rows * tp
    full = length + 2 * HALO
    conv_width = sliding_mixer_entry_matrix.shape[2]
    ssd_width = recurrent_mixer_entry_matrix.shape[2]
    state_width = latent_write_read_matrix.shape[2]
    heads = timestep_matrix.shape[2]
    pairs = heads // 2
    cw = conv_width // pairs

    share = heads * 2 * HEAD_DIM // n
    if tp == 2 and 2 * heads == n:
        return mixer(
            layer_source_rows, entry_rescale_factor, sliding_mixer_entry_matrix,
            recurrent_mixer_entry_matrix, latent_write_read_matrix,
            timestep_matrix.transpose(1, 2, 0).reshape(2 * heads, width),
            lane_forgetting_rate, spike_forgetting_rate.T, sliding_kernel_coefficients,
            recurrent_kernel_coefficients, latent_kernel_coefficients, lane_rescale_factor,
            sliding_mixer_exit_matrix, recurrent_mixer_exit_matrix,
        )

    block = jnp.concatenate(
        [sliding_mixer_entry_matrix[i] for i in range(3)]
        + [recurrent_mixer_entry_matrix[i] for i in range(2)]
        + [latent_write_read_matrix[i] for i in range(2)],
        axis=1,
    )
    gathered = gather_rows(block)
    weights = gathered.reshape(n * block.shape[0], block.shape[1])

    x32 = layer_source_rows.astype(F32)
    normed = (
        x32
        * lax.rsqrt(jnp.mean(x32 * x32, axis=-1, keepdims=True) + epsilon)
        * entry_rescale_factor.astype(F32)
    ).astype(BF16)
    up = [(i, i + 1) for i in range(n - 1)]
    down = [(i + 1, i) for i in range(n - 1)]
    before = lax.ppermute(normed[own_rows - HALO :], "sp", up)
    after = lax.ppermute(normed[:HALO], "sp", down)
    shared = lax.all_gather(jnp.concatenate([before, normed, after], axis=0), "tp", axis=0)
    rows = jnp.concatenate(
        [shared[tp - 1, :HALO]]
        + [shared[i, HALO : HALO + own_rows] for i in range(tp)]
        + [shared[0, HALO + own_rows :]],
        axis=0,
    )

    step_weight = timestep_matrix.reshape(width, 2 * heads)
    raw = jnp.dot(rows, step_weight, preferred_element_type=F32).astype(BF16)
    raw = raw[HALO : HALO + length].astype(F32).reshape(length, 2, heads)
    deltas = jax.nn.softplus(raw)
    logs = -deltas * lane_forgetting_rate[None] + spike_forgetting_rate[:, None, :]
    tri = (jnp.arange(length)[:, None] >= jnp.arange(length)[None, :]).astype(F32)
    run_f = jnp.dot(tri, logs[:, 0], precision=HIGHEST)
    run_b = jnp.dot(tri.T, logs[:, 1], precision=HIGHEST)
    table = jnp.stack([deltas[:, 0], deltas[:, 1], run_f, run_b], axis=2)
    col_table = table.reshape(length, pairs, 8).transpose(1, 0, 2)
    row_table = table.reshape(length, pairs, 8).transpose(1, 2, 0)
    span_log = jnp.stack([run_f[length - 1], run_b[0]], axis=1)
    exit_c, exit_s, weights = lax.optimization_barrier(
        (sliding_mixer_exit_matrix, recurrent_mixer_exit_matrix, weights)
    )
    proj = project(rows, weights)
    exit_c = lax.all_gather(exit_c, "sp", axis=1, tiled=True)
    exit_s = lax.all_gather(exit_s, "sp", axis=1, tiled=True)

    latent = latent_kernel_coefficients
    pw, sw = 2 * HEAD_DIM, 2 * STATE
    g0 = 3 * conv_width
    at_gate, at_x = g0 // pw, (g0 + ssd_width) // pw
    at_b = (g0 + 2 * ssd_width) // sw
    at_c = at_b + pairs
    y_conv, within, reads, states = pl.pallas_call(
        mix_kernel,
        grid=(pairs,),
        in_specs=[
            pl.BlockSpec((full, cw), lambda j: (0, j)),
            pl.BlockSpec((full, cw), lambda j: (0, pairs + j)),
            pl.BlockSpec((full, cw), lambda j: (0, 2 * pairs + j)),
            pl.BlockSpec((full, pw), lambda j: (0, at_x + j)),
            pl.BlockSpec((full, sw), lambda j: (0, at_b + j)),
            pl.BlockSpec((full, sw), lambda j: (0, at_c + j)),
            pl.BlockSpec((3, cw), lambda j: (0, j)),
            pl.BlockSpec((5, pw), lambda j: (0, j)),
            pl.BlockSpec((5, sw), lambda j: (0, j)),
            pl.BlockSpec((5, sw), lambda j: (0, pairs + j)),
            pl.BlockSpec((1, length, 8), lambda j: (j, 0, 0)),
            pl.BlockSpec((1, 8, length), lambda j: (j, 0, 0)),
        ],
        out_specs=[
            pl.BlockSpec((length, cw), lambda j: (0, j)),
            pl.BlockSpec((length, pw), lambda j: (0, j)),
            pl.BlockSpec((length, sw), lambda j: (0, j)),
            pl.BlockSpec((sw, STATE), lambda j: (j, 0)),
        ],
        out_shape=[
            jax.ShapeDtypeStruct((length, conv_width), BF16),
            jax.ShapeDtypeStruct((length, ssd_width), F32),
            jax.ShapeDtypeStruct((length, state_width), BF16),
            jax.ShapeDtypeStruct((pairs * sw, STATE), BF16),
        ],
        cost_estimate=pl.CostEstimate(
            flops=8 * length * length * heads * STATE, bytes_accessed=2**24, transcendentals=0
        ),
    )(
        proj, proj, proj, proj, proj, proj,
        sliding_kernel_coefficients, recurrent_kernel_coefficients,
        latent.reshape(latent.shape[0], -1), latent.reshape(latent.shape[0], -1),
        col_table, row_table,
    )

    entering = exchange_states(states.reshape(n, share, STATE), span_log)
    entering = entering.reshape(pairs * sw, STATE)

    y_ssd = pl.pallas_call(
        finish_kernel,
        grid=(pairs,),
        in_specs=[
            pl.BlockSpec((length, pw), lambda j: (0, j)),
            pl.BlockSpec((length, sw), lambda j: (0, j)),
            pl.BlockSpec((sw, STATE), lambda j: (j, 0)),
            pl.BlockSpec((full, pw), lambda j: (0, at_gate + j)),
            pl.BlockSpec((1, pw), lambda j: (0, j)),
            pl.BlockSpec((1, length, 8), lambda j: (j, 0, 0)),
        ],
        out_specs=pl.BlockSpec((length, pw), lambda j: (0, j)),
        out_shape=jax.ShapeDtypeStruct((length, ssd_width), BF16),
    )(within, reads, entering, proj, lane_rescale_factor.reshape(1, -1), col_table)

    def partial(y_c, y_s):
        return (
            jnp.dot(y_c, exit_c, preferred_element_type=F32)
            + jnp.dot(y_s, exit_s, preferred_element_type=F32)
        ).astype(BF16)

    if tp != 2:
        return lax.psum_scatter(
            partial(y_conv, y_ssd), "tp", scatter_dimension=0, tiled=True
        )
    tp_me = lax.axis_index("tp")

    def rows_of(owner, y):
        return lax.dynamic_slice_in_dim(y, owner * own_rows, own_rows, axis=0)

    away = partial(rows_of(1 - tp_me, y_conv), rows_of(1 - tp_me, y_ssd))
    arrived = lax.ppermute(away, "tp", [(0, 1), (1, 0)])
    kept = partial(rows_of(tp_me, y_conv), rows_of(tp_me, y_ssd))
    return (kept.astype(F32) + arrived.astype(F32)).astype(BF16)


def solution(mesh):
    placed = (
        P(("sp", "tp"), None),
        P(),
        P(None, "sp", "tp"),
        P(None, "sp", "tp"),
        P(None, "sp", "tp"),
        P(None, None, "tp"),
        P(None, "tp"),
        P(None, "tp"),
        P(None, None, "tp"),
        P(None, "tp"),
        P("sp", "tp"),
        P("tp"),
        P("tp", "sp"),
        P("tp", "sp"),
    )
    return jax.shard_map(
        local, mesh=mesh, in_specs=placed, out_specs=P(("sp", "tp"), None), check_vma=False
    )
```
